128 devices in a mesh: fs: 16 (over z, y), tp: 8 (over x, core).
Axes of the slice: x: 4, y: 4, z: 4, core: 2. Of those that a mesh axis runs over, the one named last changes fastest.
Arguments:
- weights_in: float32 [2, 2048, 5632], P(None, 'fs', 'tp'), may hold values from -6 to 6
- weights_mix: float32 [2048, 2048], P('fs', 'tp'), may hold values from -6 to 6
- momentum_in: float32 [2, 2048, 5632], P(None, 'fs', 'tp'), may hold values from -5 to 5
- momentum_mix: float32 [2048, 2048], P('fs', 'tp'), may hold values from -5 to 5
- grads_in: float32 [2, 2048, 5632], P(None, 'fs', 'tp'), may hold values from -5 to 5
- grads_mix: float32 [2048, 2048], P('fs', 'tp'), may hold values from -5 to 5
Outputs:
- momentum_in_next: float32 [2, 2048, 5632], P(None, 'fs', 'tp')
- momentum_mix_next: float32 [2048, 2048], P('fs', 'tp')
- weights_in_next: float32 [2, 2048, 5632], P(None, 'fs', 'tp')
- weights_mix_next: float32 [2048, 2048], P('fs', 'tp')
- update_in: float32 [2, 2048, 5632], P(None, 'fs', 'tp')
- update_mix: float32 [2048, 2048], P('fs', 'tp')
The draws below stay inside these ranges and needn't reach their ends.
All inputs are finite; a program needn't handle non-finite values.
Results may differ from the reference program's by a relative error of at most 0.0003.
Values sent between devices are 32-bit elements; how exact they have to be, the bound alone decides.
A program may use at most 128 MiB of HBM per device.

```python
import math
import jax
import jax.numpy as jnp
from jax import lax

D = 2048
FF = 5632
ITERS = 3


def unit_field(key, shape):
    return jnp.clip(jax.random.normal(key, shape, jnp.float32), -5.0, 5.0)


def draw_momentum_in(key, part):
    return unit_field(jax.random.fold_in(key, 11), (2, D, FF))


def draw_momentum_mix(key, part):
    return unit_field(jax.random.fold_in(key, 12), (D, D))


def draw_grads_in(key, part):
    return unit_field(jax.random.fold_in(key, 13), (2, D, FF))


def draw_grads_mix(key, part):
    return unit_field(jax.random.fold_in(key, 14), (D, D))


def steps_of(key, dims, cuts, smallest, top_value):
    def one(position, parts):
        draws = jax.random.uniform(jax.random.fold_in(jax.random.fold_in(key, 6), position), (parts,), jnp.float32, smallest / len(cuts), top_value / len(cuts))
        return jnp.repeat(jnp.exp(draws), dims[position] // parts).reshape((-1,) + (1,) * (len(dims) - position - 1))

    gain = one(*cuts[0])
    for cut in cuts[1:]:
        gain = gain * one(*cut)
    return gain


def noise(rng, extent, deviation, limit, cuts=(), dtype=jnp.bfloat16):
    factor_of = steps_of(rng, extent, cuts, -0.22, 0.18) if cuts else 1.0
    values = jax.random.normal(rng, extent, jnp.float32) * deviation * factor_of
    return jnp.minimum(jnp.maximum(values, -limit), limit).astype(dtype)


def setup_inputs(seed: int = 0) -> dict:
    streams_of = jax.random.split(jax.random.key(seed), 7)
    weights_in = noise(streams_of[0], (2, D, FF), 1.0, 6.0, ((1, 16), (2, 8)), jnp.float32)
    weights_mix = noise(streams_of[1], (D, D), 1.0, 6.0, ((0, 16), (1, 8)), jnp.float32)
    momentum_in = draw_momentum_in(jax.random.fold_in(streams_of[6], 71), 0)
    momentum_mix = draw_momentum_mix(jax.random.fold_in(streams_of[6], 71), 0)
    grads_in = draw_grads_in(jax.random.fold_in(streams_of[6], 71), 0)
    grads_mix = draw_grads_mix(jax.random.fold_in(streams_of[6], 71), 0)
    return {"weights_in": weights_in, "weights_mix": weights_mix, "momentum_in": momentum_in, "momentum_mix": momentum_mix, "grads_in": grads_in, "grads_mix": grads_mix}


A_COEF = 3.4445
B_COEF = -4.775
C_COEF = 2.0315
MOMENTUM_DECAY = 0.95
STEP_RATE = 0.02
HIGH = lax.Precision.HIGHEST

def orthogonal(moment):
    row_total, col_total = moment.shape
    current = moment
    for iteration in range(ITERS):
        gram_sum = jnp.dot(current, current.T, precision=HIGH)
        if iteration == 0:
            scaling = 0.5 * lax.rsqrt(jnp.maximum(jnp.trace(gram_sum) / D, 1.0))
        else:
            scaling = jnp.float32(1.0)
        square = jnp.dot(gram_sum, gram_sum, precision=HIGH)
        poly_mat = scaling ** 2 * B_COEF * gram_sum + scaling ** 4 * C_COEF * square
        current = scaling * (A_COEF * current + jnp.dot(poly_mat, current, precision=HIGH))
    return current * math.sqrt(max(row_total, col_total))

def reference(weights_in, weights_mix, momentum_in, momentum_mix, grads_in, grads_mix):
    moment_in = MOMENTUM_DECAY * momentum_in + grads_in
    moment_mix = MOMENTUM_DECAY * momentum_mix + grads_mix
    step_in = jnp.stack([orthogonal(moment_in[0]), orthogonal(moment_in[1])])
    step_mix = orthogonal(moment_mix)
    return (moment_in, moment_mix, weights_in - STEP_RATE * step_in, weights_mix - STEP_RATE * step_mix, step_in, step_mix)
```

```python
import functools
import math

import jax
import jax.numpy as jnp
from jax import lax
from jax.experimental import pallas as pl
from jax.experimental.pallas import tpu as pltpu
from jax.sharding import PartitionSpec as P

D = 2048
FF = 5632
ITERS = 3

A_COEF = 3.4445
B_COEF = -4.775
C_COEF = 2.0315
MOMENTUM_DECAY = 0.95
STEP_RATE = 0.02
HIGH = lax.Precision.HIGH
MESH = pl.DeviceIdType.MESH

SIDE = 4
PLANE = SIDE * SIDE
WIDE = 640
ODD = 64
MIX = 256
PACKED = 2 * WIDE + 2 * ODD + MIX


def put(src, dst, send, recv, fs, tp):
    return pltpu.make_async_remote_copy(
        src_ref=src, dst_ref=dst, send_sem=send, recv_sem=recv, device_id=(fs, tp), device_id_type=MESH
    )


def greet(peers):
    barrier = pltpu.get_barrier_semaphore()
    for fs, tp in peers:
        pl.semaphore_signal(barrier, inc=1, device_id=(fs, tp), device_id_type=MESH)
    pl.semaphore_wait(barrier, len(peers))


def ring_place(cycle, z, y):
    return SIDE * (z if cycle == 0 else y) + lax.rem(z + y, SIDE)


def ring_fs(cycle, place):
    a = place // SIDE
    b = lax.rem(place - a + SIDE, SIDE)
    return SIDE * a + b if cycle == 0 else SIDE * b + a


def plane_gather_kernel(pieces, paired, block, out, send, recv, own_sem, pair_send, pair_recv):
    fs, tp = lax.axis_index("fs"), lax.axis_index("tp")
    z, y = fs // SIDE, lax.rem(fs, SIDE)
    core = lax.rem(tp, 2)
    other = tp + 1 - 2 * core
    rows, cols = block.shape
    quarter = rows // 4
    per_ring = len(pieces)
    rings = [(cycle, way) for cycle in (0, 1) for way in (1, -1)]
    place = [ring_place(cycle, z, y) for cycle in (0, 1)]
    nexts = [ring_fs(c, lax.rem(place[c] + PLANE + w, PLANE)) for c, w in rings]
    peers = [(n, tp) for n in nexts]
    if paired:
        peers.append((fs, other))
    greet(peers)

    def slot(origin, row, height, col, width):
        where = (origin, core) if paired else (origin,)
        return out.at[where + (pl.ds(row, height), pl.ds(col, width))]

    def own(row, height, col, width):
        return block.at[pl.ds(row, height), pl.ds(col, width)]

    def piece_of(k, i):
        row, height, col, width = pieces[i]
        return quarter * k + row, height, col, width

    def hop(step, k, i, first):
        c, w = rings[k]
        origin = ring_fs(c, lax.rem(place[c] + 2 * PLANE - w * step, PLANE))
        spot = piece_of(k, i)
        lane = k * per_ring + i
        return put(own(*spot) if first else slot(origin, *spot), slot(origin, *spot), send.at[lane], recv.at[lane, step], nexts[k], tp)

    mine = out.at[fs, core] if paired else out.at[fs]
    keep = pltpu.make_async_copy(block, mine, own_sem)
    for i in range(per_ring):
        for k in range(4):
            hop(0, k, i, True).start()
    keep.start()
    if paired:
        put(block, mine, pair_send, pair_recv, fs, other).start()

    def pass_on(step, last):
        for i in range(per_ring):
            for k in range(4):
                before = hop(step - 1, k, i, False)
                before.wait_send()
                before.wait_recv()
                if not last:
                    hop(step, k, i, False).start()
        if paired:
            for k in range(4):
                c, w = rings[k]
                origin = ring_fs(c, lax.rem(place[c] + 2 * PLANE - w * step, PLANE))
                there = slot(origin, quarter * k, quarter, 0, cols)
                put(there, there, pair_send, pair_recv, fs, other).start()

    @pl.loop(1, PLANE - 1)
    def _(step):
        pass_on(step, False)

    pass_on(PLANE - 1, True)
    keep.wait()
    if paired:
        sent = put(out.at[:, core], out.at[:, 1 - core], pair_send, pair_recv, fs, other)
        sent.wait_send()
        sent.wait_recv()


def plane_gather(block, pieces, paired, cid):
    rows, cols = block.shape
    shape = (PLANE, 2, rows, cols) if paired else (PLANE, rows, cols)
    lanes = 4 * len(pieces)
    return pl.pallas_call(
        functools.partial(plane_gather_kernel, pieces, paired),
        out_shape=jax.ShapeDtypeStruct(shape, jnp.float32),
        in_specs=[pl.BlockSpec(memory_space=pltpu.VMEM)],
        out_specs=pl.BlockSpec(memory_space=pltpu.VMEM),
        scratch_shapes=[
            pltpu.SemaphoreType.DMA((lanes,)),
            pltpu.SemaphoreType.DMA((lanes, PLANE - 1)),
            pltpu.SemaphoreType.DMA,
            pltpu.SemaphoreType.DMA,
            pltpu.SemaphoreType.DMA,
        ],
        compiler_params=pltpu.CompilerParams(collective_id=cid, has_side_effects=True, vmem_limit_bytes=40 << 20),
        name=f"plane_gather_{cid}",
    )(block)


def reduce_kernel(part, out, pair, total, near, far, hold, send, recv):
    fs, tp = lax.axis_index("fs"), lax.axis_index("tp")
    x, core = tp // 2, lax.rem(tp, 2)
    right = 2 * lax.rem(x + 1, SIDE) + core
    left = 2 * lax.rem(x + SIDE - 1, SIDE) + core
    other = tp + 1 - 2 * core
    greet([(fs, right), (fs, left), (fs, other)])
    copies = [put(part.at[m, 1 - core], pair.at[m], send.at[m], recv.at[m], fs, other) for m in range(3)]
    for c in copies:
        c.start()
    for m, c in enumerate(copies):
        c.wait()
        total[m] = part[m, core] + pair[m]
    total[3] = jnp.zeros_like(total[3])
    half = total.shape[1] // 2
    up, down = pl.ds(0, half), pl.ds(half, half)
    ahead, back, across = lax.rem(x + 1, SIDE), lax.rem(x + SIDE - 1, SIDE), lax.rem(x + 2, SIDE)
    far_right = put(total.at[across, up], far.at[0], send.at[3], recv.at[3], fs, right)
    far_left = put(total.at[across, down], far.at[1], send.at[4], recv.at[4], fs, left)
    near_right = put(total.at[ahead, down], near.at[0], send.at[5], recv.at[5], fs, right)
    near_left = put(total.at[back, up], near.at[1], send.at[6], recv.at[6], fs, left)
    for c in (far_right, far_left, near_right, near_left):
        c.start()
    far_right.wait_recv()
    hold[0] = far[0] + total[ahead, up]
    on_right = put(hold.at[0], near.at[2], send.at[7], recv.at[7], fs, right)
    on_right.start()
    far_left.wait_recv()
    hold[1] = far[1] + total[back, down]
    on_left = put(hold.at[1], near.at[3], send.at[8], recv.at[8], fs, left)
    on_left.start()
    near_right.wait_recv()
    near_left.wait_recv()
    on_right.wait_recv()
    out[up, :] = total[x, up] + near[2] + near[1]
    on_left.wait_recv()
    out[down, :] = total[x, down] + near[3] + near[0]
    for c in (far_right, far_left, near_right, near_left, on_right, on_left):
        c.wait_send()


def reduce_to_planes(part, cid):
    rows, cols = part.shape[2:]
    f32 = jnp.float32
    return pl.pallas_call(
        reduce_kernel,
        out_shape=jax.ShapeDtypeStruct((rows, cols), f32),
        in_specs=[pl.BlockSpec(memory_space=pltpu.VMEM)],
        out_specs=pl.BlockSpec(memory_space=pltpu.VMEM),
        scratch_shapes=[
            pltpu.VMEM((3, rows, cols), f32),
            pltpu.VMEM((4, rows, cols), f32),
            pltpu.VMEM((4, rows // 2, cols), f32),
            pltpu.VMEM((2, rows // 2, cols), f32),
            pltpu.VMEM((2, rows // 2, cols), f32),
            pltpu.SemaphoreType.DMA((9,)),
            pltpu.SemaphoreType.DMA((9,)),
        ],
        compiler_params=pltpu.CompilerParams(collective_id=cid, has_side_effects=True, vmem_limit_bytes=32 << 20),
        name="reduce_to_planes",
    )(part)


def spread_kernel(block, out, send, recv, own_sem, pair_send, pair_recv):
    fs, tp = lax.axis_index("fs"), lax.axis_index("tp")
    x, core = tp // 2, lax.rem(tp, 2)
    right = 2 * lax.rem(x + 1, SIDE) + core
    left = 2 * lax.rem(x + SIDE - 1, SIDE) + core
    other = tp + 1 - 2 * core
    ahead, back, across = lax.rem(x + 1, SIDE), lax.rem(x + SIDE - 1, SIDE), lax.rem(x + 2, SIDE)
    greet([(fs, right), (fs, left), (fs, other)])
    half = block.shape[0] // 2
    parts = [pl.ds(0, half), pl.ds(half, half)]
    go_right = [put(block.at[parts[h]], out.at[x, core, parts[h]], send.at[h], recv.at[h], fs, right) for h in (0, 1)]
    go_left = [put(block.at[parts[1 - h]], out.at[x, core, parts[1 - h]], send.at[2 + h], recv.at[2 + h], fs, left) for h in (0, 1)]
    for h in (0, 1):
        go_right[h].start()
        go_left[h].start()
    keep = pltpu.make_async_copy(block, out.at[x, core], own_sem)
    keep.start()
    put(block, out.at[x, core], pair_send, pair_recv, fs, other).start()
    go_right[0].wait_recv()
    first = out.at[back, core, parts[0]]
    relay_right = put(first, first, send.at[4], recv.at[4], fs, right)
    relay_right.start()
    go_left[0].wait_recv()
    second = out.at[ahead, core, parts[1]]
    relay_left = put(second, second, send.at[5], recv.at[5], fs, left)
    relay_left.start()
    go_right[1].wait_recv()
    put(out.at[back, core], out.at[back, core], pair_send, pair_recv, fs, other).start()
    go_left[1].wait_recv()
    put(out.at[ahead, core], out.at[ahead, core], pair_send, pair_recv, fs, other).start()
    relay_right.wait_recv()
    relay_left.wait_recv()
    put(out.at[across, core], out.at[across, core], pair_send, pair_recv, fs, other).start()
    for c in go_right + go_left + [relay_right, relay_left]:
        c.wait_send()
    keep.wait()
    whole = put(out.at[:, core], out.at[:, 1 - core], pair_send, pair_recv, fs, other)
    whole.wait_send()
    whole.wait_recv()


def spread(block, cid):
    rows, cols = block.shape
    return pl.pallas_call(
        spread_kernel,
        out_shape=jax.ShapeDtypeStruct((SIDE, 2, rows, cols), jnp.float32),
        in_specs=[pl.BlockSpec(memory_space=pltpu.VMEM)],
        out_specs=pl.BlockSpec(memory_space=pltpu.VMEM),
        scratch_shapes=[
            pltpu.SemaphoreType.DMA((6,)),
            pltpu.SemaphoreType.DMA((6,)),
            pltpu.SemaphoreType.DMA,
            pltpu.SemaphoreType.DMA,
            pltpu.SemaphoreType.DMA,
        ],
        compiler_params=pltpu.CompilerParams(collective_id=cid, has_side_effects=True, vmem_limit_bytes=32 << 20),
        name="spread",
    )(block)


def split_into(src, scale, high, low):
    step = 64

    @pl.loop(0, src.shape[0] // step)
    def _(i):
        rows = pl.ds(pl.multiple_of(i * step, step), step)
        value = src[rows, :] * scale
        top = value.astype(jnp.bfloat16)
        high[rows, :] = top
        low[rows, :] = (value - top.astype(jnp.float32)).astype(jnp.bfloat16)


def times(src, dst, pair, high, low):
    rows, size = src.shape
    value = src[...]
    top = value.astype(jnp.bfloat16)
    pair[:rows, :] = top
    pair[rows:, :] = (value - top.astype(jnp.float32)).astype(jnp.bfloat16)
    width = 256

    @pl.loop(0, size // width)
    def _(j):
        cols = pl.ds(pl.multiple_of(j * width, width), width)
        main = jnp.dot(pair[...], high[:, cols], preferred_element_type=jnp.float32)
        rest = jnp.dot(pair[:rows, :], low[:, cols], preferred_element_type=jnp.float32)
        dst[:, cols] = main[:rows] + (main[rows:] + rest)


def first_chain_kernel(whole, own, next_rows, coef_rows, high, low, pair, v, p, w):
    size = whole.shape[1]
    lane = 128

    def diag(i, total):
        at = pl.ds(pl.multiple_of(i * lane, lane), lane)
        block = whole[at, at]
        eye = lax.broadcasted_iota(jnp.int32, block.shape, 0) == lax.broadcasted_iota(jnp.int32, block.shape, 1)
        return total + jnp.where(eye, block, 0.0)

    acc = lax.fori_loop(0, size // lane, diag, jnp.zeros((lane, lane), jnp.float32))
    ssq = jnp.sum(jnp.sum(acc, axis=0, keepdims=True), axis=1, keepdims=True)
    s = 0.5 * lax.rsqrt(jnp.maximum(ssq / D, 1.0))
    split_into(whole, s * s, high, low)
    fs, tp = lax.axis_index("fs"), lax.axis_index("tp")
    start = 128 * fs + 64 * lax.rem(tp, 2)
    shape = own.shape
    on_diag = lax.broadcasted_iota(jnp.int32, shape, 1) == start + lax.broadcasted_iota(jnp.int32, shape, 0)
    v[...] = own[...] * (s * s)
    times(v, p, pair, high, low)
    coef_rows[...] = s * (jnp.where(on_diag, A_COEF, 0.0) + B_COEF * v[...] + C_COEF * p[...])
    times(p, w, pair, high, low)
    w[...] = A_COEF * v[...] + B_COEF * p[...] + C_COEF * w[...]
    times(w, v, pair, high, low)
    times(v, p, pair, high, low)
    next_rows[...] = A_COEF * w[...] + B_COEF * v[...] + C_COEF * p[...]


def second_chain_kernel(whole, coef, out, high, low, pair, base, v, p, q):
    split_into(whole, 1.0, high, low)

    def by_a1(src, dst):
        times(src, p, pair, high, low)
        times(p, q, pair, high, low)
        dst[...] = A_COEF * src[...] + B_COEF * p[...] + C_COEF * q[...]

    by_a1(coef, base)
    out[...] = A_COEF * base[...]
    for src, weight in ((base, B_COEF), (v, C_COEF)):
        times(src, q, pair, high, low)
        v[...] = q[...]
        by_a1(v, v)
        by_a1(v, v)
        out[...] += weight * v[...]


def chain_call(kernel, whole, own, outs, works, name):
    rows, cols = own.shape
    size = whole.shape[0]
    f32, bf16 = jnp.float32, jnp.bfloat16
    vmem = pl.BlockSpec(memory_space=pltpu.VMEM)
    return pl.pallas_call(
        kernel,
        out_shape=[jax.ShapeDtypeStruct((rows, cols), f32)] * outs,
        in_specs=[vmem, vmem],
        out_specs=[vmem] * outs,
        scratch_shapes=[
            pltpu.VMEM((size, cols), bf16),
            pltpu.VMEM((size, cols), bf16),
            pltpu.VMEM((2 * rows, cols), bf16),
        ]
        + [pltpu.VMEM((rows, cols), f32)] * works,
        compiler_params=pltpu.CompilerParams(vmem_limit_bytes=56 << 20),
        name=name,
    )(whole, own)


def only(lanes_low, x):
    lane = lax.broadcasted_iota(jnp.int32, x.shape, x.ndim - 1)
    return jnp.where((lane < ODD) == lanes_low, x, 0.0)


def local(weights_in, weights_mix, momentum_in, momentum_mix, grads_in, grads_mix):
    moment_in = MOMENTUM_DECAY * momentum_in + grads_in
    moment_mix = MOMENTUM_DECAY * momentum_mix + grads_mix
    first, second = moment_in[0], moment_in[1]
    packed = jnp.concatenate(
        [first[:, :WIDE], second[:, :WIDE], first[:, WIDE:], second[:, WIDE:], moment_mix], axis=1
    )
    x_pieces = tuple((16 * i, 16, 0, PACKED) for i in range(2))
    g_pieces = tuple((8 * i, 8, 1024 * j, 1024) for i in range(2) for j in range(2))
    cols = plane_gather(packed, x_pieces, False, 0).reshape(D, PACKED)
    spans = [slice(0, WIDE), slice(WIDE, 2 * WIDE), slice(2 * WIDE, 2 * WIDE + 2 * ODD), slice(2 * WIDE + 2 * ODD, PACKED)]
    a0, a1, odd, mix = (cols[:, s] for s in spans)
    r0, r1, rodd, rmix = (packed[:, s] for s in spans)
    dot_t = functools.partial(lax.dot_general, dimension_numbers=(((1,), (1,)), ((), ())), precision=HIGH)
    part = jnp.stack(
        [
            dot_t(r0, a0) + dot_t(only(True, rodd), odd),
            dot_t(r1, a1) + dot_t(only(False, rodd), odd),
            dot_t(rmix, mix),
        ]
    ).reshape(3, 2, 64, D)
    own = reduce_to_planes(part, 1)
    gram = plane_gather(own, g_pieces, True, 2).reshape(D, D)
    next_rows, coef = chain_call(first_chain_kernel, gram, own, 2, 3, "first_chain")
    gram1 = plane_gather(next_rows, g_pieces, True, 3).reshape(D, D)
    (poly,) = chain_call(second_chain_kernel, gram1, coef, 1, 4, "second_chain")
    polys = spread(poly, 4).reshape(SIDE, 128, D)
    dot = functools.partial(jnp.dot, precision=HIGH)
    odds = dot(polys[:2].reshape(256, D), odd)
    y0 = jnp.concatenate([dot(polys[0], a0), odds[:128, :ODD]], axis=1)
    y1 = jnp.concatenate([dot(polys[1], a1), odds[128:, ODD:]], axis=1)
    step_in = jnp.stack([y0, y1]) * math.sqrt(max(D, FF))
    step_mix = dot(polys[2], mix) * math.sqrt(D)
    return (
        moment_in,
        moment_mix,
        weights_in - STEP_RATE * step_in,
        weights_mix - STEP_RATE * step_mix,
        step_in,
        step_mix,
    )


def solution(mesh):
    specs = (
        P(None, "fs", "tp"),
        P("fs", "tp"),
        P(None, "fs", "tp"),
        P("fs", "tp"),
        P(None, "fs", "tp"),
        P("fs", "tp"),
    )
    return jax.shard_map(local, mesh=mesh, in_specs=specs, out_specs=specs, check_vma=False)
```

```python
import functools
import math

import jax
import jax.numpy as jnp
from jax import lax
from jax.experimental import pallas as pl
from jax.experimental.pallas import tpu as pltpu
from jax.sharding import PartitionSpec as P

D = 2048
FF = 5632
ITERS = 3

A_COEF = 3.4445
B_COEF = -4.775
C_COEF = 2.0315
MOMENTUM_DECAY = 0.95
STEP_RATE = 0.02
HIGH = lax.Precision.HIGH
MESH = pl.DeviceIdType.MESH

SIDE = 4
PLANE = SIDE * SIDE
LANE = 128
TURN = PLANE // 2 + 1
WIDE = 640
ODD = 64
MIX = 256
PACKED = 2 * WIDE + 2 * ODD + MIX


def put(src, dst, send, recv, fs, tp):
    return pltpu.make_async_remote_copy(
        src_ref=src, dst_ref=dst, send_sem=send, recv_sem=recv, device_id=(fs, tp), device_id_type=MESH
    )


def greet(peers):
    barrier = pltpu.get_barrier_semaphore()
    for fs, tp in peers:
        pl.semaphore_signal(barrier, inc=1, device_id=(fs, tp), device_id_type=MESH)
    pl.semaphore_wait(barrier, len(peers))


def plane_gather_kernel(paired, block, out, send, recv, own_sem, pair_send, pair_recv):
    fs, tp = lax.axis_index("fs"), lax.axis_index("tp")
    z, y = fs // SIDE, lax.rem(fs, SIDE)
    core = lax.rem(tp, 2)
    other = tp + 1 - 2 * core
    half = block.shape[0] // 2
    quarter = half // 2
    ways = (1, -1)

    def at(along_y, along_z):
        return SIDE * lax.rem(z + along_z + SIDE, SIDE) + lax.rem(y + along_y + SIDE, SIDE)

    def near(h, first, second):
        return at(first, second) if h == 0 else at(second, first)

    peers = [(near(0, w, 0), tp) for w in ways] + [(near(1, w, 0), tp) for w in ways]
    if paired:
        peers.append((fs, other))
    greet(peers)

    def slot(origin, rows):
        return out.at[origin, core, rows] if paired else out.at[origin, rows]

    count = iter(range(40))
    started = []

    def move(origin, rows, target, src=None):
        lane = next(count)
        dst = slot(origin, rows)
        copy = put(dst if src is None else src, dst, send.at[lane], recv.at[lane], target, tp)
        copy.start()
        started.append(copy)
        return copy

    def halves(h):
        return pl.ds(h * half, half)

    def quarters(h, i):
        return pl.ds(h * half + i * quarter, quarter)

    def to_pair(origin, rows):
        if paired:
            put(slot(origin, rows), slot(origin, rows), pair_send, pair_recv, fs, other).start()

    direct = {(h, i): move(fs, halves(h), near(h, w, 0), block.at[halves(h)]) for i, w in enumerate(ways) for h in (0, 1)}
    second = {(h, i, 0): move(fs, halves(h), near(h, 0, w), block.at[halves(h)]) for i, w in enumerate(ways) for h in (0, 1)}
    mine = out.at[fs, core] if paired else out.at[fs]
    keep = pltpu.make_async_copy(block, mine, own_sem)
    keep.start()
    if paired:
        put(block, mine, pair_send, pair_recv, fs, other).start()
    relay = {}
    for i, w in enumerate(ways):
        for h in (0, 1):
            direct[h, i].wait_recv()
            origin = near(h, -w, 0)
            relay[h, i] = move(origin, quarters(h, i), near(h, w, 0))
            for j, w2 in enumerate(ways):
                second[h, j, -w] = move(origin, halves(h), near(h, 0, w2))
            to_pair(origin, halves(h))
    for h in (0, 1):
        for i in (0, 1):
            relay[h, i].wait_recv()
        origin = near(h, 2, 0)
        for j, w2 in enumerate(ways):
            second[h, j, 2] = move(origin, halves(h), near(h, 0, w2))
        to_pair(origin, halves(h))
    tail = []
    for e in (0, -1, 1, 2):
        for j, w2 in enumerate(ways):
            for h in (0, 1):
                second[h, j, e].wait_recv()
                origin = near(h, e, -w2)
                tail.append((h, j, e, move(origin, quarters(h, j), near(h, 0, w2))))
                to_pair(origin, halves(h))
    for h, j, e, copy in tail:
        copy.wait_recv()
        to_pair(near(h, e, 2), quarters(h, j))
    for copy in started:
        copy.wait_send()
    keep.wait()
    if paired:
        sent = put(out.at[:, core], out.at[:, 1 - core], pair_send, pair_recv, fs, other)
        sent.wait_send()
        sent.wait_recv()


def plane_gather(block, paired, cid):
    rows, cols = block.shape
    shape = (PLANE, 2, rows, cols) if paired else (PLANE, rows, cols)
    return pl.pallas_call(
        functools.partial(plane_gather_kernel, paired),
        out_shape=jax.ShapeDtypeStruct(shape, jnp.float32),
        in_specs=[pl.BlockSpec(memory_space=pltpu.VMEM)],
        out_specs=pl.BlockSpec(memory_space=pltpu.VMEM),
        scratch_shapes=[
            pltpu.SemaphoreType.DMA((40,)),
            pltpu.SemaphoreType.DMA((40,)),
            pltpu.SemaphoreType.DMA,
            pltpu.SemaphoreType.DMA,
            pltpu.SemaphoreType.DMA,
        ],
        compiler_params=pltpu.CompilerParams(collective_id=cid, has_side_effects=True, vmem_limit_bytes=24 << 20),
        name=f"plane_gather_{cid}",
    )(block)


def turned(rows, dst):
    fs = lax.axis_index("fs")
    for b in range(TURN):
        col = pl.multiple_of(LANE * lax.rem(fs + b, PLANE), LANE)
        dst[:, pl.ds(LANE * b, LANE)] = rows[:, pl.ds(col, LANE)]


def reduce_kernel(part, out, out_turned, pair, total, near, far, hold, send, recv):
    fs, tp = lax.axis_index("fs"), lax.axis_index("tp")
    x, core = tp // 2, lax.rem(tp, 2)
    right = 2 * lax.rem(x + 1, SIDE) + core
    left = 2 * lax.rem(x + SIDE - 1, SIDE) + core
    other = tp + 1 - 2 * core
    greet([(fs, right), (fs, left), (fs, other)])
    copies = [put(part.at[m, 1 - core], pair.at[m], send.at[m], recv.at[m], fs, other) for m in range(3)]
    for c in copies:
        c.start()
    for m, c in enumerate(copies):
        c.wait()
        total[m] = part[m, core] + pair[m]
    total[3] = jnp.zeros_like(total[3])
    half = total.shape[1] // 2
    up, down = pl.ds(0, half), pl.ds(half, half)
    ahead, back, across = lax.rem(x + 1, SIDE), lax.rem(x + SIDE - 1, SIDE), lax.rem(x + 2, SIDE)
    far_right = put(total.at[across, up], far.at[0], send.at[3], recv.at[3], fs, right)
    far_left = put(total.at[across, down], far.at[1], send.at[4], recv.at[4], fs, left)
    near_right = put(total.at[ahead, down], near.at[0], send.at[5], recv.at[5], fs, right)
    near_left = put(total.at[back, up], near.at[1], send.at[6], recv.at[6], fs, left)
    for c in (far_right, far_left, near_right, near_left):
        c.start()
    far_right.wait_recv()
    hold[0] = far[0] + total[ahead, up]
    on_right = put(hold.at[0], near.at[2], send.at[7], recv.at[7], fs, right)
    on_right.start()
    far_left.wait_recv()
    hold[1] = far[1] + total[back, down]
    on_left = put(hold.at[1], near.at[3], send.at[8], recv.at[8], fs, left)
    on_left.start()
    near_right.wait_recv()
    near_left.wait_recv()
    on_right.wait_recv()
    out[up, :] = total[x, up] + near[2] + near[1]
    on_left.wait_recv()
    out[down, :] = total[x, down] + near[3] + near[0]
    turned(out, out_turned)
    for c in (far_right, far_left, near_right, near_left, on_right, on_left):
        c.wait_send()


def reduce_to_planes(part, cid):
    rows, cols = part.shape[2:]
    f32 = jnp.float32
    return pl.pallas_call(
        reduce_kernel,
        out_shape=[jax.ShapeDtypeStruct((rows, cols), f32), jax.ShapeDtypeStruct((rows, TURN * LANE), f32)],
        in_specs=[pl.BlockSpec(memory_space=pltpu.VMEM)],
        out_specs=[pl.BlockSpec(memory_space=pltpu.VMEM)] * 2,
        scratch_shapes=[
            pltpu.VMEM((3, rows, cols), f32),
            pltpu.VMEM((4, rows, cols), f32),
            pltpu.VMEM((4, rows // 2, cols), f32),
            pltpu.VMEM((2, rows // 2, cols), f32),
            pltpu.VMEM((2, rows // 2, cols), f32),
            pltpu.SemaphoreType.DMA((9,)),
            pltpu.SemaphoreType.DMA((9,)),
        ],
        compiler_params=pltpu.CompilerParams(collective_id=cid, has_side_effects=True, vmem_limit_bytes=32 << 20),
        name="reduce_to_planes",
    )(part)


def spread_kernel(block, out, send, recv, own_sem, pair_send, pair_recv):
    fs, tp = lax.axis_index("fs"), lax.axis_index("tp")
    x, core = tp // 2, lax.rem(tp, 2)
    right = 2 * lax.rem(x + 1, SIDE) + core
    left = 2 * lax.rem(x + SIDE - 1, SIDE) + core
    other = tp + 1 - 2 * core
    ahead, back, across = lax.rem(x + 1, SIDE), lax.rem(x + SIDE - 1, SIDE), lax.rem(x + 2, SIDE)
    greet([(fs, right), (fs, left), (fs, other)])
    half = block.shape[0] // 2
    parts = [pl.ds(0, half), pl.ds(half, half)]
    go_right = [put(block.at[parts[h]], out.at[x, core, parts[h]], send.at[h], recv.at[h], fs, right) for h in (0, 1)]
    go_left = [put(block.at[parts[1 - h]], out.at[x, core, parts[1 - h]], send.at[2 + h], recv.at[2 + h], fs, left) for h in (0, 1)]
    for h in (0, 1):
        go_right[h].start()
        go_left[h].start()
    keep = pltpu.make_async_copy(block, out.at[x, core], own_sem)
    keep.start()
    put(block, out.at[x, core], pair_send, pair_recv, fs, other).start()
    go_right[0].wait_recv()
    first = out.at[back, core, parts[0]]
    relay_right = put(first, first, send.at[4], recv.at[4], fs, right)
    relay_right.start()
    go_left[0].wait_recv()
    second = out.at[ahead, core, parts[1]]
    relay_left = put(second, second, send.at[5], recv.at[5], fs, left)
    relay_left.start()
    go_right[1].wait_recv()
    put(out.at[back, core], out.at[back, core], pair_send, pair_recv, fs, other).start()
    go_left[1].wait_recv()
    put(out.at[ahead, core], out.at[ahead, core], pair_send, pair_recv, fs, other).start()
    relay_right.wait_recv()
    relay_left.wait_recv()
    put(out.at[across, core], out.at[across, core], pair_send, pair_recv, fs, other).start()
    for c in go_right + go_left + [relay_right, relay_left]:
        c.wait_send()
    keep.wait()
    whole = put(out.at[:, core], out.at[:, 1 - core], pair_send, pair_recv, fs, other)
    whole.wait_send()
    whole.wait_recv()


def spread(block, cid):
    rows, cols = block.shape
    return pl.pallas_call(
        spread_kernel,
        out_shape=jax.ShapeDtypeStruct((SIDE, 2, rows, cols), jnp.float32),
        in_specs=[pl.BlockSpec(memory_space=pltpu.VMEM)],
        out_specs=pl.BlockSpec(memory_space=pltpu.VMEM),
        scratch_shapes=[
            pltpu.SemaphoreType.DMA((6,)),
            pltpu.SemaphoreType.DMA((6,)),
            pltpu.SemaphoreType.DMA,
            pltpu.SemaphoreType.DMA,
            pltpu.SemaphoreType.DMA,
        ],
        compiler_params=pltpu.CompilerParams(collective_id=cid, has_side_effects=True, vmem_limit_bytes=32 << 20),
        name="spread",
    )(block)


def split(value):
    top = value.astype(jnp.bfloat16)
    return top, (value - top.astype(jnp.float32)).astype(jnp.bfloat16)


def unturn(src, scale, high, low):
    @pl.loop(0, PLANE)
    def _(i):
        rows = pl.ds(pl.multiple_of(i * LANE, LANE), LANE)
        for b in range(TURN):
            cols = pl.ds(pl.multiple_of(LANE * lax.rem(i + b, PLANE), LANE), LANE)
            value = src[rows, pl.ds(LANE * b, LANE)] * scale
            high[rows, cols], low[rows, cols] = split(value)
            if 0 < b < TURN - 1:
                high[cols, rows], low[cols, rows] = split(value.T)


def times(src, dst, pair, high, low):
    rows, size = src.shape
    pair[:rows, :], pair[rows:, :] = split(src[...])
    width = 1024

    @pl.loop(0, size // width)
    def _(j):
        cols = pl.ds(pl.multiple_of(j * width, width), width)
        main = jnp.dot(pair[...], high[:, cols], preferred_element_type=jnp.float32)
        rest = jnp.dot(pair[...], low[:, cols], preferred_element_type=jnp.float32)
        dst[:, cols] = main[:rows] + (main[rows:] + (rest[:rows] + rest[rows:]))


def first_chain_kernel(whole, own, next_rows, coef_rows, high, low, pair, v, p, w):
    def diag(i, total):
        block = whole[pl.ds(pl.multiple_of(i * LANE, LANE), LANE), pl.ds(0, LANE)]
        eye = lax.broadcasted_iota(jnp.int32, block.shape, 0) == lax.broadcasted_iota(jnp.int32, block.shape, 1)
        return total + jnp.where(eye, block, 0.0)

    acc = lax.fori_loop(0, PLANE, diag, jnp.zeros((LANE, LANE), jnp.float32))
    ssq = jnp.sum(jnp.sum(acc, axis=0, keepdims=True), axis=1, keepdims=True)
    s = 0.5 * lax.rsqrt(jnp.maximum(ssq / D, 1.0))
    unturn(whole, s * s, high, low)
    fs, tp = lax.axis_index("fs"), lax.axis_index("tp")
    start = 128 * fs + 64 * lax.rem(tp, 2)
    shape = own.shape
    on_diag = lax.broadcasted_iota(jnp.int32, shape, 1) == start + lax.broadcasted_iota(jnp.int32, shape, 0)
    v[...] = own[...] * (s * s)
    times(v, p, pair, high, low)
    coef_rows[...] = s * (jnp.where(on_diag, A_COEF, 0.0) + B_COEF * v[...] + C_COEF * p[...])
    times(p, w, pair, high, low)
    w[...] = A_COEF * v[...] + B_COEF * p[...] + C_COEF * w[...]
    times(w, v, pair, high, low)
    times(v, p, pair, high, low)
    w[...] = A_COEF * w[...] + B_COEF * v[...] + C_COEF * p[...]
    turned(w, next_rows)


def second_chain_kernel(whole, coef, out, high, low, pair, base, v, p, q):
    unturn(whole, 1.0, high, low)

    def by_a1(src, dst):
        times(src, p, pair, high, low)
        times(p, q, pair, high, low)
        dst[...] = A_COEF * src[...] + B_COEF * p[...] + C_COEF * q[...]

    by_a1(coef, base)
    v[...] = base[...]
    out[...] = A_COEF * base[...]

    @pl.loop(0, 2)
    def _(power):
        times(v, q, pair, high, low)
        v[...] = q[...]

        @pl.loop(0, 2)
        def _(_):
            by_a1(v, v)

        out[...] += jnp.where(power == 0, B_COEF, C_COEF) * v[...]


def chain_call(kernel, whole, own, widths, works, name):
    rows, cols = own.shape
    size = whole.shape[0]
    f32, bf16 = jnp.float32, jnp.bfloat16
    vmem = pl.BlockSpec(memory_space=pltpu.VMEM)
    return pl.pallas_call(
        kernel,
        out_shape=[jax.ShapeDtypeStruct((rows, width), f32) for width in widths],
        in_specs=[vmem, vmem],
        out_specs=[vmem] * len(widths),
        scratch_shapes=[
            pltpu.VMEM((size, cols), bf16),
            pltpu.VMEM((size, cols), bf16),
            pltpu.VMEM((2 * rows, cols), bf16),
        ]
        + [pltpu.VMEM((rows, cols), f32)] * works,
        compiler_params=pltpu.CompilerParams(vmem_limit_bytes=36 << 20),
        name=name,
    )(whole, own)


def only(lanes_low, x):
    lane = lax.broadcasted_iota(jnp.int32, x.shape, x.ndim - 1)
    return jnp.where((lane < ODD) == lanes_low, x, 0.0)


def local(weights_in, weights_mix, momentum_in, momentum_mix, grads_in, grads_mix):
    moment_in = MOMENTUM_DECAY * momentum_in + grads_in
    moment_mix = MOMENTUM_DECAY * momentum_mix + grads_mix
    first, second = moment_in[0], moment_in[1]
    packed = jnp.concatenate(
        [first[:, :WIDE], second[:, :WIDE], first[:, WIDE:], second[:, WIDE:], moment_mix], axis=1
    )
    cols = plane_gather(packed, False, 0).reshape(D, PACKED)
    spans = [slice(0, WIDE), slice(WIDE, 2 * WIDE), slice(2 * WIDE, 2 * WIDE + 2 * ODD), slice(2 * WIDE + 2 * ODD, PACKED)]
    a0, a1, odd, mix = (cols[:, s] for s in spans)
    r0, r1, rodd, rmix = (packed[:, s] for s in spans)
    dot_t = functools.partial(lax.dot_general, dimension_numbers=(((1,), (1,)), ((), ())), precision=HIGH)
    part = jnp.stack(
        [
            dot_t(r0, a0) + dot_t(only(True, rodd), odd),
            dot_t(r1, a1) + dot_t(only(False, rodd), odd),
            dot_t(rmix, mix),
        ]
    ).reshape(3, 2, 64, D)
    own, sent = reduce_to_planes(part, 1)
    gram = plane_gather(sent, True, 2).reshape(D, TURN * LANE)
    sent, coef = chain_call(first_chain_kernel, gram, own, (TURN * LANE, D), 3, "first_chain")
    gram = plane_gather(sent, True, 3).reshape(D, TURN * LANE)
    (poly,) = chain_call(second_chain_kernel, gram, coef, (D,), 4, "second_chain")
    polys = spread(poly, 4).reshape(SIDE, 128, D)
    dot = functools.partial(jnp.dot, precision=HIGH)
    odds = dot(polys[:2].reshape(256, D), odd)
    y0 = jnp.concatenate([dot(polys[0], a0), odds[:128, :ODD]], axis=1)
    y1 = jnp.concatenate([dot(polys[1], a1), odds[128:, ODD:]], axis=1)
    step_in = jnp.stack([y0, y1]) * math.sqrt(max(D, FF))
    step_mix = dot(polys[2], mix) * math.sqrt(D)
    return (
        moment_in,
        moment_mix,
        weights_in - STEP_RATE * step_in,
        weights_mix - STEP_RATE * step_mix,
        step_in,
        step_mix,
    )


def solution(mesh):
    specs = (
        P(None, "fs", "tp"),
        P("fs", "tp"),
        P(None, "fs", "tp"),
        P("fs", "tp"),
        P(None, "fs", "tp"),
        P("fs", "tp"),
    )
    return jax.shard_map(local, mesh=mesh, in_specs=specs, out_specs=specs, check_vma=False)
```

```python
import functools
import math

import jax
import jax.numpy as jnp
from jax import lax
from jax.experimental import pallas as pl
from jax.experimental.pallas import tpu as pltpu
from jax.sharding import PartitionSpec as P

D = 2048
FF = 5632
ITERS = 3

A_COEF = 3.4445
B_COEF = -4.775
C_COEF = 2.0315
MOMENTUM_DECAY = 0.95
STEP_RATE = 0.02
HIGH = lax.Precision.HIGH
MESH = pl.DeviceIdType.MESH

SIDE = 4
PLANE = SIDE * SIDE
LANE = 128
TURN = PLANE // 2 + 1
WIDE = 640
ODD = 64
MIX = 256
PACKED = 2 * WIDE + 2 * ODD + MIX
WAYS = (1, -1)
FAR = (-1, 1, 2)
CUT = 768
EARLY = ((-1, 0, PACKED), (1, 0, CUT))
LATE = ((2, 0, PACKED), (1, CUT, PACKED - CUT))


def put(src, dst, send, recv, fs, tp):
    return pltpu.make_async_remote_copy(
        src_ref=src, dst_ref=dst, send_sem=send, recv_sem=recv, device_id=(fs, tp), device_id_type=MESH
    )


def greet(peers):
    barrier = pltpu.get_barrier_semaphore()
    for fs, tp in peers:
        pl.semaphore_signal(barrier, inc=1, device_id=(fs, tp), device_id_type=MESH)
    pl.semaphore_wait(barrier, len(peers))


def plane_gather_kernel(paired, block, out, send, recv, own_sem, pair_send, pair_recv):
    fs, tp = lax.axis_index("fs"), lax.axis_index("tp")
    z, y = fs // SIDE, lax.rem(fs, SIDE)
    core = lax.rem(tp, 2)
    other = tp + 1 - 2 * core
    half = block.shape[0] // 2
    quarter = half // 2
    ways = (1, -1)

    def at(along_y, along_z):
        return SIDE * lax.rem(z + along_z + SIDE, SIDE) + lax.rem(y + along_y + SIDE, SIDE)

    def near(h, first, second):
        return at(first, second) if h == 0 else at(second, first)

    peers = [(near(0, w, 0), tp) for w in ways] + [(near(1, w, 0), tp) for w in ways]
    if paired:
        peers.append((fs, other))
    greet(peers)

    def slot(origin, rows):
        return out.at[origin, core, rows] if paired else out.at[origin, rows]

    count = iter(range(40))
    started = []

    def move(origin, rows, target, src=None):
        lane = next(count)
        dst = slot(origin, rows)
        copy = put(dst if src is None else src, dst, send.at[lane], recv.at[lane], target, tp)
        copy.start()
        started.append(copy)
        return copy

    def halves(h):
        return pl.ds(h * half, half)

    def quarters(h, i):
        return pl.ds(h * half + i * quarter, quarter)

    def to_pair(origin, rows):
        if paired:
            put(slot(origin, rows), slot(origin, rows), pair_send, pair_recv, fs, other).start()

    direct = {(h, i): move(fs, halves(h), near(h, w, 0), block.at[halves(h)]) for i, w in enumerate(ways) for h in (0, 1)}
    second = {(h, i, 0): move(fs, halves(h), near(h, 0, w), block.at[halves(h)]) for i, w in enumerate(ways) for h in (0, 1)}
    mine = out.at[fs, core] if paired else out.at[fs]
    keep = pltpu.make_async_copy(block, mine, own_sem)
    keep.start()
    if paired:
        put(block, mine, pair_send, pair_recv, fs, other).start()
    relay = {}
    for i, w in enumerate(ways):
        for h in (0, 1):
            direct[h, i].wait_recv()
            origin = near(h, -w, 0)
            relay[h, i] = move(origin, quarters(h, i), near(h, w, 0))
            for j, w2 in enumerate(ways):
                second[h, j, -w] = move(origin, halves(h), near(h, 0, w2))
            to_pair(origin, halves(h))
    for h in (0, 1):
        for i in (0, 1):
            relay[h, i].wait_recv()
        origin = near(h, 2, 0)
        for j, w2 in enumerate(ways):
            second[h, j, 2] = move(origin, halves(h), near(h, 0, w2))
        to_pair(origin, halves(h))
    tail = []
    for e in (0, -1, 1, 2):
        for j, w2 in enumerate(ways):
            for h in (0, 1):
                second[h, j, e].wait_recv()
                origin = near(h, e, -w2)
                tail.append((h, j, e, move(origin, quarters(h, j), near(h, 0, w2))))
                to_pair(origin, halves(h))
    for h, j, e, copy in tail:
        copy.wait_recv()
        to_pair(near(h, e, 2), quarters(h, j))
    for copy in started:
        copy.wait_send()
    keep.wait()
    if paired:
        sent = put(out.at[:, core], out.at[:, 1 - core], pair_send, pair_recv, fs, other)
        sent.wait_send()
        sent.wait_recv()


def plane_gather(block, paired, cid):
    rows, cols = block.shape
    shape = (PLANE, 2, rows, cols) if paired else (PLANE, rows, cols)
    return pl.pallas_call(
        functools.partial(plane_gather_kernel, paired),
        out_shape=jax.ShapeDtypeStruct(shape, jnp.float32),
        in_specs=[pl.BlockSpec(memory_space=pltpu.VMEM)],
        out_specs=pl.BlockSpec(memory_space=pltpu.VMEM),
        scratch_shapes=[
            pltpu.SemaphoreType.DMA((40,)),
            pltpu.SemaphoreType.DMA((40,)),
            pltpu.SemaphoreType.DMA,
            pltpu.SemaphoreType.DMA,
            pltpu.SemaphoreType.DMA,
        ],
        compiler_params=pltpu.CompilerParams(collective_id=cid, has_side_effects=True, vmem_limit_bytes=24 << 20),
        name=f"plane_gather_{cid}",
    )(block)


def places():
    fs, tp = lax.axis_index("fs"), lax.axis_index("tp")
    return fs, tp, fs // SIDE, lax.rem(fs, SIDE), tp // 2, lax.rem(tp, 2)


def plane_at(z, y, along_z, along_y):
    return SIDE * lax.rem(z + along_z + SIDE, SIDE) + lax.rem(y + along_y + SIDE, SIDE)


def cross_kernel(block, row_y, col_z, send, recv, own):
    fs, tp, z, y, x, core = places()
    near = [[plane_at(z, y, 0, w) for w in WAYS], [plane_at(z, y, w, 0) for w in WAYS]]
    greet([(n, tp) for side in near for n in side])
    outs, here = (row_y, col_z), (y, z)
    half = block.shape[0] // 2
    lane = iter(range(8))

    def move(src, dst, target):
        i = next(lane)
        copy = put(src, dst, send.at[i], recv.at[i], target, tp)
        copy.start()
        return copy

    direct = {(i, d): move(block, outs[d].at[here[d]], near[d][i]) for i in (0, 1) for d in (0, 1)}
    keeps = [pltpu.make_async_copy(block, outs[d].at[here[d]], own.at[d]) for d in (0, 1)]
    for keep in keeps:
        keep.start()
    relays = []
    for i, w in enumerate(WAYS):
        for d in (0, 1):
            direct[i, d].wait_recv()
            part = outs[d].at[lax.rem(here[d] - w + SIDE, SIDE), pl.ds(half * i, half)]
            relays.append(move(part, part, near[d][i]))
    for copy in relays:
        copy.wait()
    for copy in direct.values():
        copy.wait_send()
    for keep in keeps:
        keep.wait()


def cross_gather(block, cid):
    rows, cols = block.shape
    vmem = pl.BlockSpec(memory_space=pltpu.VMEM)
    return pl.pallas_call(
        cross_kernel,
        out_shape=[jax.ShapeDtypeStruct((SIDE, rows, cols), jnp.float32)] * 2,
        in_specs=[vmem],
        out_specs=[vmem] * 2,
        scratch_shapes=[pltpu.SemaphoreType.DMA((8,)), pltpu.SemaphoreType.DMA((8,)), pltpu.SemaphoreType.DMA((2,))],
        compiler_params=pltpu.CompilerParams(collective_id=cid, has_side_effects=True, vmem_limit_bytes=16 << 20),
        name="cross_gather",
    )(block)


class Rest:
    def __init__(self, row_y, col_z, spans, slot, send, recv):
        fs, tp, z, y, x, core = places()
        self.tp, self.spans, self.slot, self.send, self.recv = tp, spans, slot, send, recv
        self.sources, self.here = (row_y, col_z), (y, z)
        self.half = row_y.shape[1] // 2
        self.near = [[plane_at(z, y, w, 0) for w in WAYS], [plane_at(z, y, 0, w) for w in WAYS]]
        self.peers = [(n, tp) for side in self.near for n in side]
        self.count = 0
        self.started = []

    def move(self, src, dst, target):
        i = self.count
        self.count += 1
        copy = put(src, dst, self.send.at[i], self.recv.at[i], target, self.tp)
        copy.start()
        self.started.append(copy)
        return copy

    def start(self):
        self.direct = {}
        for s, (e, col, width) in enumerate(self.spans):
            for i, w in enumerate(WAYS):
                for h in (0, 1):
                    rows = pl.ds(h * self.half, self.half)
                    block = lax.rem(self.here[h] + e + SIDE, SIDE)
                    src = self.sources[h].at[block, rows, pl.ds(col, width)]
                    self.direct[s, i, h] = self.move(src, self.slot(h, s, e, -w, w, 0, self.half), self.near[h][i])

    def relay(self, s):
        e = self.spans[s][0]
        part = self.half // 2
        for i, w in enumerate(WAYS):
            for h in (0, 1):
                self.direct[s, i, h].wait_recv()
                src = self.slot(h, s, e, -w, 0, part * i, part)
                self.direct[s, i, h, 2] = self.move(src, self.slot(h, s, e, 2, w, part * i, part), self.near[h][i])

    def finish(self):
        for key, copy in self.direct.items():
            if len(key) == 4:
                copy.wait_recv()
        for copy in self.started:
            copy.wait_send()


def reduce_kernel(part, row_y, col_z, out, rest_a, rest_b, pair, total, near, far, hold, send, recv, rest_send, rest_recv):
    fs, tp, z, y, x, core = places()
    right = 2 * lax.rem(x + 1, SIDE) + core
    left = 2 * lax.rem(x + SIDE - 1, SIDE) + core
    other = tp + 1 - 2 * core

    def slot(h, s, e, f, to, row, rows):
        return (rest_a, rest_b)[s].at[h, FAR.index(f), pl.ds(row, rows)]

    rest = Rest(row_y, col_z, EARLY, slot, rest_send, rest_recv)
    greet([(fs, right), (fs, left), (fs, other)] + rest.peers)
    copies = [put(part.at[m, :, 1 - core], pair.at[m], send.at[m], recv.at[m], fs, other) for m in range(3)]
    for c in copies:
        c.start()
    rest.start()
    for m, c in enumerate(copies):
        c.wait()
        total[m] = part[m, :, core] + pair[m]
    total[3] = jnp.zeros_like(total[3])
    half = total.shape[1] // 2
    up, down = pl.ds(0, half), pl.ds(half, half)
    ahead, back, across = lax.rem(x + 1, SIDE), lax.rem(x + SIDE - 1, SIDE), lax.rem(x + 2, SIDE)
    far_right = put(total.at[across, up], far.at[0], send.at[3], recv.at[3], fs, right)
    far_left = put(total.at[across, down], far.at[1], send.at[4], recv.at[4], fs, left)
    near_right = put(total.at[ahead, down], near.at[0], send.at[5], recv.at[5], fs, right)
    near_left = put(total.at[back, up], near.at[1], send.at[6], recv.at[6], fs, left)
    for c in (far_right, far_left, near_right, near_left):
        c.start()
    far_right.wait_recv()
    hold[0] = far[0] + total[ahead, up]
    on_right = put(hold.at[0], near.at[2], send.at[7], recv.at[7], fs, right)
    on_right.start()
    far_left.wait_recv()
    hold[1] = far[1] + total[back, down]
    on_left = put(hold.at[1], near.at[3], send.at[8], recv.at[8], fs, left)
    on_left.start()
    rest.relay(0)
    near_right.wait_recv()
    near_left.wait_recv()
    on_right.wait_recv()
    on_left.wait_recv()
    hold_up, hold_down = pair.at[0, up], pair.at[0, down]
    hold_up[...] = total[x, up] + near[2] + near[1]
    hold_down[...] = total[x, down] + near[3] + near[0]
    for b in range(TURN):
        chip = lax.rem(fs + b, PLANE)
        col = pl.multiple_of(LANE * (chip // SIDE), LANE)
        out[:, pl.ds(LANE * b, LANE)] = pair[0, lax.rem(chip, SIDE), :, pl.ds(col, LANE)]
    for s in range(1, len(EARLY)):
        rest.relay(s)
    for c in (far_right, far_left, near_right, near_left, on_right, on_left):
        c.wait_send()
    rest.finish()


def reduce_to_planes(part, row_y, col_z, cid):
    f32 = jnp.float32
    shape = (part.shape[1],) + part.shape[3:]
    half = (shape[0] // 2,) + shape[1:]
    rows = row_y.shape[1] // 2
    vmem = pl.BlockSpec(memory_space=pltpu.VMEM)
    lanes = 8 * len(EARLY)
    return pl.pallas_call(
        reduce_kernel,
        out_shape=[jax.ShapeDtypeStruct((shape[1], TURN * LANE), f32)]
        + [jax.ShapeDtypeStruct((2, len(FAR), rows, width), f32) for _, _, width in EARLY],
        in_specs=[vmem] * 3,
        out_specs=[vmem] * 3,
        scratch_shapes=[
            pltpu.VMEM((3,) + shape, f32),
            pltpu.VMEM((4,) + shape, f32),
            pltpu.VMEM((4,) + half, f32),
            pltpu.VMEM((2,) + half, f32),
            pltpu.VMEM((2,) + half, f32),
            pltpu.SemaphoreType.DMA((9,)),
            pltpu.SemaphoreType.DMA((9,)),
            pltpu.SemaphoreType.DMA((lanes,)),
            pltpu.SemaphoreType.DMA((lanes,)),
        ],
        compiler_params=pltpu.CompilerParams(collective_id=cid, has_side_effects=True, vmem_limit_bytes=32 << 20),
        name="reduce_to_planes",
    )(part, row_y, col_z)


def spread_kernel(block, row_y, col_z, rest_a, rest_b, out, full, send, recv, own, pair_send, pair_recv, rest_send, rest_recv):
    fs, tp, z, y, x, core = places()
    right = 2 * lax.rem(x + 1, SIDE) + core
    left = 2 * lax.rem(x + SIDE - 1, SIDE) + core
    other = tp + 1 - 2 * core
    ahead, back, across = lax.rem(x + 1, SIDE), lax.rem(x + SIDE - 1, SIDE), lax.rem(x + 2, SIDE)

    def origin(h, e, f):
        return plane_at(z, y, f, e) if h == 0 else plane_at(z, y, e, f)

    def slot(h, s, e, f, to, row, rows):
        _, col, width = LATE[s]
        return full.at[origin(h, e, f + to), pl.ds(h * rest.half + row, rows), pl.ds(col, width)]

    rest = Rest(row_y, col_z, LATE, slot, rest_send, rest_recv)
    greet([(fs, right), (fs, left), (fs, other)] + rest.peers)
    half = block.shape[0] // 2
    parts = [pl.ds(0, half), pl.ds(half, half)]
    go_right = [put(block.at[parts[h]], out.at[x, core, parts[h]], send.at[h], recv.at[h], fs, right) for h in (0, 1)]
    go_left = [put(block.at[parts[1 - h]], out.at[x, core, parts[1 - h]], send.at[2 + h], recv.at[2 + h], fs, left) for h in (0, 1)]
    for h in (0, 1):
        go_right[h].start()
        go_left[h].start()
    rest.start()
    moves = [(block, out.at[x, core])]
    moves += [(row_y.at[lax.rem(y + e + SIDE, SIDE)], full.at[plane_at(z, y, 0, e)]) for e in (0,) + FAR]
    moves += [(col_z.at[lax.rem(z + e + SIDE, SIDE)], full.at[plane_at(z, y, e, 0)]) for e in FAR]
    for buf, (e, col, width) in zip((rest_a, rest_b), EARLY):
        for h in (0, 1):
            for i, f in enumerate(FAR):
                dst = full.at[origin(h, e, f), pl.ds(h * rest.half, rest.half), pl.ds(col, width)]
                moves.append((buf.at[h, i], dst))
    keeps = [pltpu.make_async_copy(src, dst, own.at[i]) for i, (src, dst) in enumerate(moves)]
    for keep in keeps:
        keep.start()
    put(block, out.at[x, core], pair_send, pair_recv, fs, other).start()
    go_right[0].wait_recv()
    first = out.at[back, core, parts[0]]
    relay_right = put(first, first, send.at[4], recv.at[4], fs, right)
    relay_right.start()
    go_left[0].wait_recv()
    second = out.at[ahead, core, parts[1]]
    relay_left = put(second, second, send.at[5], recv.at[5], fs, left)
    relay_left.start()
    rest.relay(0)
    go_right[1].wait_recv()
    put(out.at[back, core], out.at[back, core], pair_send, pair_recv, fs, other).start()
    go_left[1].wait_recv()
    put(out.at[ahead, core], out.at[ahead, core], pair_send, pair_recv, fs, other).start()
    for s in range(1, len(LATE)):
        rest.relay(s)
    relay_right.wait_recv()
    relay_left.wait_recv()
    put(out.at[across, core], out.at[across, core], pair_send, pair_recv, fs, other).start()
    for c in go_right + go_left + [relay_right, relay_left]:
        c.wait_send()
    for keep in keeps:
        keep.wait()
    rest.finish()
    whole = put(out.at[:, core], out.at[:, 1 - core], pair_send, pair_recv, fs, other)
    whole.wait_send()
    whole.wait_recv()


def spread(block, row_y, col_z, rest_a, rest_b, cid):
    rows, cols = block.shape
    vmem = pl.BlockSpec(memory_space=pltpu.VMEM)
    lanes = 8 * len(LATE)
    return pl.pallas_call(
        spread_kernel,
        out_shape=[
            jax.ShapeDtypeStruct((SIDE, 2, rows, cols), jnp.float32),
            jax.ShapeDtypeStruct((PLANE,) + row_y.shape[1:], jnp.float32),
        ],
        in_specs=[vmem] * 5,
        out_specs=[vmem] * 2,
        scratch_shapes=[
            pltpu.SemaphoreType.DMA((6,)),
            pltpu.SemaphoreType.DMA((6,)),
            pltpu.SemaphoreType.DMA((8 + 12,)),
            pltpu.SemaphoreType.DMA,
            pltpu.SemaphoreType.DMA,
            pltpu.SemaphoreType.DMA((lanes,)),
            pltpu.SemaphoreType.DMA((lanes,)),
        ],
        compiler_params=pltpu.CompilerParams(collective_id=cid, has_side_effects=True, vmem_limit_bytes=44 << 20),
        name="spread",
    )(block, row_y, col_z, rest_a, rest_b)


def turned(rows, dst):
    fs = lax.axis_index("fs")
    for b in range(TURN):
        col = pl.multiple_of(LANE * lax.rem(fs + b, PLANE), LANE)
        dst[:, pl.ds(LANE * b, LANE)] = rows[:, pl.ds(col, LANE)]


def split(value):
    top = value.astype(jnp.bfloat16)
    return top, (value - top.astype(jnp.float32)).astype(jnp.bfloat16)


def unturn(src, scale, high, low, crossed):
    @pl.loop(0, PLANE)
    def _(i):
        sent = pl.ds(pl.multiple_of(i * LANE, LANE), LANE)
        for b in range(TURN):
            j = lax.rem(i + b, PLANE)
            row, col = i, j
            if crossed:
                row = i - lax.rem(i, SIDE) + lax.rem(j, SIDE)
                col = j - lax.rem(j, SIDE) + lax.rem(i, SIDE)
            rows = pl.ds(pl.multiple_of(LANE * row, LANE), LANE)
            cols = pl.ds(pl.multiple_of(LANE * col, LANE), LANE)
            value = src[sent, pl.ds(LANE * b, LANE)] * scale
            high[rows, cols], low[rows, cols] = split(value)
            if 0 < b < TURN - 1:
                high[cols, rows], low[cols, rows] = split(value.T)


def times(src, dst, pair, high, low):
    rows, size = src.shape
    pair[:rows, :], pair[rows:, :] = split(src[...])
    width = 1024

    @pl.loop(0, size // width)
    def _(j):
        cols = pl.ds(pl.multiple_of(j * width, width), width)
        main = jnp.dot(pair[...], high[:, cols], preferred_element_type=jnp.float32)
        rest = jnp.dot(pair[...], low[:, cols], preferred_element_type=jnp.float32)
        dst[:, cols] = main[:rows] + (main[rows:] + (rest[:rows] + rest[rows:]))


def first_chain_kernel(whole, next_rows, coef_rows, high, low, pair, v, p, w):
    def diag(i, total):
        block = whole[pl.ds(pl.multiple_of(i * LANE, LANE), LANE), pl.ds(0, LANE)]
        eye = lax.broadcasted_iota(jnp.int32, block.shape, 0) == lax.broadcasted_iota(jnp.int32, block.shape, 1)
        return total + jnp.where(eye, block, 0.0)

    acc = lax.fori_loop(0, PLANE, diag, jnp.zeros((LANE, LANE), jnp.float32))
    ssq = jnp.sum(jnp.sum(acc, axis=0, keepdims=True), axis=1, keepdims=True)
    s = 0.5 * lax.rsqrt(jnp.maximum(ssq / D, 1.0))
    unturn(whole, s * s, high, low, True)
    fs, tp = lax.axis_index("fs"), lax.axis_index("tp")
    shape = v.shape
    start = pl.multiple_of(128 * fs + 64 * lax.rem(tp, 2), 64)
    on_diag = lax.broadcasted_iota(jnp.int32, shape, 1) == start + lax.broadcasted_iota(jnp.int32, shape, 0)
    mine = pl.ds(start, shape[0])
    v[...] = high[mine, :].astype(jnp.float32) + low[mine, :].astype(jnp.float32)
    times(v, p, pair, high, low)
    coef_rows[...] = s * (jnp.where(on_diag, A_COEF, 0.0) + B_COEF * v[...] + C_COEF * p[...])
    times(p, w, pair, high, low)
    w[...] = A_COEF * v[...] + B_COEF * p[...] + C_COEF * w[...]
    times(w, v, pair, high, low)
    times(v, p, pair, high, low)
    w[...] = A_COEF * w[...] + B_COEF * v[...] + C_COEF * p[...]
    turned(w, next_rows)


def second_chain_kernel(whole, coef, out, high, low, pair, base, v, p, q):
    unturn(whole, 1.0, high, low, False)

    def by_a1(src, dst):
        times(src, p, pair, high, low)
        times(p, q, pair, high, low)
        dst[...] = A_COEF * src[...] + B_COEF * p[...] + C_COEF * q[...]

    by_a1(coef, base)
    v[...] = base[...]
    out[...] = A_COEF * base[...]

    @pl.loop(0, 2)
    def _(power):
        times(v, q, pair, high, low)
        v[...] = q[...]

        @pl.loop(0, 2)
        def _(_):
            by_a1(v, v)

        out[...] += jnp.where(power == 0, B_COEF, C_COEF) * v[...]


def chain_call(kernel, args, widths, works, name):
    size, rows = D, 64
    f32, bf16 = jnp.float32, jnp.bfloat16
    vmem = pl.BlockSpec(memory_space=pltpu.VMEM)
    return pl.pallas_call(
        kernel,
        out_shape=[jax.ShapeDtypeStruct((rows, width), f32) for width in widths],
        in_specs=[vmem] * len(args),
        out_specs=[vmem] * len(widths),
        scratch_shapes=[pltpu.VMEM((size, size), bf16)] * 2
        + [pltpu.VMEM((2 * rows, size), bf16)]
        + [pltpu.VMEM((rows, size), f32)] * works,
        compiler_params=pltpu.CompilerParams(vmem_limit_bytes=36 << 20),
        name=name,
    )(*args)


def only(lanes_low, x):
    lane = lax.broadcasted_iota(jnp.int32, x.shape, x.ndim - 1)
    return jnp.where((lane < ODD) == lanes_low, x, 0.0)


def local(weights_in, weights_mix, momentum_in, momentum_mix, grads_in, grads_mix):
    moment_in = MOMENTUM_DECAY * momentum_in + grads_in
    moment_mix = MOMENTUM_DECAY * momentum_mix + grads_mix
    first, second = moment_in[0], moment_in[1]
    packed = jnp.concatenate(
        [first[:, :WIDE], second[:, :WIDE], first[:, WIDE:], second[:, WIDE:], moment_mix], axis=1
    )
    row_y, col_z = cross_gather(packed, 0)
    spans = [slice(0, WIDE), slice(WIDE, 2 * WIDE), slice(2 * WIDE, 2 * WIDE + 2 * ODD), slice(2 * WIDE + 2 * ODD, PACKED)]
    l0, l1, lodd, lmix = (row_y.reshape(-1, PACKED)[:, s] for s in spans)
    r0, r1, rodd, rmix = (col_z.reshape(-1, PACKED)[:, s] for s in spans)
    dot_t = functools.partial(lax.dot_general, dimension_numbers=(((1,), (1,)), ((), ())), precision=HIGH)
    part = jnp.stack(
        [
            dot_t(l0, r0) + dot_t(only(True, lodd), rodd),
            dot_t(l1, r1) + dot_t(only(False, lodd), rodd),
            dot_t(lmix, rmix),
        ]
    ).reshape(3, SIDE, 2, 64, SIDE * LANE)
    sent, rest_a, rest_b = reduce_to_planes(part, row_y, col_z, 1)
    gram = plane_gather(sent, True, 2).reshape(D, TURN * LANE)
    sent, coef = chain_call(first_chain_kernel, (gram,), (TURN * LANE, D), 3, "first_chain")
    gram = plane_gather(sent, True, 3).reshape(D, TURN * LANE)
    (poly,) = chain_call(second_chain_kernel, (gram, coef), (D,), 4, "second_chain")
    polys, cols = spread(poly, row_y, col_z, rest_a, rest_b, 4)
    polys = polys.reshape(SIDE, 128, D)
    a0, a1, odd, mix = (cols.reshape(D, PACKED)[:, s] for s in spans)
    dot = functools.partial(jnp.dot, precision=HIGH)
    odds = dot(polys[:2].reshape(256, D), odd)
    y0 = jnp.concatenate([dot(polys[0], a0), odds[:128, :ODD]], axis=1)
    y1 = jnp.concatenate([dot(polys[1], a1), odds[128:, ODD:]], axis=1)
    step_in = jnp.stack([y0, y1]) * math.sqrt(max(D, FF))
    step_mix = dot(polys[2], mix) * math.sqrt(D)
    return (
        moment_in,
        moment_mix,
        weights_in - STEP_RATE * step_in,
        weights_mix - STEP_RATE * step_mix,
        step_in,
        step_mix,
    )


def solution(mesh):
    specs = (
        P(None, "fs", "tp"),
        P("fs", "tp"),
        P(None, "fs", "tp"),
        P("fs", "tp"),
        P(None, "fs", "tp"),
        P("fs", "tp"),
    )
    return jax.shard_map(local, mesh=mesh, in_specs=specs, out_specs=specs, check_vma=False)
```

```python
import functools
import math

import jax
import jax.numpy as jnp
from jax import lax
from jax.experimental import pallas as pl
from jax.experimental.pallas import tpu as pltpu
from jax.sharding import PartitionSpec as P

D = 2048
FF = 5632
ITERS = 3

A_COEF = 3.4445
B_COEF = -4.775
C_COEF = 2.0315
MOMENTUM_DECAY = 0.95
STEP_RATE = 0.02
HIGH = lax.Precision.HIGH
MESH = pl.DeviceIdType.MESH
ANY = pl.BlockSpec(memory_space=pl.ANY)

SIDE = 4
PLANE = SIDE * SIDE
LANE = 128
TURN = PLANE // 2 + 1
WIDE = 640
ODD = 64
MIX = 256
FFB = WIDE + ODD
PACKED = 2 * FFB + MIX
WAYS = (1, -1)
FAR = (-1, 1, 2)
CUT = 768
EARLY = ((-1, 0, CUT),)
AMID = ((1, 0, PACKED), (2, 0, PACKED))
LATE = ((-1, CUT, PACKED - CUT),)


def put(src, dst, send, recv, fs, tp):
    return pltpu.make_async_remote_copy(
        src_ref=src, dst_ref=dst, send_sem=send, recv_sem=recv, device_id=(fs, tp), device_id_type=MESH
    )


def greet(peers):
    barrier = pltpu.get_barrier_semaphore()
    for fs, tp in peers:
        pl.semaphore_signal(barrier, inc=1, device_id=(fs, tp), device_id_type=MESH)
    pl.semaphore_wait(barrier, len(peers))


def plane_gather(block, buf, high, low, crossed, send, recv, own_sem, pair_send, pair_recv):
    fs, tp, z, y, x, core = places()
    other = tp + 1 - 2 * core
    half = block.shape[0] // 2
    quarter = half // 2

    def near(h, first, second):
        return plane_at(z, y, second, first) if h == 0 else plane_at(z, y, first, second)

    started, moves, pairs = [], iter(range(40)), {}

    def move(origin, rows, target, src=None):
        lane = next(moves)
        dst = buf.at[origin, core, rows]
        copy = put(dst if src is None else src, dst, send.at[lane], recv.at[lane], target, tp)
        copy.start()
        started.append(copy)
        return copy

    def halves(h):
        return pl.ds(h * half, half)

    def quarters(h, i):
        return pl.ds(h * half + i * quarter, quarter)

    def to_pair(along_z, along_y, src=None):
        at = buf.at[plane_at(z, y, along_z, along_y), core]
        k = len(pairs)
        copy = put(at if src is None else src, at, pair_send.at[k], pair_recv.at[k], fs, other)
        copy.start()
        pairs[along_z, along_y] = copy
        started.append(copy)

    direct = {(h, i): move(fs, halves(h), near(h, w, 0), block.at[halves(h)]) for i, w in enumerate(WAYS) for h in (0, 1)}
    second = {(h, i, 0): move(fs, halves(h), near(h, 0, w), block.at[halves(h)]) for i, w in enumerate(WAYS) for h in (0, 1)}
    keep = pltpu.make_async_copy(block, buf.at[fs, core], own_sem)
    keep.start()
    to_pair(0, 0, block)
    relay = {}
    for i, w in enumerate(WAYS):
        for h in (0, 1):
            direct[h, i].wait_recv()
            origin = near(h, -w, 0)
            relay[h, i] = move(origin, quarters(h, i), near(h, w, 0))
            for j, w2 in enumerate(WAYS):
                second[h, j, -w] = move(origin, halves(h), near(h, 0, w2))
    for h in (0, 1):
        for i in (0, 1):
            relay[h, i].wait_recv()
        origin = near(h, 2, 0)
        for j, w2 in enumerate(WAYS):
            second[h, j, 2] = move(origin, halves(h), near(h, 0, w2))
    tail = {}
    for e in (0, -1, 1, 2):
        for j, w2 in enumerate(WAYS):
            for h in (0, 1):
                second[h, j, e].wait_recv()
                tail[h, j, e] = move(near(h, e, -w2), quarters(h, j), near(h, 0, w2))
        if e == 0:
            for w in WAYS:
                to_pair(0, w)
                to_pair(w, 0)
        if e == 1:
            for w in WAYS:
                for w2 in WAYS:
                    to_pair(w, w2)

    def rebuild(i):
        sent = buf.at[i]
        for b in range(TURN):
            j = lax.rem(i + b, PLANE)
            row, col = i, j
            if crossed:
                row = SIDE * (i // SIDE) + lax.rem(j, SIDE)
                col = SIDE * (j // SIDE) + lax.rem(i, SIDE)
            rows = pl.ds(pl.multiple_of(LANE * row, LANE), LANE)
            cols = pl.ds(pl.multiple_of(LANE * col, LANE), LANE)
            value = sent[:, :, pl.ds(LANE * b, LANE)].reshape(LANE, LANE)
            high[rows, cols], low[rows, cols] = split(value)
            if 0 < b < TURN - 1:
                high[cols, rows], low[cols, rows] = split(value.T)

    keep.wait()
    for copy in pairs.values():
        copy.wait_recv()

    @pl.loop(0, 9)
    def _(n):
        rebuild(plane_at(z, y, n // 3 - 1, lax.rem(n, 3) - 1))

    for e in (0, -1, 1, 2):
        for j in (0, 1):
            for h in (0, 1):
                tail[h, j, e].wait_recv()
        to_pair(2, e)
        if e != 2:
            to_pair(e, 2)
    for e in FAR[:2] + (0,):
        pairs[e, 2].wait_recv()
        pairs[2, e].wait_recv()

    @pl.loop(0, 3)
    def _(n):
        rebuild(plane_at(z, y, n - 1, 2))

    pairs[2, 2].wait_recv()

    @pl.loop(0, 4)
    def _(n):
        rebuild(plane_at(z, y, 2, n - 1))

    for copy in started:
        copy.wait_send()


def places():
    fs, tp = lax.axis_index("fs"), lax.axis_index("tp")
    return fs, tp, fs // SIDE, lax.rem(fs, SIDE), tp // 2, lax.rem(tp, 2)


def plane_at(z, y, along_z, along_y):
    return SIDE * lax.rem(z + along_z + SIDE, SIDE) + lax.rem(y + along_y + SIDE, SIDE)


def cross_kernel(block, row_y, col_z, send, recv, own):
    fs, tp, z, y, x, core = places()
    near = [[plane_at(z, y, 0, w) for w in WAYS], [plane_at(z, y, w, 0) for w in WAYS]]
    greet([(n, tp) for side in near for n in side])
    outs, here = (row_y, col_z), (y, z)
    half = block.shape[0] // 2
    lane = iter(range(12))

    def move(src, dst, target):
        i = next(lane)
        copy = put(src, dst, send.at[i], recv.at[i], target, tp)
        copy.start()
        return copy

    parts = [pl.ds(0, half), pl.ds(half, half)]
    direct = {
        (i, d, k): move(block.at[parts[(i + k) % 2]], outs[d].at[here[d], parts[(i + k) % 2]], near[d][i])
        for k in (0, 1)
        for i in (0, 1)
        for d in (0, 1)
    }
    keeps = [pltpu.make_async_copy(block, outs[d].at[here[d]], own.at[d]) for d in (0, 1)]
    for keep in keeps:
        keep.start()
    relays = []
    for i, w in enumerate(WAYS):
        for d in (0, 1):
            direct[i, d, 0].wait_recv()
            part = outs[d].at[lax.rem(here[d] - w + SIDE, SIDE), parts[i]]
            relays.append(move(part, part, near[d][i]))
    for (i, d, k), copy in direct.items():
        copy.wait_send()
        if k == 1:
            copy.wait_recv()
    for copy in relays:
        copy.wait()
    for keep in keeps:
        keep.wait()


def cross_gather(block, cid):
    rows, cols = block.shape
    vmem = pl.BlockSpec(memory_space=pltpu.VMEM)
    return pl.pallas_call(
        cross_kernel,
        out_shape=[jax.ShapeDtypeStruct((SIDE, rows, cols), jnp.float32)] * 2,
        in_specs=[vmem],
        out_specs=[vmem] * 2,
        scratch_shapes=[pltpu.SemaphoreType.DMA((12,)), pltpu.SemaphoreType.DMA((12,)), pltpu.SemaphoreType.DMA((2,))],
        compiler_params=pltpu.CompilerParams(collective_id=cid, has_side_effects=True, vmem_limit_bytes=16 << 20),
        name="cross_gather",
    )(block)


class Rest:
    def __init__(self, row_y, col_z, spans, slot, send, recv):
        fs, tp, z, y, x, core = places()
        self.tp, self.spans, self.slot, self.send, self.recv = tp, spans, slot, send, recv
        self.sources, self.here = (row_y, col_z), (y, z)
        self.half = row_y.shape[1] // 2
        self.near = [[plane_at(z, y, w, 0) for w in WAYS], [plane_at(z, y, 0, w) for w in WAYS]]
        self.peers = [(n, tp) for side in self.near for n in side]
        self.count = 0
        self.started = []

    def move(self, src, dst, target):
        i = self.count
        self.count += 1
        copy = put(src, dst, self.send.at[i], self.recv.at[i], target, self.tp)
        copy.start()
        self.started.append(copy)
        return copy

    def start(self):
        self.direct = {}
        for s, (e, col, width) in enumerate(self.spans):
            for i, w in enumerate(WAYS):
                for h in (0, 1):
                    rows = pl.ds(h * self.half, self.half)
                    block = lax.rem(self.here[h] + e + SIDE, SIDE)
                    src = self.sources[h].at[block, rows, pl.ds(col, width)]
                    self.direct[s, i, h] = self.move(src, self.slot(h, s, e, -w, w, 0, self.half), self.near[h][i])

    def relay(self, s):
        e = self.spans[s][0]
        part = self.half // 2
        for i, w in enumerate(WAYS):
            for h in (0, 1):
                self.direct[s, i, h].wait_recv()
                src = self.slot(h, s, e, -w, 0, part * i, part)
                self.direct[s, i, h, 2] = self.move(src, self.slot(h, s, e, 2, w, part * i, part), self.near[h][i])

    def finish(self):
        for key, copy in self.direct.items():
            if len(key) == 4:
                copy.wait_recv()
        for copy in self.started:
            copy.wait_send()


def reduce_kernel(part, row_y, col_z, out, rest_a, pair, total, near, far, hold, send, recv, rest_send, rest_recv):
    fs, tp, z, y, x, core = places()
    right = 2 * lax.rem(x + 1, SIDE) + core
    left = 2 * lax.rem(x + SIDE - 1, SIDE) + core
    other = tp + 1 - 2 * core

    def slot(h, s, e, f, to, row, rows):
        return rest_a.at[h, FAR.index(f), pl.ds(row, rows)]

    rest = Rest(row_y, col_z, EARLY, slot, rest_send, rest_recv)
    greet([(fs, right), (fs, left), (fs, other)] + rest.peers)
    copies = [put(part.at[m, :, 1 - core], pair.at[m], send.at[m], recv.at[m], fs, other) for m in range(3)]
    for c in copies:
        c.start()
    rest.start()
    for m, c in enumerate(copies):
        c.wait()
        total[m] = part[m, :, core] + pair[m]
    total[3] = jnp.zeros_like(total[3])
    half = total.shape[1] // 2
    up, down = pl.ds(0, half), pl.ds(half, half)
    ahead, back, across = lax.rem(x + 1, SIDE), lax.rem(x + SIDE - 1, SIDE), lax.rem(x + 2, SIDE)
    far_right = put(total.at[across, up], far.at[0], send.at[3], recv.at[3], fs, right)
    far_left = put(total.at[across, down], far.at[1], send.at[4], recv.at[4], fs, left)
    near_right = put(total.at[ahead, down], near.at[0], send.at[5], recv.at[5], fs, right)
    near_left = put(total.at[back, up], near.at[1], send.at[6], recv.at[6], fs, left)
    for c in (far_right, far_left, near_right, near_left):
        c.start()
    far_right.wait_recv()
    hold[0] = far[0] + total[ahead, up]
    on_right = put(hold.at[0], near.at[2], send.at[7], recv.at[7], fs, right)
    on_right.start()
    far_left.wait_recv()
    hold[1] = far[1] + total[back, down]
    on_left = put(hold.at[1], near.at[3], send.at[8], recv.at[8], fs, left)
    on_left.start()
    rest.relay(0)
    near_right.wait_recv()
    near_left.wait_recv()
    on_right.wait_recv()
    on_left.wait_recv()
    hold_up, hold_down = pair.at[0, up], pair.at[0, down]
    hold_up[...] = total[x, up] + near[2] + near[1]
    hold_down[...] = total[x, down] + near[3] + near[0]
    for b in range(TURN):
        chip = lax.rem(fs + b, PLANE)
        col = pl.multiple_of(LANE * (chip // SIDE), LANE)
        out[:, pl.ds(LANE * b, LANE)] = pair[0, lax.rem(chip, SIDE), :, pl.ds(col, LANE)]
    for c in (far_right, far_left, near_right, near_left, on_right, on_left):
        c.wait_send()
    rest.finish()


def reduce_to_planes(part, row_y, col_z, cid):
    f32 = jnp.float32
    shape = (part.shape[1],) + part.shape[3:]
    half = (shape[0] // 2,) + shape[1:]
    rows = row_y.shape[1] // 2
    vmem = pl.BlockSpec(memory_space=pltpu.VMEM)
    lanes = 8 * len(EARLY)
    return pl.pallas_call(
        reduce_kernel,
        out_shape=[jax.ShapeDtypeStruct((shape[1], TURN * LANE), f32)]
        + [jax.ShapeDtypeStruct((2, len(FAR), rows, width), f32) for _, _, width in EARLY],
        in_specs=[vmem, ANY, ANY],
        out_specs=[vmem, ANY],
        scratch_shapes=[
            pltpu.VMEM((3,) + shape, f32),
            pltpu.VMEM((4,) + shape, f32),
            pltpu.VMEM((4,) + half, f32),
            pltpu.VMEM((2,) + half, f32),
            pltpu.VMEM((2,) + half, f32),
            pltpu.SemaphoreType.DMA((9,)),
            pltpu.SemaphoreType.DMA((9,)),
            pltpu.SemaphoreType.DMA((lanes,)),
            pltpu.SemaphoreType.DMA((lanes,)),
        ],
        compiler_params=pltpu.CompilerParams(collective_id=cid, has_side_effects=True, vmem_limit_bytes=32 << 20),
        name="reduce_to_planes",
    )(part, row_y, col_z)


def last_kernel(
    block, row_y, col_z, rest_a, rest_m, y_out, out, full, high, low, pair, send, recv, own, pair_send, pair_recv, rest_send, rest_recv
):
    fs, tp, z, y, x, core = places()
    right = 2 * lax.rem(x + 1, SIDE) + core
    left = 2 * lax.rem(x + SIDE - 1, SIDE) + core
    other = tp + 1 - 2 * core
    ahead, back, across = lax.rem(x + 1, SIDE), lax.rem(x + SIDE - 1, SIDE), lax.rem(x + 2, SIDE)

    def origin(h, e, f):
        return plane_at(z, y, f, e) if h == 0 else plane_at(z, y, e, f)

    def slot(h, s, e, f, to, row, rows):
        _, col, width = LATE[s]
        return full.at[origin(h, e, f + to), pl.ds(h * rest.half + row, rows), pl.ds(col, width)]

    rest = Rest(row_y, col_z, LATE, slot, rest_send, rest_recv)
    greet([(fs, right), (fs, left), (fs, other)] + rest.peers)
    half = block.shape[0] // 2
    parts = [pl.ds(0, half), pl.ds(half, half)]
    go_right = [put(block.at[parts[h]], out.at[x, core, parts[h]], send.at[h], recv.at[h], fs, right) for h in (0, 1)]
    go_left = [put(block.at[parts[1 - h]], out.at[x, core, parts[1 - h]], send.at[2 + h], recv.at[2 + h], fs, left) for h in (0, 1)]
    for h in (0, 1):
        go_right[h].start()
        go_left[h].start()
    rest.start()
    moves = [(block, out.at[x, core])]
    moves += [(row_y.at[lax.rem(y + e + SIDE, SIDE)], full.at[plane_at(z, y, 0, e)]) for e in (0,) + FAR]
    moves += [(col_z.at[lax.rem(z + e + SIDE, SIDE)], full.at[plane_at(z, y, e, 0)]) for e in FAR]
    for buf, (e, col, width) in ((rest_a, EARLY[0]), (rest_m.at[0], AMID[0]), (rest_m.at[1], AMID[1])):
        for h in (0, 1):
            for i, f in enumerate(FAR):
                dst = full.at[origin(h, e, f), pl.ds(h * rest.half, rest.half), pl.ds(col, width)]
                moves.append((buf.at[h, i], dst))
    keeps = [pltpu.make_async_copy(src, dst, own.at[i]) for i, (src, dst) in enumerate(moves)]
    for keep in keeps:
        keep.start()
    put(block, out.at[x, core], pair_send, pair_recv, fs, other).start()
    go_right[0].wait_recv()
    first = out.at[back, core, parts[0]]
    relay_right = put(first, first, send.at[4], recv.at[4], fs, right)
    relay_right.start()
    go_left[0].wait_recv()
    second = out.at[ahead, core, parts[1]]
    relay_left = put(second, second, send.at[5], recv.at[5], fs, left)
    relay_left.start()
    rest.relay(0)
    go_right[1].wait_recv()
    put(out.at[back, core], out.at[back, core], pair_send, pair_recv, fs, other).start()
    go_left[1].wait_recv()
    put(out.at[ahead, core], out.at[ahead, core], pair_send, pair_recv, fs, other).start()
    for keep in keeps:
        keep.wait()
    rest.finish()

    @pl.loop(0, PLANE)
    def _(i):
        for k in (0, 1):
            rows = pl.ds(pl.multiple_of(LANE * i + 64 * k, 64), 64)
            high[rows, :], low[rows, :] = split(full[i, pl.ds(64 * k, 64), :])

    relay_right.wait_recv()
    relay_left.wait_recv()
    put(out.at[across, core], out.at[across, core], pair_send, pair_recv, fs, other).start()
    for c in go_right + go_left + [relay_right, relay_left]:
        c.wait_send()
    whole = put(out.at[:, core], out.at[:, 1 - core], pair_send, pair_recv, fs, other)
    whole.wait_send()
    whole.wait_recv()
    for m, (start, tiles) in enumerate(((0, 3), (WIDE, 3), (2 * FFB, 1))):
        for c in (0, 1):
            pair[pl.ds(64 * c, 64), :], pair[pl.ds(LANE + 64 * c, 64), :] = split(out[m, c])
        scale = math.sqrt(D) if m == 2 else math.sqrt(max(D, FF))
        for t in range(tiles):
            cols = pl.ds(start + 256 * t, 256)
            main = jnp.dot(pair[...], high[:, cols], preferred_element_type=jnp.float32)
            side = jnp.dot(pair[:LANE, :], low[:, cols], preferred_element_type=jnp.float32)
            value = scale * (main[:LANE] + (main[LANE:] + side))
            if m == 1 and t == 0:
                shared = pl.ds(start, LANE)
                lane = lax.broadcasted_iota(jnp.int32, (LANE, LANE), 1)
                y_out[:, shared] = jnp.where(lane < ODD, y_out[:, shared], value[:, :LANE])
                y_out[:, pl.ds(start + LANE, LANE)] = value[:, LANE:]
            else:
                y_out[:, cols] = value


def last_product(block, row_y, col_z, rest_a, rest_m, cid):
    rows, cols = block.shape
    f32, bf16 = jnp.float32, jnp.bfloat16
    vmem = pl.BlockSpec(memory_space=pltpu.VMEM)
    lanes = 8 * len(LATE)
    return pl.pallas_call(
        last_kernel,
        out_shape=jax.ShapeDtypeStruct((LANE, PACKED), f32),
        in_specs=[vmem] + [ANY] * 4,
        out_specs=vmem,
        scratch_shapes=[
            pltpu.VMEM((SIDE, 2, rows, cols), f32),
            pltpu.VMEM((PLANE,) + row_y.shape[1:], f32),
            pltpu.VMEM((D, PACKED), bf16),
            pltpu.VMEM((D, PACKED), bf16),
            pltpu.VMEM((2 * LANE, D), bf16),
            pltpu.SemaphoreType.DMA((6,)),
            pltpu.SemaphoreType.DMA((6,)),
            pltpu.SemaphoreType.DMA((8 + 18,)),
            pltpu.SemaphoreType.DMA,
            pltpu.SemaphoreType.DMA,
            pltpu.SemaphoreType.DMA((lanes,)),
            pltpu.SemaphoreType.DMA((lanes,)),
        ],
        compiler_params=pltpu.CompilerParams(collective_id=cid, has_side_effects=True, vmem_limit_bytes=44 << 20),
        name="last_product",
    )(block, row_y, col_z, rest_a, rest_m)


def turned(rows, dst):
    fs = lax.axis_index("fs")
    for b in range(TURN):
        col = pl.multiple_of(LANE * lax.rem(fs + b, PLANE), LANE)
        dst[:, pl.ds(LANE * b, LANE)] = rows[:, pl.ds(col, LANE)]


def split(value):
    top = value.astype(jnp.bfloat16)
    return top, (value - top.astype(jnp.float32)).astype(jnp.bfloat16)


def times(src, dst, pair, high, low, scale=None):
    rows, size = src.shape
    pair[:rows, :], pair[rows:, :] = split(src[...])
    width = 1024

    @pl.loop(0, size // width)
    def _(j):
        cols = pl.ds(pl.multiple_of(j * width, width), width)
        main = jnp.dot(pair[...], high[:, cols], preferred_element_type=jnp.float32)
        rest = jnp.dot(pair[...], low[:, cols], preferred_element_type=jnp.float32)
        value = main[:rows] + (main[rows:] + (rest[:rows] + rest[rows:]))
        dst[:, cols] = value if scale is None else scale * value


def plane_peers():
    fs, tp, z, y, x, core = places()
    return [(plane_at(z, y, 0, w), tp) for w in WAYS] + [(plane_at(z, y, w, 0), tp) for w in WAYS] + [(fs, tp + 1 - 2 * core)]


def first_chain_kernel(sent, next_rows, coef_rows, buf, high, low, pair, v, p, w, *sems):
    greet(plane_peers())
    plane_gather(sent, buf, high, low, True, *sems)

    def diag(i, total):
        block = buf[i, :, :, pl.ds(0, LANE)].reshape(LANE, LANE)
        eye = lax.broadcasted_iota(jnp.int32, block.shape, 0) == lax.broadcasted_iota(jnp.int32, block.shape, 1)
        return total + jnp.where(eye, block, 0.0)

    acc = lax.fori_loop(0, PLANE, diag, jnp.zeros((LANE, LANE), jnp.float32))
    ssq = jnp.sum(jnp.sum(acc, axis=0, keepdims=True), axis=1, keepdims=True)
    s = 0.5 * lax.rsqrt(jnp.maximum(ssq / D, 1.0))
    s2 = s * s
    fs, tp = lax.axis_index("fs"), lax.axis_index("tp")
    shape = v.shape
    start = pl.multiple_of(128 * fs + 64 * lax.rem(tp, 2), 64)
    on_diag = lax.broadcasted_iota(jnp.int32, shape, 1) == start + lax.broadcasted_iota(jnp.int32, shape, 0)
    mine = pl.ds(start, shape[0])
    v[...] = s2 * (high[mine, :].astype(jnp.float32) + low[mine, :].astype(jnp.float32))
    times(v, p, pair, high, low, s2)
    coef_rows[...] = s * (jnp.where(on_diag, A_COEF, 0.0) + B_COEF * v[...] + C_COEF * p[...])
    times(p, w, pair, high, low, s2)
    w[...] = A_COEF * v[...] + B_COEF * p[...] + C_COEF * w[...]
    times(w, v, pair, high, low, s2)
    times(v, p, pair, high, low, s2)
    w[...] = A_COEF * w[...] + B_COEF * v[...] + C_COEF * p[...]
    turned(w, next_rows)


def second_chain_kernel(
    sent, coef, row_y, col_z, out, rest_m, buf, high, low, pair, v, p, q, send, recv, own_sem, pair_send, pair_recv, rest_send, rest_recv
):
    def slot(h, s, e, f, to, row, rows):
        return rest_m.at[s, h, FAR.index(f), pl.ds(row, rows)]

    greet(plane_peers())
    plane_gather(sent, buf, high, low, False, send, recv, own_sem, pair_send, pair_recv)
    rest = Rest(row_y, col_z, AMID, slot, rest_send, rest_recv)
    rest.start()

    def by_a1(src, dst):
        times(src, p, pair, high, low)
        times(p, q, pair, high, low)
        dst[...] = A_COEF * src[...] + B_COEF * p[...] + C_COEF * q[...]

    def by_t2():
        times(v, q, pair, high, low)
        v[...] = q[...]

        @pl.loop(0, 2)
        def _(_):
            by_a1(v, v)

    by_a1(coef, v)
    out[...] = A_COEF * v[...]
    by_t2()
    out[...] += B_COEF * v[...]
    for s in range(len(AMID)):
        rest.relay(s)
    by_t2()
    out[...] += C_COEF * v[...]
    rest.finish()


def chain_call(kernel, args, outs, cid, extra_sems, name):
    size, rows = D, 64
    f32, bf16 = jnp.float32, jnp.bfloat16
    vmem = pl.BlockSpec(memory_space=pltpu.VMEM)
    dma = pltpu.SemaphoreType.DMA
    return pl.pallas_call(
        kernel,
        out_shape=[jax.ShapeDtypeStruct(shape, f32) for shape in outs],
        in_specs=[vmem if a.ndim == 2 else ANY for a in args],
        out_specs=[vmem if len(shape) == 2 else ANY for shape in outs],
        scratch_shapes=[pltpu.VMEM((PLANE, 2, rows, TURN * LANE), f32)]
        + [pltpu.VMEM((size, size), bf16)] * 2
        + [pltpu.VMEM((2 * rows, size), bf16)]
        + [pltpu.VMEM((rows, size), f32)] * 3
        + [dma((40,)), dma((40,)), dma, dma((PLANE,)), dma((PLANE,))]
        + [dma((extra_sems,))] * (2 if extra_sems else 0),
        compiler_params=pltpu.CompilerParams(collective_id=cid, has_side_effects=True, vmem_limit_bytes=40 << 20),
        name=name,
    )(*args)


def only(lanes_low, x):
    lane = lax.broadcasted_iota(jnp.int32, x.shape, x.ndim - 1)
    return jnp.where((lane < ODD) == lanes_low, x, 0.0)


def local(weights_in, weights_mix, momentum_in, momentum_mix, grads_in, grads_mix):
    moment_in = MOMENTUM_DECAY * momentum_in + grads_in
    moment_mix = MOMENTUM_DECAY * momentum_mix + grads_mix
    packed = jnp.concatenate([moment_in[0], moment_in[1], moment_mix], axis=1)
    row_y, col_z = cross_gather(packed, 0)
    spans = [slice(0, WIDE), slice(WIDE + LANE, 2 * FFB), slice(WIDE, WIDE + LANE), slice(2 * FFB, PACKED)]
    l0, l1, lodd, lmix = (row_y.reshape(-1, PACKED)[:, s] for s in spans)
    r0, r1, rodd, rmix = (col_z.reshape(-1, PACKED)[:, s] for s in spans)
    dot_t = functools.partial(lax.dot_general, dimension_numbers=(((1,), (1,)), ((), ())), precision=HIGH)
    part = jnp.stack(
        [
            dot_t(l0, r0) + dot_t(only(True, lodd), rodd),
            dot_t(l1, r1) + dot_t(only(False, lodd), rodd),
            dot_t(lmix, rmix),
        ]
    ).reshape(3, SIDE, 2, 64, SIDE * LANE)
    sent, rest_a = reduce_to_planes(part, row_y, col_z, 1)
    turn = (64, TURN * LANE)
    sent, coef = chain_call(first_chain_kernel, (sent,), (turn, (64, D)), 2, 0, "first_chain")
    mid = (len(AMID), 2, len(FAR), 64, PACKED)
    poly, rest_m = chain_call(second_chain_kernel, (sent, coef, row_y, col_z), ((64, D), mid), 3, 8 * len(AMID), "second_chain")
    steps = last_product(poly, row_y, col_z, rest_a, rest_m, 4)
    step_in = jnp.stack([steps[:, :FFB], steps[:, FFB : 2 * FFB]])
    step_mix = steps[:, 2 * FFB :]
    return (
        moment_in,
        moment_mix,
        weights_in - STEP_RATE * step_in,
        weights_mix - STEP_RATE * step_mix,
        step_in,
        step_mix,
    )


def solution(mesh):
    specs = (
        P(None, "fs", "tp"),
        P("fs", "tp"),
        P(None, "fs", "tp"),
        P("fs", "tp"),
        P(None, "fs", "tp"),
        P("fs", "tp"),
    )
    return jax.shard_map(local, mesh=mesh, in_specs=specs, out_specs=specs, check_vma=False)
```

```python
import functools
import math

import jax
import jax.numpy as jnp
from jax import lax
from jax.experimental import pallas as pl
from jax.experimental.pallas import tpu as pltpu
from jax.sharding import PartitionSpec as P

D = 2048
FF = 5632
ITERS = 3

A_COEF = 3.4445
B_COEF = -4.775
C_COEF = 2.0315
MOMENTUM_DECAY = 0.95
STEP_RATE = 0.02
MESH = pl.DeviceIdType.MESH
ANY = pl.BlockSpec(memory_space=pl.ANY)

SIDE = 4
PLANE = SIDE * SIDE
LANE = 128
TURN = PLANE // 2 + 1
WIDE = 640
ODD = 64
MIX = 256
FFB = WIDE + ODD
PACKED = 2 * FFB + MIX
WAYS = (1, -1)
FAR = (-1, 1, 2)
CUT = 768
EARLY = ((-1, 0, PACKED),)
AMID = ((1, 0, PACKED), (2, 0, CUT))
LATE = ((2, CUT, PACKED - CUT),)
GROUPS = ((0, WIDE + LANE), (WIDE + LANE, WIDE), (2 * FFB, MIX))
LEFT = ((0, WIDE + LANE), (WIDE + LANE, WIDE + LANE), (2 * (WIDE + LANE), MIX))
RIGHT = (0, WIDE, 2 * FFB)
WIDTH_LEFT = 2 * (WIDE + LANE) + MIX


def put(src, dst, send, recv, fs, tp):
    return pltpu.make_async_remote_copy(
        src_ref=src, dst_ref=dst, send_sem=send, recv_sem=recv, device_id=(fs, tp), device_id_type=MESH
    )


def greet(peers):
    barrier = pltpu.get_barrier_semaphore()
    for fs, tp in peers:
        pl.semaphore_signal(barrier, inc=1, device_id=(fs, tp), device_id_type=MESH)
    pl.semaphore_wait(barrier, len(peers))


def plane_gather(block, buf, high, low, crossed, send, recv, own_sem, pair_send, pair_recv):
    fs, tp, z, y, x, core = places()
    other = tp + 1 - 2 * core
    half = block.shape[0] // 2
    quarter = half // 2

    def near(h, first, second):
        return plane_at(z, y, second, first) if h == 0 else plane_at(z, y, first, second)

    started, moves, pairs = [], iter(range(40)), {}

    def move(origin, rows, target, src=None):
        lane = next(moves)
        dst = buf.at[origin, core, rows]
        copy = put(dst if src is None else src, dst, send.at[lane], recv.at[lane], target, tp)
        copy.start()
        started.append(copy)
        return copy

    def halves(h):
        return pl.ds(h * half, half)

    def quarters(h, i):
        return pl.ds(h * half + i * quarter, quarter)

    def to_pair(along_z, along_y, src=None):
        at = buf.at[plane_at(z, y, along_z, along_y), core]
        k = len(pairs)
        copy = put(at if src is None else src, at, pair_send.at[k], pair_recv.at[k], fs, other)
        copy.start()
        pairs[along_z, along_y] = copy
        started.append(copy)

    direct = {(h, i): move(fs, halves(h), near(h, w, 0), block.at[halves(h)]) for i, w in enumerate(WAYS) for h in (0, 1)}
    second = {(h, i, 0): move(fs, halves(h), near(h, 0, w), block.at[halves(h)]) for i, w in enumerate(WAYS) for h in (0, 1)}
    keep = pltpu.make_async_copy(block, buf.at[fs, core], own_sem)
    keep.start()
    to_pair(0, 0, block)
    relay = {}
    for i, w in enumerate(WAYS):
        for h in (0, 1):
            direct[h, i].wait_recv()
            origin = near(h, -w, 0)
            relay[h, i] = move(origin, quarters(h, i), near(h, w, 0))
            for j, w2 in enumerate(WAYS):
                second[h, j, -w] = move(origin, halves(h), near(h, 0, w2))
    for h in (0, 1):
        for i in (0, 1):
            relay[h, i].wait_recv()
        origin = near(h, 2, 0)
        for j, w2 in enumerate(WAYS):
            second[h, j, 2] = move(origin, halves(h), near(h, 0, w2))
    tail = {}
    for e in (0, -1, 1, 2):
        for j, w2 in enumerate(WAYS):
            for h in (0, 1):
                second[h, j, e].wait_recv()
                tail[h, j, e] = move(near(h, e, -w2), quarters(h, j), near(h, 0, w2))
        if e == 0:
            for w in WAYS:
                to_pair(0, w)
                to_pair(w, 0)
        if e == 1:
            for w in WAYS:
                for w2 in WAYS:
                    to_pair(w, w2)

    def rebuild(i):
        sent = buf.at[i]
        for b in range(TURN):
            j = lax.rem(i + b, PLANE)
            row, col = i, j
            if crossed:
                row = SIDE * (i // SIDE) + lax.rem(j, SIDE)
                col = SIDE * (j // SIDE) + lax.rem(i, SIDE)
            rows = pl.ds(pl.multiple_of(LANE * row, LANE), LANE)
            cols = pl.ds(pl.multiple_of(LANE * col, LANE), LANE)
            value = sent[:, :, pl.ds(LANE * b, LANE)].reshape(LANE, LANE)
            high[rows, cols], low[rows, cols] = split(value)
            if 0 < b < TURN - 1:
                high[cols, rows], low[cols, rows] = split(value.T)

    keep.wait()
    for copy in pairs.values():
        copy.wait_recv()

    @pl.loop(0, 9)
    def _(n):
        rebuild(plane_at(z, y, n // 3 - 1, lax.rem(n, 3) - 1))

    for e in (0, -1, 1, 2):
        for j in (0, 1):
            for h in (0, 1):
                tail[h, j, e].wait_recv()
        to_pair(2, e)
        if e != 2:
            to_pair(e, 2)
    for e in FAR[:2] + (0,):
        pairs[e, 2].wait_recv()
        pairs[2, e].wait_recv()

    @pl.loop(0, 3)
    def _(n):
        rebuild(plane_at(z, y, n - 1, 2))

    pairs[2, 2].wait_recv()

    @pl.loop(0, 4)
    def _(n):
        rebuild(plane_at(z, y, 2, n - 1))

    for copy in started:
        copy.wait_send()


def places():
    fs, tp = lax.axis_index("fs"), lax.axis_index("tp")
    return fs, tp, fs // SIDE, lax.rem(fs, SIDE), tp // 2, lax.rem(tp, 2)


def plane_at(z, y, along_z, along_y):
    return SIDE * lax.rem(z + along_z + SIDE, SIDE) + lax.rem(y + along_y + SIDE, SIDE)


class Rest:
    def __init__(self, row_y, col_z, spans, slot, send, recv):
        fs, tp, z, y, x, core = places()
        self.tp, self.spans, self.slot, self.send, self.recv = tp, spans, slot, send, recv
        self.sources, self.here = (row_y, col_z), (y, z)
        self.half = row_y.shape[1] // 2
        self.near = [[plane_at(z, y, w, 0) for w in WAYS], [plane_at(z, y, 0, w) for w in WAYS]]
        self.peers = [(n, tp) for side in self.near for n in side]
        self.count = 0
        self.started = []

    def move(self, src, dst, target):
        i = self.count
        self.count += 1
        copy = put(src, dst, self.send.at[i], self.recv.at[i], target, self.tp)
        copy.start()
        self.started.append(copy)
        return copy

    def start(self):
        self.direct = {}
        for s, (e, col, width) in enumerate(self.spans):
            for i, w in enumerate(WAYS):
                for h in (0, 1):
                    rows = pl.ds(h * self.half, self.half)
                    block = lax.rem(self.here[h] + e + SIDE, SIDE)
                    src = self.sources[h].at[block, rows, pl.ds(col, width)]
                    self.direct[s, i, h] = self.move(src, self.slot(h, s, e, -w, w, 0, self.half), self.near[h][i])

    def relay(self, s):
        e = self.spans[s][0]
        part = self.half // 2
        for i, w in enumerate(WAYS):
            for h in (0, 1):
                self.direct[s, i, h].wait_recv()
                src = self.slot(h, s, e, -w, 0, part * i, part)
                self.direct[s, i, h, 2] = self.move(src, self.slot(h, s, e, 2, w, part * i, part), self.near[h][i])

    def finish(self):
        for key, copy in self.direct.items():
            if len(key) == 4:
                copy.wait_recv()
        for copy in self.started:
            copy.wait_send()


def opening_kernel(
    block, row_y, col_z, out, rest_a, lh, ll, rh, rl, part, pair, total, far, near, hold,
    send, recv, own, pair_send, pair_recv, sum_send, sum_recv, rest_send, rest_recv,
):
    fs, tp, z, y, x, core = places()
    right = 2 * lax.rem(x + 1, SIDE) + core
    left = 2 * lax.rem(x + SIDE - 1, SIDE) + core
    other = tp + 1 - 2 * core
    near_by = [[plane_at(z, y, 0, w) for w in WAYS], [plane_at(z, y, w, 0) for w in WAYS]]
    outs, here = (row_y, col_z), (y, z)
    rows = block.shape[0] // 2
    parts = [pl.ds(0, rows), pl.ds(rows, rows)]
    lane = iter(range(12 * len(GROUPS)))
    direct, relays, started = {}, {}, []

    def move(src, dst, target):
        i = next(lane)
        copy = put(src, dst, send.at[i], recv.at[i], target, tp)
        copy.start()
        started.append(copy)
        return copy

    def set_off(g):
        cols = pl.ds(*GROUPS[g])
        for k in (0, 1):
            for i in (0, 1):
                for d in (0, 1):
                    half = parts[(i + k) % 2]
                    direct[g, i, d, k] = move(block.at[half, cols], outs[d].at[here[d], half, cols], near_by[d][i])

    def relay(g):
        cols = pl.ds(*GROUPS[g])
        for i, w in enumerate(WAYS):
            for d in (0, 1):
                direct[g, i, d, 0].wait_recv()
                half = outs[d].at[lax.rem(here[d] - w + SIDE, SIDE), parts[i], cols]
                relays[g, i, d] = move(half, half, near_by[d][i])

    def arrived(g):
        for i in (0, 1):
            for d in (0, 1):
                direct[g, i, d, 1].wait_recv()
                relays[g, i, d].wait_recv()

    def prepare(g):
        first, width = GROUPS[g]
        last = first + width

        @pl.loop(0, 2 * SIDE)
        def _(n):
            at = pl.ds(pl.multiple_of(64 * n, 64), 64)
            src = pl.ds(pl.multiple_of(64 * lax.rem(n, 2), 64), 64)
            cols = pl.ds(first, width)
            rh[at, cols], rl[at, cols] = split(col_z[n // 2, src, cols])
            if g == 0:
                plain, shared = pl.ds(0, WIDE), pl.ds(WIDE, LANE)
                lh[at, plain], ll[at, plain] = split(row_y[n // 2, src, plain])
                value = row_y[n // 2, src, shared]
                low_lane = lax.broadcasted_iota(jnp.int32, value.shape, 1) < ODD
                lh[at, shared], ll[at, shared] = split(jnp.where(low_lane, value, 0.0))
                next_to = pl.ds(WIDE + LANE, LANE)
                lh[at, next_to], ll[at, next_to] = split(jnp.where(low_lane, 0.0, value))
            else:
                to = pl.ds(first + LANE, width)
                lh[at, to], ll[at, to] = split(row_y[n // 2, src, cols])

    def gram(m):
        lc = pl.ds(*LEFT[m])
        rc = pl.ds(RIGHT[m], LEFT[m][1])
        dot = functools.partial(
            lax.dot_general, dimension_numbers=(((1,), (1,)), ((), ())), preferred_element_type=jnp.float32
        )
        for r in (0, 1):
            at = pl.ds(256 * r, 256)
            value = dot(lh[at, lc], rh[:, rc]) + (dot(lh[at, lc], rl[:, rc]) + dot(ll[at, lc], rh[:, rc]))
            part[m, pl.ds(2 * r, 2)] = value.reshape((2,) + part.shape[2:])

    def to_pair(m):
        return put(part.at[m, :, 1 - core], pair.at[m], pair_send.at[m], pair_recv.at[m], fs, other)

    up, down = pl.ds(0, 2), pl.ds(2, 2)

    def far_copy(m, side, c):
        src = total.at[m, c] if side == 0 else total.at[m, 2 + c]
        i = 2 * side + c
        return put(src, far.at[m, side, c], sum_send.at[m, i], sum_recv.at[m, i], fs, (right, left)[side])

    def near_copy(m, side):
        src = total.at[m, down] if side == 0 else total.at[m, up]
        return put(src, near.at[side], sum_send.at[m, 4 + side], sum_recv.at[m, 4 + side], fs, (right, left)[side])

    def hold_copy(m, side, c):
        i = 6 + 2 * side + c
        return put(hold.at[m, side, c], near.at[2 + side, c], sum_send.at[m, i], sum_recv.at[m, i], fs, (right, left)[side])

    def before(m):
        return x == (m + SIDE - 1) % SIDE

    def after(m):
        return x == (m + 1) % SIDE

    def beyond(m):
        return x == (m + 2) % SIDE

    def sums(m):
        to_pair(m).wait()
        total[m] = part[m, :, core] + pair[m]

        @pl.when(beyond(m))
        def _():
            for c in (0, 1):
                for side in (0, 1):
                    far_copy(m, side, c).start()

        for side, role in ((0, before), (1, after)):

            @pl.when(role(m))
            def _():
                near_copy(m, side).start()

    def pass_on(m):
        for side, role in ((0, before), (1, after)):

            @pl.when(role(m))
            def _():
                for c in (0, 1):
                    far_copy(m, side, c).wait_recv()
                    hold[m, side, c] = far[m, side, c] + total[m, c if side == 0 else 2 + c]
                    hold_copy(m, side, c).start()

    def keep_sum(m):
        @pl.when(x == m)
        def _():
            near_copy(m, 0).wait_recv()
            near_copy(m, 1).wait_recv()
            for c in (0, 1):
                for side in (0, 1):
                    hold_copy(m, side, c).wait_recv()
            pair[m, up] = total[m, up] + near[2] + near[1]
            pair[m, down] = total[m, down] + near[3] + near[0]
            for b in range(TURN):
                chip = lax.rem(fs + b, PLANE)
                col = pl.multiple_of(LANE * (chip // SIDE), LANE)
                out[:, pl.ds(LANE * b, LANE)] = pair[m, lax.rem(chip, SIDE), :, pl.ds(col, LANE)]

    def sent(m):
        @pl.when(beyond(m))
        def _():
            for c in (0, 1):
                for side in (0, 1):
                    far_copy(m, side, c).wait_send()

        for side, role in ((0, before), (1, after)):

            @pl.when(role(m))
            def _():
                near_copy(m, side).wait_send()
                for c in (0, 1):
                    hold_copy(m, side, c).wait_send()

    def slot(h, s, e, f, to, row, count):
        return rest_a.at[h, FAR.index(f), pl.ds(row, count)]

    rest = Rest(row_y, col_z, EARLY, slot, rest_send, rest_recv)
    greet([(fs, right), (fs, left), (fs, other)] + rest.peers)
    set_off(0)
    keeps = [pltpu.make_async_copy(block, outs[d].at[here[d]], own.at[d]) for d in (0, 1)]
    for copy in keeps:
        copy.start()
    relay(0)
    set_off(1)
    for copy in keeps:
        copy.wait()
    arrived(0)
    prepare(0)
    gram(0)
    to_pair(0).start()
    relay(1)
    set_off(2)
    sums(0)
    pass_on(0)
    arrived(1)
    prepare(1)
    relay(2)
    gram(1)
    to_pair(1).start()
    arrived(2)
    prepare(2)
    gram(2)
    to_pair(2).start()
    sums(1)
    sums(2)
    rest.start()
    pass_on(1)
    pass_on(2)
    rest.relay(0)

    @pl.when(x == SIDE - 1)
    def _():
        out[...] = jnp.zeros_like(out)

    for m in range(3):
        keep_sum(m)
    for m in range(3):
        sent(m)
    for copy in started:
        copy.wait_send()
    rest.finish()


def opening(block, cid):
    f32, bf16 = jnp.float32, jnp.bfloat16
    rows, cols = block.shape
    size = SIDE * rows
    quad = (SIDE, rows // 2, size)
    duo = (2,) + quad[1:]
    vmem = pl.BlockSpec(memory_space=pltpu.VMEM)
    dma = pltpu.SemaphoreType.DMA
    moves = 12 * len(GROUPS)
    return pl.pallas_call(
        opening_kernel,
        out_shape=[
            jax.ShapeDtypeStruct((SIDE, rows, cols), f32),
            jax.ShapeDtypeStruct((SIDE, rows, cols), f32),
            jax.ShapeDtypeStruct((rows // 2, TURN * LANE), f32),
            jax.ShapeDtypeStruct((2, len(FAR), rows // 2, PACKED), f32),
        ],
        in_specs=[vmem],
        out_specs=[vmem, vmem, vmem, ANY],
        scratch_shapes=[
            pltpu.VMEM((size, WIDTH_LEFT), bf16),
            pltpu.VMEM((size, WIDTH_LEFT), bf16),
            pltpu.VMEM((size, cols), bf16),
            pltpu.VMEM((size, cols), bf16),
            pltpu.VMEM((3, SIDE, 2, rows // 2, size), f32),
            pltpu.VMEM((3,) + quad, f32),
            pltpu.VMEM((3,) + quad, f32),
            pltpu.VMEM((3, 2) + duo, f32),
            pltpu.VMEM((4,) + duo, f32),
            pltpu.VMEM((3, 2) + duo, f32),
            dma((moves,)),
            dma((moves,)),
            dma((2,)),
            dma((3,)),
            dma((3,)),
            dma((3, 10)),
            dma((3, 10)),
            dma((8 * len(EARLY),)),
            dma((8 * len(EARLY),)),
        ],
        compiler_params=pltpu.CompilerParams(collective_id=cid, has_side_effects=True, vmem_limit_bytes=36 << 20),
        name="opening",
    )(block)


def last_kernel(
    block, row_y, col_z, rest_a, rest_m, y_out, out, full, high, low, pair, send, recv, own, pair_send, pair_recv, rest_send, rest_recv
):
    fs, tp, z, y, x, core = places()
    right = 2 * lax.rem(x + 1, SIDE) + core
    left = 2 * lax.rem(x + SIDE - 1, SIDE) + core
    other = tp + 1 - 2 * core
    ahead, back, across = lax.rem(x + 1, SIDE), lax.rem(x + SIDE - 1, SIDE), lax.rem(x + 2, SIDE)

    def origin(h, e, f):
        return plane_at(z, y, f, e) if h == 0 else plane_at(z, y, e, f)

    def slot(h, s, e, f, to, row, rows):
        _, col, width = LATE[s]
        return full.at[origin(h, e, f + to), pl.ds(h * rest.half + row, rows), pl.ds(col, width)]

    rest = Rest(row_y, col_z, LATE, slot, rest_send, rest_recv)
    greet([(fs, right), (fs, left), (fs, other)] + rest.peers)
    half = block.shape[0] // 2
    parts = [pl.ds(0, half), pl.ds(half, half)]
    go_right = [put(block.at[parts[h]], out.at[x, core, parts[h]], send.at[h], recv.at[h], fs, right) for h in (0, 1)]
    go_left = [put(block.at[parts[1 - h]], out.at[x, core, parts[1 - h]], send.at[2 + h], recv.at[2 + h], fs, left) for h in (0, 1)]
    for h in (0, 1):
        go_right[h].start()
        go_left[h].start()
    rest.start()
    moves = [(block, out.at[x, core])]
    moves += [(row_y.at[lax.rem(y + e + SIDE, SIDE)], full.at[plane_at(z, y, 0, e)]) for e in (0,) + FAR]
    moves += [(col_z.at[lax.rem(z + e + SIDE, SIDE)], full.at[plane_at(z, y, e, 0)]) for e in FAR]
    for buf, (e, col, width) in ((rest_a, EARLY[0]), (rest_m.at[0], AMID[0]), (rest_m.at[1], AMID[1])):
        for h in (0, 1):
            for i, f in enumerate(FAR):
                dst = full.at[origin(h, e, f), pl.ds(h * rest.half, rest.half), pl.ds(col, width)]
                moves.append((buf.at[h, i, :, pl.ds(0, width)], dst))
    keeps = [pltpu.make_async_copy(src, dst, own.at[i]) for i, (src, dst) in enumerate(moves)]
    for keep in keeps:
        keep.start()
    put(block, out.at[x, core], pair_send, pair_recv, fs, other).start()
    go_right[0].wait_recv()
    first = out.at[back, core, parts[0]]
    relay_right = put(first, first, send.at[4], recv.at[4], fs, right)
    relay_right.start()
    go_left[0].wait_recv()
    second = out.at[ahead, core, parts[1]]
    relay_left = put(second, second, send.at[5], recv.at[5], fs, left)
    relay_left.start()
    rest.relay(0)
    go_right[1].wait_recv()
    put(out.at[back, core], out.at[back, core], pair_send, pair_recv, fs, other).start()
    go_left[1].wait_recv()
    put(out.at[ahead, core], out.at[ahead, core], pair_send, pair_recv, fs, other).start()
    for keep in keeps:
        keep.wait()
    rest.finish()

    @pl.loop(0, PLANE)
    def _(i):
        for k in (0, 1):
            rows = pl.ds(pl.multiple_of(LANE * i + 64 * k, 64), 64)
            high[rows, :], low[rows, :] = split(full[i, pl.ds(64 * k, 64), :])

    relay_right.wait_recv()
    relay_left.wait_recv()
    put(out.at[across, core], out.at[across, core], pair_send, pair_recv, fs, other).start()
    for c in go_right + go_left + [relay_right, relay_left]:
        c.wait_send()
    whole = put(out.at[:, core], out.at[:, 1 - core], pair_send, pair_recv, fs, other)
    whole.wait_send()
    whole.wait_recv()
    for m, (start, tiles) in enumerate(((0, 3), (WIDE, 3), (2 * FFB, 1))):
        for c in (0, 1):
            pair[pl.ds(64 * c, 64), :], pair[pl.ds(LANE + 64 * c, 64), :] = split(out[m, c])
        scale = math.sqrt(D) if m == 2 else math.sqrt(max(D, FF))
        for t in range(tiles):
            cols = pl.ds(start + 256 * t, 256)
            main = jnp.dot(pair[...], high[:, cols], preferred_element_type=jnp.float32)
            side = jnp.dot(pair[:LANE, :], low[:, cols], preferred_element_type=jnp.float32)
            value = scale * (main[:LANE] + (main[LANE:] + side))
            if m == 1 and t == 0:
                shared = pl.ds(start, LANE)
                lane = lax.broadcasted_iota(jnp.int32, (LANE, LANE), 1)
                y_out[:, shared] = jnp.where(lane < ODD, y_out[:, shared], value[:, :LANE])
                y_out[:, pl.ds(start + LANE, LANE)] = value[:, LANE:]
            else:
                y_out[:, cols] = value


def last_product(block, row_y, col_z, rest_a, rest_m, cid):
    rows, cols = block.shape
    f32, bf16 = jnp.float32, jnp.bfloat16
    vmem = pl.BlockSpec(memory_space=pltpu.VMEM)
    lanes = 8 * len(LATE)
    return pl.pallas_call(
        last_kernel,
        out_shape=jax.ShapeDtypeStruct((LANE, PACKED), f32),
        in_specs=[vmem] + [ANY] * 4,
        out_specs=vmem,
        scratch_shapes=[
            pltpu.VMEM((SIDE, 2, rows, cols), f32),
            pltpu.VMEM((PLANE,) + row_y.shape[1:], f32),
            pltpu.VMEM((D, PACKED), bf16),
            pltpu.VMEM((D, PACKED), bf16),
            pltpu.VMEM((2 * LANE, D), bf16),
            pltpu.SemaphoreType.DMA((6,)),
            pltpu.SemaphoreType.DMA((6,)),
            pltpu.SemaphoreType.DMA((8 + 18,)),
            pltpu.SemaphoreType.DMA,
            pltpu.SemaphoreType.DMA,
            pltpu.SemaphoreType.DMA((lanes,)),
            pltpu.SemaphoreType.DMA((lanes,)),
        ],
        compiler_params=pltpu.CompilerParams(collective_id=cid, has_side_effects=True, vmem_limit_bytes=36 << 20),
        name="last_product",
    )(block, row_y, col_z, rest_a, rest_m)


def turned(rows, dst):
    fs = lax.axis_index("fs")
    for b in range(TURN):
        col = pl.multiple_of(LANE * lax.rem(fs + b, PLANE), LANE)
        dst[:, pl.ds(LANE * b, LANE)] = rows[:, pl.ds(col, LANE)]


def split(value):
    top = value.astype(jnp.bfloat16)
    return top, (value - top.astype(jnp.float32)).astype(jnp.bfloat16)


def times(src, dst, pair, high, low, scale=None):
    rows, size = src.shape
    pair[:rows, :], pair[rows:, :] = split(src[...])
    width = 1024

    @pl.loop(0, size // width)
    def _(j):
        cols = pl.ds(pl.multiple_of(j * width, width), width)
        main = jnp.dot(pair[...], high[:, cols], preferred_element_type=jnp.float32)
        rest = jnp.dot(pair[...], low[:, cols], preferred_element_type=jnp.float32)
        value = main[:rows] + (main[rows:] + (rest[:rows] + rest[rows:]))
        dst[:, cols] = value if scale is None else scale * value


def plane_peers():
    fs, tp, z, y, x, core = places()
    return [(plane_at(z, y, 0, w), tp) for w in WAYS] + [(plane_at(z, y, w, 0), tp) for w in WAYS] + [(fs, tp + 1 - 2 * core)]


def first_chain_kernel(sent, next_rows, coef_rows, buf, high, low, pair, v, p, w, *sems):
    greet(plane_peers())
    plane_gather(sent, buf, high, low, True, *sems)

    def diag(i, total):
        block = buf[i, :, :, pl.ds(0, LANE)].reshape(LANE, LANE)
        eye = lax.broadcasted_iota(jnp.int32, block.shape, 0) == lax.broadcasted_iota(jnp.int32, block.shape, 1)
        return total + jnp.where(eye, block, 0.0)

    acc = lax.fori_loop(0, PLANE, diag, jnp.zeros((LANE, LANE), jnp.float32))
    ssq = jnp.sum(jnp.sum(acc, axis=0, keepdims=True), axis=1, keepdims=True)
    s = 0.5 * lax.rsqrt(jnp.maximum(ssq / D, 1.0))
    s2 = s * s
    fs, tp = lax.axis_index("fs"), lax.axis_index("tp")
    shape = v.shape
    start = pl.multiple_of(128 * fs + 64 * lax.rem(tp, 2), 64)
    on_diag = lax.broadcasted_iota(jnp.int32, shape, 1) == start + lax.broadcasted_iota(jnp.int32, shape, 0)
    mine = pl.ds(start, shape[0])
    v[...] = s2 * (high[mine, :].astype(jnp.float32) + low[mine, :].astype(jnp.float32))
    times(v, p, pair, high, low, s2)
    coef_rows[...] = s * (jnp.where(on_diag, A_COEF, 0.0) + B_COEF * v[...] + C_COEF * p[...])
    times(p, w, pair, high, low, s2)
    w[...] = A_COEF * v[...] + B_COEF * p[...] + C_COEF * w[...]
    times(w, v, pair, high, low, s2)
    times(v, p, pair, high, low, s2)
    w[...] = A_COEF * w[...] + B_COEF * v[...] + C_COEF * p[...]
    turned(w, next_rows)


def second_chain_kernel(
    sent, coef, row_y, col_z, out, rest_m, buf, high, low, pair, v, p, q, send, recv, own_sem, pair_send, pair_recv, rest_send, rest_recv
):
    def slot(h, s, e, f, to, row, rows):
        return rest_m.at[s, h, FAR.index(f), pl.ds(row, rows), pl.ds(0, AMID[s][2])]

    greet(plane_peers())
    plane_gather(sent, buf, high, low, False, send, recv, own_sem, pair_send, pair_recv)
    rest = Rest(row_y, col_z, AMID, slot, rest_send, rest_recv)
    rest.start()

    def by_a1(src, dst):
        times(src, p, pair, high, low)
        times(p, q, pair, high, low)
        dst[...] = A_COEF * src[...] + B_COEF * p[...] + C_COEF * q[...]

    def by_t2():
        times(v, q, pair, high, low)
        v[...] = q[...]

        @pl.loop(0, 2)
        def _(_):
            by_a1(v, v)

    by_a1(coef, v)
    out[...] = A_COEF * v[...]
    by_t2()
    out[...] += B_COEF * v[...]
    for s in range(len(AMID)):
        rest.relay(s)
    by_t2()
    out[...] += C_COEF * v[...]
    rest.finish()


def chain_call(kernel, args, outs, cid, extra_sems, name):
    size, rows = D, 64
    f32, bf16 = jnp.float32, jnp.bfloat16
    vmem = pl.BlockSpec(memory_space=pltpu.VMEM)
    dma = pltpu.SemaphoreType.DMA
    return pl.pallas_call(
        kernel,
        out_shape=[jax.ShapeDtypeStruct(shape, f32) for shape in outs],
        in_specs=[vmem if a.ndim == 2 else ANY for a in args],
        out_specs=[vmem if len(shape) == 2 else ANY for shape in outs],
        scratch_shapes=[pltpu.VMEM((PLANE, 2, rows, TURN * LANE), f32)]
        + [pltpu.VMEM((size, size), bf16)] * 2
        + [pltpu.VMEM((2 * rows, size), bf16)]
        + [pltpu.VMEM((rows, size), f32)] * 3
        + [dma((40,)), dma((40,)), dma, dma((PLANE,)), dma((PLANE,))]
        + [dma((extra_sems,))] * (2 if extra_sems else 0),
        compiler_params=pltpu.CompilerParams(collective_id=cid, has_side_effects=True, vmem_limit_bytes=40 << 20),
        name=name,
    )(*args)


def local(weights_in, weights_mix, momentum_in, momentum_mix, grads_in, grads_mix):
    moment_in = MOMENTUM_DECAY * momentum_in + grads_in
    moment_mix = MOMENTUM_DECAY * momentum_mix + grads_mix
    packed = jnp.concatenate([moment_in[0], moment_in[1], moment_mix], axis=1)
    row_y, col_z, sent, rest_a = opening(packed, 0)
    turn = (64, TURN * LANE)
    sent, coef = chain_call(first_chain_kernel, (sent,), (turn, (64, D)), 2, 0, "first_chain")
    mid = (len(AMID), 2, len(FAR), 64, PACKED)
    poly, rest_m = chain_call(second_chain_kernel, (sent, coef, row_y, col_z), ((64, D), mid), 3, 8 * len(AMID), "second_chain")
    steps = last_product(poly, row_y, col_z, rest_a, rest_m, 4)
    step_in = jnp.stack([steps[:, :FFB], steps[:, FFB : 2 * FFB]])
    step_mix = steps[:, 2 * FFB :]
    return (
        moment_in,
        moment_mix,
        weights_in - STEP_RATE * step_in,
        weights_mix - STEP_RATE * step_mix,
        step_in,
        step_mix,
    )


def solution(mesh):
    specs = (
        P(None, "fs", "tp"),
        P("fs", "tp"),
        P(None, "fs", "tp"),
        P("fs", "tp"),
        P(None, "fs", "tp"),
        P("fs", "tp"),
    )
    return jax.shard_map(local, mesh=mesh, in_specs=specs, out_specs=specs, check_vma=False)
```

```python
import functools
import math

import jax
import jax.numpy as jnp
from jax import lax
from jax.experimental import pallas as pl
from jax.experimental.pallas import tpu as pltpu
from jax.sharding import PartitionSpec as P

D = 2048
FF = 5632
ITERS = 3

A_COEF = 3.4445
B_COEF = -4.775
C_COEF = 2.0315
MOMENTUM_DECAY = 0.95
STEP_RATE = 0.02
MESH = pl.DeviceIdType.MESH
ANY = pl.BlockSpec(memory_space=pl.ANY)

SIDE = 4
PLANE = SIDE * SIDE
LANE = 128
TURN = PLANE // 2 + 1
WIDE = 640
ODD = 64
MIX = 256
FFB = WIDE + ODD
PACKED = 2 * FFB + MIX
WAYS = (1, -1)
FAR = (-1, 1, 2)
SPANS = tuple((e, 0, PACKED) for e in FAR)
GROUPS = ((0, WIDE + LANE), (WIDE + LANE, WIDE), (2 * FFB, MIX))
LEFT = ((0, WIDE + LANE), (WIDE + LANE, WIDE + LANE), (2 * (WIDE + LANE), MIX))
RIGHT = (0, WIDE, 2 * FFB)
WIDTH_LEFT = 2 * (WIDE + LANE) + MIX


def put(src, dst, send, recv, fs, tp):
    return pltpu.make_async_remote_copy(
        src_ref=src, dst_ref=dst, send_sem=send, recv_sem=recv, device_id=(fs, tp), device_id_type=MESH
    )


def greet(peers):
    barrier = pltpu.get_barrier_semaphore()
    for fs, tp in peers:
        pl.semaphore_signal(barrier, inc=1, device_id=(fs, tp), device_id_type=MESH)
    pl.semaphore_wait(barrier, len(peers))


def plane_gather(block, buf, high, low, crossed, send, recv, own_sem, pair_send, pair_recv):
    fs, tp, z, y, x, core = places()
    other = tp + 1 - 2 * core
    half = block.shape[0] // 2
    quarter = half // 2

    def near(h, first, second):
        return plane_at(z, y, second, first) if h == 0 else plane_at(z, y, first, second)

    started, moves, pairs = [], iter(range(40)), {}

    def move(origin, rows, target, src=None):
        lane = next(moves)
        dst = buf.at[origin, core, rows]
        copy = put(dst if src is None else src, dst, send.at[lane], recv.at[lane], target, tp)
        copy.start()
        started.append(copy)
        return copy

    def halves(h):
        return pl.ds(h * half, half)

    def quarters(h, i):
        return pl.ds(h * half + i * quarter, quarter)

    def to_pair(along_z, along_y, src=None):
        at = buf.at[plane_at(z, y, along_z, along_y), core]
        k = len(pairs)
        copy = put(at if src is None else src, at, pair_send.at[k], pair_recv.at[k], fs, other)
        copy.start()
        pairs[along_z, along_y] = copy
        started.append(copy)

    direct = {(h, i): move(fs, halves(h), near(h, w, 0), block.at[halves(h)]) for i, w in enumerate(WAYS) for h in (0, 1)}
    second = {(h, i, 0): move(fs, halves(h), near(h, 0, w), block.at[halves(h)]) for i, w in enumerate(WAYS) for h in (0, 1)}
    keep = pltpu.make_async_copy(block, buf.at[fs, core], own_sem)
    keep.start()
    to_pair(0, 0, block)
    relay = {}
    for i, w in enumerate(WAYS):
        for h in (0, 1):
            direct[h, i].wait_recv()
            origin = near(h, -w, 0)
            relay[h, i] = move(origin, quarters(h, i), near(h, w, 0))
            for j, w2 in enumerate(WAYS):
                second[h, j, -w] = move(origin, halves(h), near(h, 0, w2))
    for h in (0, 1):
        for i in (0, 1):
            relay[h, i].wait_recv()
        origin = near(h, 2, 0)
        for j, w2 in enumerate(WAYS):
            second[h, j, 2] = move(origin, halves(h), near(h, 0, w2))

    def rebuild(i):
        sent = buf.at[i]
        for b in range(TURN):
            j = lax.rem(i + b, PLANE)
            row, col = i, j
            if crossed:
                row = SIDE * (i // SIDE) + lax.rem(j, SIDE)
                col = SIDE * (j // SIDE) + lax.rem(i, SIDE)
            rows = pl.ds(pl.multiple_of(LANE * row, LANE), LANE)
            cols = pl.ds(pl.multiple_of(LANE * col, LANE), LANE)
            value = sent[:, :, pl.ds(LANE * b, LANE)].reshape(LANE, LANE)
            high[rows, cols], low[rows, cols] = split(value)
            if 0 < b < TURN - 1:
                high[cols, rows], low[cols, rows] = split(value.T)

    tail = {}
    for e in (0, -1, 1, 2):
        for j, w2 in enumerate(WAYS):
            for h in (0, 1):
                second[h, j, e].wait_recv()
                tail[h, j, e] = move(near(h, e, -w2), quarters(h, j), near(h, 0, w2))
        if e == 0:
            for w in WAYS:
                to_pair(0, w)
                to_pair(w, 0)
        if e == -1:
            keep.wait()
            for w in WAYS:
                pairs[0, w].wait_recv()
                pairs[w, 0].wait_recv()
            pairs[0, 0].wait_recv()

            @pl.loop(0, 3)
            def _(n):
                rebuild(plane_at(z, y, 0, n - 1))

            @pl.loop(0, 2)
            def _(n):
                rebuild(plane_at(z, y, 2 * n - 1, 0))

        if e == 1:
            for w in WAYS:
                for w2 in WAYS:
                    to_pair(w, w2)

    for w in WAYS:
        for w2 in WAYS:
            pairs[w, w2].wait_recv()

    @pl.loop(0, 4)
    def _(n):
        rebuild(plane_at(z, y, 2 * (n // 2) - 1, 2 * lax.rem(n, 2) - 1))

    def last_hop(e):
        for j in (0, 1):
            for h in (0, 1):
                tail[h, j, e].wait_recv()
        to_pair(2, e)
        if e != 2:
            to_pair(e, 2)

    for e in (0, -1, 1):
        last_hop(e)
    for e in (0, -1, 1):
        pairs[e, 2].wait_recv()
        pairs[2, e].wait_recv()

    @pl.loop(0, 3)
    def _(n):
        rebuild(plane_at(z, y, n - 1, 2))

    last_hop(2)

    @pl.loop(0, 3)
    def _(n):
        rebuild(plane_at(z, y, 2, n - 1))

    pairs[2, 2].wait_recv()
    rebuild(plane_at(z, y, 2, 2))
    for copy in started:
        copy.wait_send()


def places():
    fs, tp = lax.axis_index("fs"), lax.axis_index("tp")
    return fs, tp, fs // SIDE, lax.rem(fs, SIDE), tp // 2, lax.rem(tp, 2)


def plane_at(z, y, along_z, along_y):
    return SIDE * lax.rem(z + along_z + SIDE, SIDE) + lax.rem(y + along_y + SIDE, SIDE)


class Rest:
    def __init__(self, row_y, col_z, spans, slot, send, recv):
        fs, tp, z, y, x, core = places()
        self.tp, self.spans, self.slot, self.send, self.recv = tp, spans, slot, send, recv
        self.sources, self.here = (row_y, col_z), (y, z)
        self.half = row_y.shape[1] // 2
        self.near = [[plane_at(z, y, w, 0) for w in WAYS], [plane_at(z, y, 0, w) for w in WAYS]]
        self.peers = [(n, tp) for side in self.near for n in side]
        self.count = 0
        self.started = []
        self.direct = {}

    def move(self, src, dst, target):
        i = self.count
        self.count += 1
        copy = put(src, dst, self.send.at[i], self.recv.at[i], target, self.tp)
        copy.start()
        self.started.append(copy)
        return copy

    def start(self, s):
        e, col, width = self.spans[s]
        for i, w in enumerate(WAYS):
            for h in (0, 1):
                rows = pl.ds(h * self.half, self.half)
                block = lax.rem(self.here[h] + e + SIDE, SIDE)
                src = self.sources[h].at[block, rows, pl.ds(col, width)]
                self.direct[s, i, h] = self.move(src, self.slot(h, s, e, -w, w, 0, self.half), self.near[h][i])

    def relay(self, s):
        e = self.spans[s][0]
        part = self.half // 2
        for i, w in enumerate(WAYS):
            for h in (0, 1):
                self.direct[s, i, h].wait_recv()
                src = self.slot(h, s, e, -w, 0, part * i, part)
                self.direct[s, i, h, 2] = self.move(src, self.slot(h, s, e, 2, w, part * i, part), self.near[h][i])

    def finish(self):
        for key, copy in self.direct.items():
            if len(key) == 4:
                copy.wait_recv()
        for copy in self.started:
            copy.wait_send()


def opening_kernel(
    turned_in, mix, row_y, col_z, out, block, lh, ll, rh, rl, part, pair, total, far, near, hold,
    send, recv, own, pair_send, pair_recv, sum_send, sum_recv,
):
    fs, tp, z, y, x, core = places()
    right = 2 * lax.rem(x + 1, SIDE) + core
    left = 2 * lax.rem(x + SIDE - 1, SIDE) + core
    other = tp + 1 - 2 * core
    near_by = [[plane_at(z, y, 0, w) for w in WAYS], [plane_at(z, y, w, 0) for w in WAYS]]
    outs, here = (row_y, col_z), (y, z)
    rows = block.shape[0] // 2
    parts = [pl.ds(0, rows), pl.ds(rows, rows)]
    lane = iter(range(12 * len(GROUPS)))
    direct, relays, started = {}, {}, []

    def move(src, dst, target):
        i = next(lane)
        copy = put(src, dst, send.at[i], recv.at[i], target, tp)
        copy.start()
        started.append(copy)
        return copy

    def set_off(g):
        cols = pl.ds(*GROUPS[g])
        for k in (0, 1):
            for i in (0, 1):
                for d in (0, 1):
                    half = parts[(i + k) % 2]
                    direct[g, i, d, k] = move(block.at[half, cols], outs[d].at[here[d], half, cols], near_by[d][i])

    def relay(g):
        cols = pl.ds(*GROUPS[g])
        for i, w in enumerate(WAYS):
            for d in (0, 1):
                direct[g, i, d, 0].wait_recv()
                half = outs[d].at[lax.rem(here[d] - w + SIDE, SIDE), parts[i], cols]
                relays[g, i, d] = move(half, half, near_by[d][i])

    def arrived(g):
        for i in (0, 1):
            for d in (0, 1):
                direct[g, i, d, 1].wait_recv()
                relays[g, i, d].wait_recv()

    def prepare(g):
        first, width = GROUPS[g]
        last = first + width

        @pl.loop(0, 2 * SIDE)
        def _(n):
            at = pl.ds(pl.multiple_of(64 * n, 64), 64)
            src = pl.ds(pl.multiple_of(64 * lax.rem(n, 2), 64), 64)
            cols = pl.ds(first, width)
            rh[at, cols], rl[at, cols] = split(col_z[n // 2, src, cols])
            if g == 0:
                plain, shared = pl.ds(0, WIDE), pl.ds(WIDE, LANE)
                lh[at, plain], ll[at, plain] = split(row_y[n // 2, src, plain])
                value = row_y[n // 2, src, shared]
                low_lane = lax.broadcasted_iota(jnp.int32, value.shape, 1) < ODD
                lh[at, shared], ll[at, shared] = split(jnp.where(low_lane, value, 0.0))
                next_to = pl.ds(WIDE + LANE, LANE)
                lh[at, next_to], ll[at, next_to] = split(jnp.where(low_lane, 0.0, value))
            else:
                to = pl.ds(first + LANE, width)
                lh[at, to], ll[at, to] = split(row_y[n // 2, src, cols])

    def gram(m):
        lc = pl.ds(*LEFT[m])
        rc = pl.ds(RIGHT[m], LEFT[m][1])
        dot = functools.partial(
            lax.dot_general, dimension_numbers=(((1,), (1,)), ((), ())), preferred_element_type=jnp.float32
        )
        for r in (0, 1):
            at = pl.ds(256 * r, 256)
            value = dot(lh[at, lc], rh[:, rc]) + (dot(lh[at, lc], rl[:, rc]) + dot(ll[at, lc], rh[:, rc]))
            part[m, pl.ds(2 * r, 2)] = value.reshape((2,) + part.shape[2:])

    def to_pair(m):
        return put(part.at[m, :, 1 - core], pair.at[m], pair_send.at[m], pair_recv.at[m], fs, other)

    up, down = pl.ds(0, 2), pl.ds(2, 2)

    def far_copy(m, side, c):
        src = total.at[m, c] if side == 0 else total.at[m, 2 + c]
        i = 2 * side + c
        return put(src, far.at[m, side, c], sum_send.at[m, i], sum_recv.at[m, i], fs, (right, left)[side])

    def near_copy(m, side):
        src = total.at[m, down] if side == 0 else total.at[m, up]
        return put(src, near.at[side], sum_send.at[m, 4 + side], sum_recv.at[m, 4 + side], fs, (right, left)[side])

    def hold_copy(m, side, c):
        i = 6 + 2 * side + c
        return put(hold.at[m, side, c], near.at[2 + side, c], sum_send.at[m, i], sum_recv.at[m, i], fs, (right, left)[side])

    def before(m):
        return x == (m + SIDE - 1) % SIDE

    def after(m):
        return x == (m + 1) % SIDE

    def beyond(m):
        return x == (m + 2) % SIDE

    def sums(m):
        to_pair(m).wait()
        total[m] = part[m, :, core] + pair[m]

        @pl.when(beyond(m))
        def _():
            for c in (0, 1):
                for side in (0, 1):
                    far_copy(m, side, c).start()

        for side, role in ((0, before), (1, after)):

            @pl.when(role(m))
            def _():
                near_copy(m, side).start()

    def pass_on(m):
        for side, role in ((0, before), (1, after)):

            @pl.when(role(m))
            def _():
                for c in (0, 1):
                    far_copy(m, side, c).wait_recv()
                    hold[m, side, c] = far[m, side, c] + total[m, c if side == 0 else 2 + c]
                    hold_copy(m, side, c).start()

    def keep_sum(m):
        @pl.when(x == m)
        def _():
            near_copy(m, 0).wait_recv()
            near_copy(m, 1).wait_recv()
            for c in (0, 1):
                for side in (0, 1):
                    hold_copy(m, side, c).wait_recv()
            pair[m, up] = total[m, up] + near[2] + near[1]
            pair[m, down] = total[m, down] + near[3] + near[0]
            for b in range(TURN):
                chip = lax.rem(fs + b, PLANE)
                col = pl.multiple_of(LANE * (chip // SIDE), LANE)
                out[:, pl.ds(LANE * b, LANE)] = pair[m, lax.rem(chip, SIDE), :, pl.ds(col, LANE)]

    def sent(m):
        @pl.when(beyond(m))
        def _():
            for c in (0, 1):
                for side in (0, 1):
                    far_copy(m, side, c).wait_send()

        for side, role in ((0, before), (1, after)):

            @pl.when(role(m))
            def _():
                near_copy(m, side).wait_send()
                for c in (0, 1):
                    hold_copy(m, side, c).wait_send()

    for i in range(2 * FFB // LANE):
        block[:, pl.ds(LANE * i, LANE)] = turned_in[pl.ds(LANE * i, LANE), :].T
    block[:, pl.ds(2 * FFB, MIX)] = mix[...]
    greet([(fs, right), (fs, left), (fs, other)] + [(n, tp) for side in near_by for n in side])
    set_off(0)
    keeps = [pltpu.make_async_copy(block, outs[d].at[here[d]], own.at[d]) for d in (0, 1)]
    for copy in keeps:
        copy.start()
    relay(0)
    set_off(1)
    for copy in keeps:
        copy.wait()
    arrived(0)
    prepare(0)
    gram(0)
    to_pair(0).start()
    relay(1)
    set_off(2)
    sums(0)
    pass_on(0)
    arrived(1)
    prepare(1)
    relay(2)
    gram(1)
    to_pair(1).start()
    arrived(2)
    prepare(2)
    gram(2)
    to_pair(2).start()
    sums(1)
    sums(2)
    pass_on(1)
    pass_on(2)

    @pl.when(x == SIDE - 1)
    def _():
        out[...] = jnp.zeros_like(out)

    for m in range(3):
        keep_sum(m)
    for m in range(3):
        sent(m)
    for copy in started:
        copy.wait_send()


def opening(turned_in, mix, cid):
    f32, bf16 = jnp.float32, jnp.bfloat16
    rows, cols = LANE, PACKED
    size = SIDE * rows
    quad = (SIDE, rows // 2, size)
    duo = (2,) + quad[1:]
    vmem = pl.BlockSpec(memory_space=pltpu.VMEM)
    dma = pltpu.SemaphoreType.DMA
    moves = 12 * len(GROUPS)
    return pl.pallas_call(
        opening_kernel,
        out_shape=[
            jax.ShapeDtypeStruct((SIDE, rows, cols), f32),
            jax.ShapeDtypeStruct((SIDE, rows, cols), f32),
            jax.ShapeDtypeStruct((rows // 2, TURN * LANE), f32),
        ],
        in_specs=[vmem] * 2,
        out_specs=[vmem] * 3,
        scratch_shapes=[
            pltpu.VMEM((rows, cols), f32),
            pltpu.VMEM((size, WIDTH_LEFT), bf16),
            pltpu.VMEM((size, WIDTH_LEFT), bf16),
            pltpu.VMEM((size, cols), bf16),
            pltpu.VMEM((size, cols), bf16),
            pltpu.VMEM((3, SIDE, 2, rows // 2, size), f32),
            pltpu.VMEM((3,) + quad, f32),
            pltpu.VMEM((3,) + quad, f32),
            pltpu.VMEM((3, 2) + duo, f32),
            pltpu.VMEM((4,) + duo, f32),
            pltpu.VMEM((3, 2) + duo, f32),
            dma((moves,)),
            dma((moves,)),
            dma((2,)),
            dma((3,)),
            dma((3,)),
            dma((3, 10)),
            dma((3, 10)),
        ],
        compiler_params=pltpu.CompilerParams(collective_id=cid, has_side_effects=True, vmem_limit_bytes=36 << 20),
        name="opening",
    )(turned_in, mix)


def turned(rows, dst):
    fs = lax.axis_index("fs")
    for b in range(TURN):
        col = pl.multiple_of(LANE * lax.rem(fs + b, PLANE), LANE)
        dst[:, pl.ds(LANE * b, LANE)] = rows[:, pl.ds(col, LANE)]


def split(value):
    top = value.astype(jnp.bfloat16)
    return top, (value - top.astype(jnp.float32)).astype(jnp.bfloat16)


def times(src, dst, pair, high, low, scale=None):
    rows, size = src.shape
    pair[:rows, :], pair[rows:, :] = split(src[...])
    width = 1024

    @pl.loop(0, size // width)
    def _(j):
        cols = pl.ds(pl.multiple_of(j * width, width), width)
        main = jnp.dot(pair[...], high[:, cols], preferred_element_type=jnp.float32)
        rest = jnp.dot(pair[...], low[:, cols], preferred_element_type=jnp.float32)
        value = main[:rows] + (main[rows:] + (rest[:rows] + rest[rows:]))
        dst[:, cols] = value if scale is None else scale * value


def plane_peers():
    fs, tp, z, y, x, core = places()
    return [(plane_at(z, y, 0, w), tp) for w in WAYS] + [(plane_at(z, y, w, 0), tp) for w in WAYS] + [(fs, tp + 1 - 2 * core)]


def first_chain_kernel(sent, next_rows, coef_rows, buf, high, low, pair, v, p, w, *sems):
    greet(plane_peers())
    plane_gather(sent, buf, high, low, True, *sems)

    def diag(i, total):
        block = buf[i, :, :, pl.ds(0, LANE)].reshape(LANE, LANE)
        eye = lax.broadcasted_iota(jnp.int32, block.shape, 0) == lax.broadcasted_iota(jnp.int32, block.shape, 1)
        return total + jnp.where(eye, block, 0.0)

    acc = lax.fori_loop(0, PLANE, diag, jnp.zeros((LANE, LANE), jnp.float32))
    ssq = jnp.sum(jnp.sum(acc, axis=0, keepdims=True), axis=1, keepdims=True)
    s = 0.5 * lax.rsqrt(jnp.maximum(ssq / D, 1.0))
    s2 = s * s
    fs, tp = lax.axis_index("fs"), lax.axis_index("tp")
    shape = v.shape
    start = pl.multiple_of(128 * fs + 64 * lax.rem(tp, 2), 64)
    on_diag = lax.broadcasted_iota(jnp.int32, shape, 1) == start + lax.broadcasted_iota(jnp.int32, shape, 0)
    mine = pl.ds(start, shape[0])
    v[...] = s2 * (high[mine, :].astype(jnp.float32) + low[mine, :].astype(jnp.float32))
    times(v, p, pair, high, low, s2)
    coef_rows[...] = s * (jnp.where(on_diag, A_COEF, 0.0) + B_COEF * v[...] + C_COEF * p[...])
    times(p, w, pair, high, low, s2)
    w[...] = A_COEF * v[...] + B_COEF * p[...] + C_COEF * w[...]
    times(w, v, pair, high, low, s2)
    times(v, p, pair, high, low, s2)
    w[...] = A_COEF * w[...] + B_COEF * v[...] + C_COEF * p[...]
    turned(w, next_rows)


def closing_kernel(
    sent, coef, row_y, col_z, turned_out, mix_out, buf, high, low, pair, v, p, q, send, recv, own_sem, pair_send, pair_recv,
    full, poly, rows, left_side, rest_send, rest_recv, moved, go_send, go_recv, poly_own, poly_send, poly_recv,
):
    fs, tp, z, y, x, core = places()
    right = 2 * lax.rem(x + 1, SIDE) + core
    left = 2 * lax.rem(x + SIDE - 1, SIDE) + core
    other = tp + 1 - 2 * core
    ahead, back, across = lax.rem(x + 1, SIDE), lax.rem(x + SIDE - 1, SIDE), lax.rem(x + 2, SIDE)

    def slot(h, s, e, f, to, row, count):
        origin = plane_at(z, y, f + to, e) if h == 0 else plane_at(z, y, e, f + to)
        return full.at[origin, pl.ds(h * rest.half + row, count)]

    rest = Rest(row_y, col_z, SPANS, slot, rest_send, rest_recv)
    greet(plane_peers() + [(fs, right), (fs, left)])
    plane_gather(sent, buf, high, low, False, send, recv, own_sem, pair_send, pair_recv)
    rest.start(0)
    rest.start(1)
    moves = [(row_y.at[lax.rem(y + e + SIDE, SIDE)], full.at[plane_at(z, y, 0, e)]) for e in (0,) + FAR]
    moves += [(col_z.at[lax.rem(z + e + SIDE, SIDE)], full.at[plane_at(z, y, e, 0)]) for e in FAR]
    copies = [pltpu.make_async_copy(src, dst, moved.at[i]) for i, (src, dst) in enumerate(moves)]
    for copy in copies:
        copy.start()

    def by_a1(src, dst):
        times(src, p, pair, high, low)
        times(p, q, pair, high, low)
        dst[...] = A_COEF * src[...] + B_COEF * p[...] + C_COEF * q[...]

    def by_t2():
        times(v, q, pair, high, low)
        v[...] = q[...]

        @pl.loop(0, 2)
        def _(_):
            by_a1(v, v)

    by_a1(coef, v)
    poly[...] = A_COEF * v[...]
    by_t2()
    poly[...] += B_COEF * v[...]
    rest.relay(0)
    rest.start(2)
    by_t2()
    poly[...] += C_COEF * v[...]

    half = poly.shape[0] // 2
    parts = [pl.ds(0, half), pl.ds(half, half)]

    def go(i, src, slot_x, part, target):
        return put(src, rows.at[slot_x, core, part], go_send.at[i], go_recv.at[i], fs, target)

    go_right = [go(h, poly.at[parts[h]], x, parts[h], right) for h in (0, 1)]
    go_left = [go(2 + h, poly.at[parts[1 - h]], x, parts[1 - h], left) for h in (0, 1)]
    for h in (0, 1):
        go_right[h].start()
        go_left[h].start()
    mine = pltpu.make_async_copy(poly, rows.at[x, core], poly_own)
    mine.start()

    def to_pair(i, slot_x, src=None):
        at = rows.at[slot_x, core]
        copy = put(at if src is None else src, at, poly_send.at[i], poly_recv.at[i], fs, other)
        copy.start()
        return copy

    pairs = [to_pair(0, x, poly)]
    rest.relay(1)
    go_right[0].wait_recv()
    relay_right = go(4, rows.at[back, core, parts[0]], back, parts[0], right)
    relay_right.start()
    go_left[0].wait_recv()
    relay_left = go(5, rows.at[ahead, core, parts[1]], ahead, parts[1], left)
    relay_left.start()
    rest.relay(2)
    go_right[1].wait_recv()
    pairs.append(to_pair(1, back))
    go_left[1].wait_recv()
    pairs.append(to_pair(2, ahead))
    for copy in copies:
        copy.wait()
    rest.finish()

    @pl.loop(0, 2 * PLANE)
    def _(n):
        at = pl.ds(pl.multiple_of(64 * n, 64), 64)
        src = pl.ds(pl.multiple_of(64 * lax.rem(n, 2), 64), 64)
        high[at, pl.ds(0, PACKED)], low[at, pl.ds(0, PACKED)] = split(full[n // 2, src, :])

    def product(m):
        for c in (0, 1):
            left_side[pl.ds(64 * c, 64), :], left_side[pl.ds(LANE + 64 * c, 64), :] = split(rows[m, c])
        first, tiles = ((0, 3), (WIDE, 3), (2 * FFB, 1))[m]
        for t in range(tiles):
            start = first + 256 * t
            cols = pl.ds(start, 256)
            main = jnp.dot(left_side[...], high[:, cols], preferred_element_type=jnp.float32)
            side = jnp.dot(left_side[:LANE, :], low[:, cols], preferred_element_type=jnp.float32)
            value = main[:LANE] + (main[LANE:] + side)
            if m == 2:
                mix_out[...] = value
                continue
            value = value.T
            low_cut, high_cut = max(start, FFB * m), min(start + 256, FFB * (m + 1))
            turned_out[pl.ds(low_cut, high_cut - low_cut), :] = value[low_cut - start : high_cut - start]

    mine.wait()
    for copy in pairs:
        copy.wait_recv()
    for m in range(3):

        @pl.when(across != m)
        def _():
            product(m)

    relay_right.wait_recv()
    relay_left.wait_recv()
    pairs.append(to_pair(3, across))
    pairs[3].wait_recv()
    for m in range(3):

        @pl.when(across == m)
        def _():
            product(m)

    for copy in go_right + go_left + [relay_right, relay_left] + pairs:
        copy.wait_send()


def chain_call(kernel, args, outs, cid, extra, limit, name):
    size, rows = D, 64
    f32, bf16 = jnp.float32, jnp.bfloat16
    vmem = pl.BlockSpec(memory_space=pltpu.VMEM)
    dma = pltpu.SemaphoreType.DMA
    return pl.pallas_call(
        kernel,
        out_shape=[jax.ShapeDtypeStruct(shape, f32) for shape in outs],
        in_specs=[vmem if a.ndim == 2 else ANY for a in args],
        out_specs=[vmem] * len(outs),
        scratch_shapes=[pltpu.VMEM((PLANE, 2, rows, TURN * LANE), f32)]
        + [pltpu.VMEM((size, size), bf16)] * 2
        + [pltpu.VMEM((2 * rows, size), bf16)]
        + [pltpu.VMEM((rows, size), f32)] * 3
        + [dma((40,)), dma((40,)), dma, dma((PLANE,)), dma((PLANE,))]
        + extra,
        compiler_params=pltpu.CompilerParams(collective_id=cid, has_side_effects=True, vmem_limit_bytes=limit << 20),
        name=name,
    )(*args)


def local(weights_in, weights_mix, momentum_in, momentum_mix, grads_in, grads_mix):
    f32, dma = jnp.float32, pltpu.SemaphoreType.DMA
    turned_in = MOMENTUM_DECAY * jnp.swapaxes(momentum_in, 1, 2) + jnp.swapaxes(grads_in, 1, 2)
    moment_mix = MOMENTUM_DECAY * momentum_mix + grads_mix
    row_y, col_z, sent = opening(turned_in.reshape(2 * FFB, LANE), moment_mix, 0)
    turn = (64, TURN * LANE)
    sent, coef = chain_call(first_chain_kernel, (sent,), (turn, (64, D)), 1, [], 30, "first_chain")
    extra = [
        pltpu.VMEM((PLANE, LANE, PACKED), f32),
        pltpu.VMEM((64, D), f32),
        pltpu.VMEM((SIDE, 2, 64, D), f32),
        pltpu.VMEM((2 * LANE, D), jnp.bfloat16),
        dma((8 * len(SPANS),)),
        dma((8 * len(SPANS),)),
        dma((7,)),
        dma((6,)),
        dma((6,)),
        dma,
        dma((4,)),
        dma((4,)),
    ]
    outs = ((2 * FFB, LANE), (LANE, MIX))
    turned_step, step_mix = chain_call(closing_kernel, (sent, coef, row_y, col_z), outs, 2, extra, 47, "closing")
    turned_step = math.sqrt(max(D, FF)) * turned_step.reshape(2, FFB, LANE)
    step_mix = math.sqrt(D) * step_mix
    turned_weights = jnp.swapaxes(weights_in, 1, 2) - STEP_RATE * turned_step
    return (
        jnp.swapaxes(turned_in, 1, 2),
        moment_mix,
        jnp.swapaxes(turned_weights, 1, 2),
        weights_mix - STEP_RATE * step_mix,
        jnp.swapaxes(turned_step, 1, 2),
        step_mix,
    )


def solution(mesh):
    specs = (
        P(None, "fs", "tp"),
        P("fs", "tp"),
        P(None, "fs", "tp"),
        P("fs", "tp"),
        P(None, "fs", "tp"),
        P("fs", "tp"),
    )
    return jax.shard_map(local, mesh=mesh, in_specs=specs, out_specs=specs, check_vma=False)
```

```python
import functools
import math

import jax
import jax.numpy as jnp
from jax import lax
from jax.experimental import pallas as pl
from jax.experimental.pallas import tpu as pltpu
from jax.sharding import PartitionSpec as P

D = 2048
FF = 5632
ITERS = 3

A_COEF = 3.4445
B_COEF = -4.775
C_COEF = 2.0315
MOMENTUM_DECAY = 0.95
STEP_RATE = 0.02
MESH = pl.DeviceIdType.MESH

SIDE = 4
PLANE = SIDE * SIDE
LANE = 128
TURN = PLANE // 2 + 1
WIDE = 640
ODD = 64
MIX = 256
FFB = WIDE + ODD
PACKED = 2 * FFB + MIX
WAYS = (1, -1)
FAR = (-1, 1, 2)
SPANS = tuple((e, 0, PACKED) for e in FAR)
GROUPS = ((0, WIDE + LANE), (WIDE + LANE, WIDE), (2 * FFB, MIX))
LEFT = ((0, WIDE + LANE), (WIDE + LANE, WIDE + LANE), (2 * (WIDE + LANE), MIX))
RIGHT = (0, WIDE, 2 * FFB)
WIDTH_LEFT = 2 * (WIDE + LANE) + MIX
OWNER = (1, 0, 2)


def put(src, dst, send, recv, fs, tp):
    return pltpu.make_async_remote_copy(
        src_ref=src, dst_ref=dst, send_sem=send, recv_sem=recv, device_id=(fs, tp), device_id_type=MESH
    )


def greet(peers):
    barrier = pltpu.get_barrier_semaphore()
    for fs, tp in peers:
        pl.semaphore_signal(barrier, inc=1, device_id=(fs, tp), device_id_type=MESH)
    pl.semaphore_wait(barrier, len(peers))


def plane_gather(block, buf, high, low, crossed, send, recv, own_sem, pair_send, pair_recv):
    fs, tp, z, y, x, core = places()
    other = tp + 1 - 2 * core
    half = block.shape[0] // 2
    quarter = half // 2

    def near(h, first, second):
        return plane_at(z, y, second, first) if h == 0 else plane_at(z, y, first, second)

    started, moves, pairs = [], iter(range(40)), {}

    def move(origin, rows, target, src=None):
        lane = next(moves)
        dst = buf.at[origin, core, rows]
        copy = put(dst if src is None else src, dst, send.at[lane], recv.at[lane], target, tp)
        copy.start()
        started.append(copy)
        return copy

    def halves(h):
        return pl.ds(h * half, half)

    def quarters(h, i):
        return pl.ds(h * half + i * quarter, quarter)

    def to_pair(along_z, along_y, src=None):
        at = buf.at[plane_at(z, y, along_z, along_y), core]
        k = len(pairs)
        copy = put(at if src is None else src, at, pair_send.at[k], pair_recv.at[k], fs, other)
        copy.start()
        pairs[along_z, along_y] = copy
        started.append(copy)

    direct = {(h, i): move(fs, halves(h), near(h, w, 0), block.at[halves(h)]) for i, w in enumerate(WAYS) for h in (0, 1)}
    second = {(h, i, 0): move(fs, halves(h), near(h, 0, w), block.at[halves(h)]) for i, w in enumerate(WAYS) for h in (0, 1)}
    keep = pltpu.make_async_copy(block, buf.at[fs, core], own_sem)
    keep.start()
    to_pair(0, 0, block)
    relay = {}
    for i, w in enumerate(WAYS):
        for h in (0, 1):
            direct[h, i].wait_recv()
            origin = near(h, -w, 0)
            relay[h, i] = move(origin, quarters(h, i), near(h, w, 0))
            for j, w2 in enumerate(WAYS):
                second[h, j, -w] = move(origin, halves(h), near(h, 0, w2))
    for h in (0, 1):
        for i in (0, 1):
            relay[h, i].wait_recv()
        origin = near(h, 2, 0)
        for j, w2 in enumerate(WAYS):
            second[h, j, 2] = move(origin, halves(h), near(h, 0, w2))

    def rebuild(i):
        sent = buf.at[i]
        for b in range(TURN):
            j = lax.rem(i + b, PLANE)
            row, col = i, j
            if crossed:
                row = SIDE * (i // SIDE) + lax.rem(j, SIDE)
                col = SIDE * (j // SIDE) + lax.rem(i, SIDE)
            rows = pl.ds(pl.multiple_of(LANE * row, LANE), LANE)
            cols = pl.ds(pl.multiple_of(LANE * col, LANE), LANE)
            value = sent[:, :, pl.ds(LANE * b, LANE)].reshape(LANE, LANE)
            high[rows, cols], low[rows, cols] = split(value)
            if 0 < b < TURN - 1:
                high[cols, rows], low[cols, rows] = split(value.T)

    tail = {}
    for e in (0, -1, 1, 2):
        for j, w2 in enumerate(WAYS):
            for h in (0, 1):
                second[h, j, e].wait_recv()
                tail[h, j, e] = move(near(h, e, -w2), quarters(h, j), near(h, 0, w2))
        if e == 0:
            for w in WAYS:
                to_pair(0, w)
                to_pair(w, 0)
        if e == -1:
            keep.wait()
            for w in WAYS:
                pairs[0, w].wait_recv()
                pairs[w, 0].wait_recv()
            pairs[0, 0].wait_recv()

            @pl.loop(0, 3)
            def _(n):
                rebuild(plane_at(z, y, 0, n - 1))

            @pl.loop(0, 2)
            def _(n):
                rebuild(plane_at(z, y, 2 * n - 1, 0))

        if e == 1:
            for w in WAYS:
                for w2 in WAYS:
                    to_pair(w, w2)

    for w in WAYS:
        for w2 in WAYS:
            pairs[w, w2].wait_recv()

    @pl.loop(0, 4)
    def _(n):
        rebuild(plane_at(z, y, 2 * (n // 2) - 1, 2 * lax.rem(n, 2) - 1))

    def last_hop(e):
        for j in (0, 1):
            for h in (0, 1):
                tail[h, j, e].wait_recv()
        to_pair(2, e)
        if e != 2:
            to_pair(e, 2)

    for e in (0, -1, 1):
        last_hop(e)
    for e in (0, -1, 1):
        pairs[e, 2].wait_recv()
        pairs[2, e].wait_recv()

    @pl.loop(0, 3)
    def _(n):
        rebuild(plane_at(z, y, n - 1, 2))

    last_hop(2)

    @pl.loop(0, 3)
    def _(n):
        rebuild(plane_at(z, y, 2, n - 1))

    pairs[2, 2].wait_recv()
    rebuild(plane_at(z, y, 2, 2))
    for copy in started:
        copy.wait_send()


def places():
    fs, tp = lax.axis_index("fs"), lax.axis_index("tp")
    return fs, tp, fs // SIDE, lax.rem(fs, SIDE), tp // 2, lax.rem(tp, 2)


def plane_at(z, y, along_z, along_y):
    return SIDE * lax.rem(z + along_z + SIDE, SIDE) + lax.rem(y + along_y + SIDE, SIDE)


class Rest:
    def __init__(self, full, spans, send, recv):
        fs, tp, z, y, x, core = places()
        self.z, self.y, self.tp, self.full, self.spans, self.send, self.recv = z, y, tp, full, spans, send, recv
        self.half = full.shape[1] // 2

    def part(self, s, h, f, row, count):
        e, col, width = self.spans[s]
        origin = plane_at(self.z, self.y, f, e) if h == 0 else plane_at(self.z, self.y, e, f)
        return self.full.at[origin, pl.ds(h * self.half + row, count), pl.ds(col, width)]

    def copy(self, s, i, h, again):
        w, quarter = WAYS[i], self.half // 2
        part = self.part(s, h, -w, quarter * i, quarter) if again else self.part(s, h, 0, 0, self.half)
        target = plane_at(self.z, self.y, w, 0) if h == 0 else plane_at(self.z, self.y, 0, w)
        lane = 8 * s + 4 * again + 2 * i + h
        return put(part, part, self.send.at[lane], self.recv.at[lane], target, self.tp)

    def start(self, s):
        for i in (0, 1):
            for h in (0, 1):
                self.copy(s, i, h, 0).start()

    def relay(self, s):
        for i in (0, 1):
            for h in (0, 1):
                self.copy(s, i, h, 0).wait_recv()
                self.copy(s, i, h, 1).start()

    def finish(self):
        for s in range(len(self.spans)):
            for i in (0, 1):
                for h in (0, 1):
                    self.copy(s, i, h, 1).wait_recv()
                    for again in (0, 1):
                        self.copy(s, i, h, again).wait_send()


def opening(full, out, lh, ll, rh, rl, part, pair, total, far, near, hold, send, recv, pair_send, pair_recv, sum_send, sum_recv):
    fs, tp, z, y, x, core = places()
    right = 2 * lax.rem(x + 1, SIDE) + core
    left = 2 * lax.rem(x + SIDE - 1, SIDE) + core
    other = tp + 1 - 2 * core
    near_by = [[plane_at(z, y, 0, w) for w in WAYS], [plane_at(z, y, w, 0) for w in WAYS]]
    rows = full.shape[1] // 2
    parts = [pl.ds(0, rows), pl.ds(rows, rows)]
    lane = iter(range(12 * len(GROUPS)))
    direct, relays, started = {}, {}, []

    def move(src, dst, target):
        i = next(lane)
        copy = put(src, dst, send.at[i], recv.at[i], target, tp)
        copy.start()
        started.append(copy)
        return copy

    def set_off(g):
        cols = pl.ds(*GROUPS[g])
        for k in (0, 1):
            for i in (0, 1):
                for d in (0, 1):
                    half = parts[(i + k) % 2]
                    mine = full.at[fs, half, cols]
                    direct[g, i, d, k] = move(mine, mine, near_by[d][i])

    def relay(g):
        cols = pl.ds(*GROUPS[g])
        for i, w in enumerate(WAYS):
            for d in (0, 1):
                direct[g, i, d, 0].wait_recv()
                half = full.at[near_by[d][1 - i], parts[i], cols]
                relays[g, i, d] = move(half, half, near_by[d][i])

    def arrived(g):
        for i in (0, 1):
            for d in (0, 1):
                direct[g, i, d, 1].wait_recv()
                relays[g, i, d].wait_recv()

    def prepare(g):
        first, width = GROUPS[g]
        last = first + width

        @pl.loop(0, 2 * SIDE)
        def _(n):
            at = pl.ds(pl.multiple_of(64 * n, 64), 64)
            src = pl.ds(pl.multiple_of(64 * lax.rem(n, 2), 64), 64)
            cols = pl.ds(first, width)
            rh[at, cols], rl[at, cols] = split(full[SIDE * (n // 2) + y, src, cols])
            if g == 0:
                plain, shared = pl.ds(0, WIDE), pl.ds(WIDE, LANE)
                lh[at, plain], ll[at, plain] = split(full[SIDE * z + n // 2, src, plain])
                value = full[SIDE * z + n // 2, src, shared]
                low_lane = lax.broadcasted_iota(jnp.int32, value.shape, 1) < ODD
                lh[at, shared], ll[at, shared] = split(jnp.where(low_lane, value, 0.0))
                next_to = pl.ds(WIDE + LANE, LANE)
                lh[at, next_to], ll[at, next_to] = split(jnp.where(low_lane, 0.0, value))
            else:
                to = pl.ds(first + LANE, width)
                lh[at, to], ll[at, to] = split(full[SIDE * z + n // 2, src, cols])

    def gram(m):
        lc = pl.ds(*LEFT[m])
        rc = pl.ds(RIGHT[m], LEFT[m][1])
        dot = functools.partial(
            lax.dot_general, dimension_numbers=(((1,), (1,)), ((), ())), preferred_element_type=jnp.float32
        )
        for r in (0, 1):
            at = pl.ds(256 * r, 256)
            value = dot(lh[at, lc], rh[:, rc]) + (dot(lh[at, lc], rl[:, rc]) + dot(ll[at, lc], rh[:, rc]))
            part[m, pl.ds(2 * r, 2)] = value.reshape((2,) + part.shape[2:])

    def to_pair(m):
        return put(part.at[m, :, 1 - core], pair.at[m], pair_send.at[m], pair_recv.at[m], fs, other)

    up, down = pl.ds(0, 2), pl.ds(2, 2)

    def far_copy(m, side, c):
        src = total.at[m, c] if side == 0 else total.at[m, 2 + c]
        i = 2 * side + c
        return put(src, far.at[m, side, c], sum_send.at[m, i], sum_recv.at[m, i], fs, (right, left)[side])

    def near_copy(m, side):
        src = total.at[m, down] if side == 0 else total.at[m, up]
        return put(src, near.at[side], sum_send.at[m, 4 + side], sum_recv.at[m, 4 + side], fs, (right, left)[side])

    def hold_copy(m, side, c):
        i = 6 + 2 * side + c
        return put(hold.at[m, side, c], near.at[2 + side, c], sum_send.at[m, i], sum_recv.at[m, i], fs, (right, left)[side])

    def before(m):
        return x == (OWNER[m] + SIDE - 1) % SIDE

    def after(m):
        return x == (OWNER[m] + 1) % SIDE

    def beyond(m):
        return x == (OWNER[m] + 2) % SIDE

    def sums(m):
        to_pair(m).wait()
        total[m] = part[m, :, core] + pair[m]

        @pl.when(beyond(m))
        def _():
            for c in (0, 1):
                for side in (0, 1):
                    far_copy(m, side, c).start()

        for side, role in ((0, before), (1, after)):

            @pl.when(role(m))
            def _():
                near_copy(m, side).start()

    def pass_on(m):
        for side, role in ((0, before), (1, after)):

            @pl.when(role(m))
            def _():
                for c in (0, 1):
                    far_copy(m, side, c).wait_recv()
                    hold[m, side, c] = far[m, side, c] + total[m, c if side == 0 else 2 + c]
                    hold_copy(m, side, c).start()

    def keep_sum(m):
        @pl.when(x == OWNER[m])
        def _():
            near_copy(m, 0).wait_recv()
            near_copy(m, 1).wait_recv()
            for c in (0, 1):
                for side in (0, 1):
                    hold_copy(m, side, c).wait_recv()
            pair[m, up] = total[m, up] + near[2] + near[1]
            pair[m, down] = total[m, down] + near[3] + near[0]
            for b in range(TURN):
                chip = lax.rem(fs + b, PLANE)
                col = pl.multiple_of(LANE * (chip // SIDE), LANE)
                out[:, pl.ds(LANE * b, LANE)] = pair[m, lax.rem(chip, SIDE), :, pl.ds(col, LANE)]

    def sent(m):
        @pl.when(beyond(m))
        def _():
            for c in (0, 1):
                for side in (0, 1):
                    far_copy(m, side, c).wait_send()

        for side, role in ((0, before), (1, after)):

            @pl.when(role(m))
            def _():
                near_copy(m, side).wait_send()
                for c in (0, 1):
                    hold_copy(m, side, c).wait_send()

    set_off(0)
    relay(0)
    set_off(1)
    arrived(0)
    prepare(0)
    gram(0)
    to_pair(0).start()
    relay(1)
    set_off(2)
    sums(0)
    pass_on(0)
    arrived(1)
    prepare(1)
    relay(2)
    gram(1)
    to_pair(1).start()
    arrived(2)
    prepare(2)
    gram(2)
    to_pair(2).start()
    sums(1)
    sums(2)
    pass_on(1)
    pass_on(2)

    @pl.when(x == SIDE - 1)
    def _():
        out[...] = jnp.zeros_like(out)

    for m in range(3):
        keep_sum(m)
    for m in range(3):
        sent(m)
    for copy in started:
        copy.wait_send()


def turned(rows, dst):
    fs = lax.axis_index("fs")
    for b in range(TURN):
        col = pl.multiple_of(LANE * lax.rem(fs + b, PLANE), LANE)
        dst[:, pl.ds(LANE * b, LANE)] = rows[:, pl.ds(col, LANE)]


def split(value):
    top = value.astype(jnp.bfloat16)
    return top, (value - top.astype(jnp.float32)).astype(jnp.bfloat16)


def times(src, dst, pair, high, low, scale=None):
    rows = src.shape[0]
    pair[:rows, :], pair[rows:, :] = split(src[...])
    main = jnp.dot(pair[...], high[...], preferred_element_type=jnp.float32)
    rest = jnp.dot(pair[...], low[...], preferred_element_type=jnp.float32)
    value = main[:rows] + (main[rows:] + (rest[:rows] + rest[rows:]))
    dst[...] = value if scale is None else scale * value


def plane_peers():
    fs, tp, z, y, x, core = places()
    return [(plane_at(z, y, 0, w), tp) for w in WAYS] + [(plane_at(z, y, w, 0), tp) for w in WAYS] + [(fs, tp + 1 - 2 * core)]


def first_chain(buf, high, low, pair, v, p, q, sent, coef, release):
    def diag(i, total):
        block = buf[i, :, :, pl.ds(0, LANE)].reshape(LANE, LANE)
        eye = lax.broadcasted_iota(jnp.int32, block.shape, 0) == lax.broadcasted_iota(jnp.int32, block.shape, 1)
        return total + jnp.where(eye, block, 0.0)

    acc = lax.fori_loop(0, PLANE, diag, jnp.zeros((LANE, LANE), jnp.float32))
    ssq = jnp.sum(jnp.sum(acc, axis=0, keepdims=True), axis=1, keepdims=True)
    s = 0.5 * lax.rsqrt(jnp.maximum(ssq / D, 1.0))
    s2 = s * s
    release()
    fs, tp = lax.axis_index("fs"), lax.axis_index("tp")
    shape = v.shape
    start = pl.multiple_of(128 * fs + 64 * lax.rem(tp, 2), 64)
    on_diag = lax.broadcasted_iota(jnp.int32, shape, 1) == start + lax.broadcasted_iota(jnp.int32, shape, 0)
    mine = pl.ds(start, shape[0])
    v[...] = s2 * (high[mine, :].astype(jnp.float32) + low[mine, :].astype(jnp.float32))

    @pl.loop(0, 2)
    def _(n):
        times(v, p, pair, high, low, s2)

        @pl.when(n == 0)
        def _():
            coef[...] = s * (jnp.where(on_diag, A_COEF, 0.0) + B_COEF * v[...] + C_COEF * p[...])

        times(p, q, pair, high, low, s2)
        v[...] = A_COEF * v[...] + B_COEF * p[...] + C_COEF * q[...]

    turned(v, sent)


def closing(
    poly, turned_out, mix_out, high, low, pair, v, p, q, full, rows, left_side, rest_send, rest_recv, go_send, go_recv, poly_own,
    poly_send, poly_recv,
):
    fs, tp, z, y, x, core = places()
    right = 2 * lax.rem(x + 1, SIDE) + core
    left = 2 * lax.rem(x + SIDE - 1, SIDE) + core
    other = tp + 1 - 2 * core
    ahead, back, across = lax.rem(x + 1, SIDE), lax.rem(x + SIDE - 1, SIDE), lax.rem(x + 2, SIDE)

    rest = Rest(full, SPANS, rest_send, rest_recv)
    rest.start(0)
    rest.start(1)
    v[...] = poly[...]

    @pl.loop(0, 5)
    def _(n):
        @pl.when(lax.rem(n, 2) == 1)
        def _():
            times(v, q, pair, high, low)
            v[...] = q[...]

        times(v, p, pair, high, low)
        times(p, q, pair, high, low)
        v[...] = A_COEF * v[...] + B_COEF * p[...] + C_COEF * q[...]

        @pl.when(n == 0)
        def _():
            poly[...] = A_COEF * v[...]

        @pl.when(n == 2)
        def _():
            poly[...] += B_COEF * v[...]
            rest.relay(0)
            rest.start(2)

        @pl.when(n == 4)
        def _():
            poly[...] += C_COEF * v[...]

    half = poly.shape[0] // 2
    parts = [pl.ds(0, half), pl.ds(half, half)]

    def go(i, src, slot_x, part, target):
        return put(src, rows.at[slot_x, core, part], go_send.at[i], go_recv.at[i], fs, target)

    go_right = [go(h, poly.at[parts[h]], x, parts[h], right) for h in (0, 1)]
    go_left = [go(2 + h, poly.at[parts[1 - h]], x, parts[1 - h], left) for h in (0, 1)]
    for h in (0, 1):
        go_right[h].start()
        go_left[h].start()
    mine = pltpu.make_async_copy(poly, rows.at[x, core], poly_own)
    mine.start()

    def to_pair(i, slot_x, src=None):
        at = rows.at[slot_x, core]
        copy = put(at if src is None else src, at, poly_send.at[i], poly_recv.at[i], fs, other)
        copy.start()
        return copy

    pairs = [to_pair(0, x, poly)]
    rest.relay(1)
    go_right[0].wait_recv()
    relay_right = go(4, rows.at[back, core, parts[0]], back, parts[0], right)
    relay_right.start()
    go_left[0].wait_recv()
    relay_left = go(5, rows.at[ahead, core, parts[1]], ahead, parts[1], left)
    relay_left.start()
    rest.relay(2)
    go_right[1].wait_recv()
    pairs.append(to_pair(1, back))
    go_left[1].wait_recv()
    pairs.append(to_pair(2, ahead))
    rest.finish()

    @pl.loop(0, 2 * PLANE)
    def _(n):
        at = pl.ds(pl.multiple_of(64 * n, 64), 64)
        src = pl.ds(pl.multiple_of(64 * lax.rem(n, 2), 64), 64)
        high[at, pl.ds(0, PACKED)], low[at, pl.ds(0, PACKED)] = split(full[n // 2, src, :])

    def product(m):
        for c in (0, 1):
            left_side[pl.ds(64 * c, 64), :], left_side[pl.ds(LANE + 64 * c, 64), :] = split(rows[OWNER[m], c])
        first, tiles = ((0, 3), (WIDE, 3), (2 * FFB, 1))[m]
        for t in range(tiles):
            start = first + 256 * t
            cols = pl.ds(start, 256)
            main = jnp.dot(left_side[...], high[:, cols], preferred_element_type=jnp.float32)
            side = jnp.dot(left_side[:LANE, :], low[:, cols], preferred_element_type=jnp.float32)
            value = main[:LANE] + (main[LANE:] + side)
            if m == 2:
                mix_out[...] = value
                continue
            value = value.T
            low_cut, high_cut = max(start, FFB * m), min(start + 256, FFB * (m + 1))
            turned_out[pl.ds(low_cut, high_cut - low_cut), :] = value[low_cut - start : high_cut - start]

    mine.wait()
    for copy in pairs:
        copy.wait_recv()
    for m in range(3):

        @pl.when(across != OWNER[m])
        def _():
            product(m)

    relay_right.wait_recv()
    relay_left.wait_recv()
    pairs.append(to_pair(3, across))
    pairs[3].wait_recv()
    for m in range(3):

        @pl.when(across == OWNER[m])
        def _():
            product(m)

    for copy in go_right + go_left + [relay_right, relay_left] + pairs:
        copy.wait_send()


def whole_kernel(
    turned_in, mix, turned_out, mix_out, full, part, twin, total, far, near, hold, buf, high, low, left_side, v, p, q, coef, sent, rows,
    free, cross_send, cross_recv, twin_send, twin_recv, sum_send, sum_recv, first_send, first_recv, first_own, first_pair_send,
    first_pair_recv, next_send, next_recv, next_own, next_pair_send, next_pair_recv, rest_send, rest_recv, go_send, go_recv,
    poly_own, poly_send, poly_recv,
):
    fs, tp, z, y, x, core = places()
    for i in range(2 * FFB // LANE):
        full[fs, :, pl.ds(LANE * i, LANE)] = turned_in[pl.ds(LANE * i, LANE), :].T
    full[fs, :, pl.ds(2 * FFB, MIX)] = mix[...]
    peers = plane_peers()
    greet(peers + [(fs, 2 * lax.rem(x + w + SIDE, SIDE) + core) for w in WAYS])
    size = SIDE * LANE
    top, under = pl.ds(0, size), pl.ds(size, size)
    lh, ll = (ref.at[top, pl.ds(0, WIDTH_LEFT)] for ref in (high, low))
    rh, rl = (ref.at[under, pl.ds(0, PACKED)] for ref in (high, low))
    opening(full, sent, lh, ll, rh, rl, part, twin, total, far, near, hold, cross_send, cross_recv, twin_send, twin_recv, sum_send, sum_recv)
    plane_gather(sent, buf, high, low, True, first_send, first_recv, first_own, first_pair_send, first_pair_recv)
    pair = left_side.at[pl.ds(0, LANE)]

    def release():
        for to_fs, to_tp in peers:
            pl.semaphore_signal(free, inc=1, device_id=(to_fs, to_tp), device_id_type=MESH)

    first_chain(buf, high, low, pair, v, p, q, sent, coef, release)
    pl.semaphore_wait(free, len(peers))
    plane_gather(sent, buf, high, low, False, next_send, next_recv, next_own, next_pair_send, next_pair_recv)
    closing(
        coef, turned_out, mix_out, high, low, pair, v, p, q, full, rows, left_side, rest_send, rest_recv, go_send, go_recv, poly_own,
        poly_send, poly_recv,
    )


def whole(turned_in, mix):
    f32, bf16, dma = jnp.float32, jnp.bfloat16, pltpu.SemaphoreType.DMA
    vmem = pl.BlockSpec(memory_space=pltpu.VMEM)
    half = 64
    quad = (SIDE, half, SIDE * LANE)
    duo = (2,) + quad[1:]
    gather = [dma((40,)), dma((40,)), dma, dma((PLANE,)), dma((PLANE,))]
    moves = 12 * len(GROUPS)
    return pl.pallas_call(
        whole_kernel,
        out_shape=[jax.ShapeDtypeStruct((2 * FFB, LANE), f32), jax.ShapeDtypeStruct((LANE, MIX), f32)],
        in_specs=[vmem] * 2,
        out_specs=[vmem] * 2,
        scratch_shapes=[
            pltpu.VMEM((PLANE, LANE, PACKED), f32),
            pltpu.VMEM((3, SIDE, 2) + quad[1:], f32),
            pltpu.VMEM((3,) + quad, f32),
            pltpu.VMEM((3,) + quad, f32),
            pltpu.VMEM((3, 2) + duo, f32),
            pltpu.VMEM((4,) + duo, f32),
            pltpu.VMEM((3, 2) + duo, f32),
            pltpu.VMEM((PLANE, 2, half, TURN * LANE), f32),
            pltpu.VMEM((D, D), bf16),
            pltpu.VMEM((D, D), bf16),
            pltpu.VMEM((2 * LANE, D), bf16),
        ]
        + [pltpu.VMEM((half, D), f32)] * 4
        + [
            pltpu.VMEM((half, TURN * LANE), f32),
            pltpu.VMEM((SIDE, 2, half, D), f32),
            pltpu.SemaphoreType.REGULAR,
            dma((moves,)),
            dma((moves,)),
            dma((3,)),
            dma((3,)),
            dma((3, 10)),
            dma((3, 10)),
        ]
        + gather
        + gather
        + [dma((8 * len(SPANS),))] * 2
        + [dma((6,)), dma((6,)), dma, dma((4,)), dma((4,))],
        compiler_params=pltpu.CompilerParams(collective_id=0, has_side_effects=True, vmem_limit_bytes=64000000),
        name="whole",
    )(turned_in, mix)


def local(weights_in, weights_mix, momentum_in, momentum_mix, grads_in, grads_mix):
    turned_in = MOMENTUM_DECAY * jnp.swapaxes(momentum_in, 1, 2) + jnp.swapaxes(grads_in, 1, 2)
    moment_mix = MOMENTUM_DECAY * momentum_mix + grads_mix
    turned_step, step_mix = whole(turned_in.reshape(2 * FFB, LANE), moment_mix)
    turned_step = math.sqrt(max(D, FF)) * turned_step.reshape(2, FFB, LANE)
    step_mix = math.sqrt(D) * step_mix
    turned_weights = jnp.swapaxes(weights_in, 1, 2) - STEP_RATE * turned_step
    return (
        jnp.swapaxes(turned_in, 1, 2),
        moment_mix,
        jnp.swapaxes(turned_weights, 1, 2),
        weights_mix - STEP_RATE * step_mix,
        jnp.swapaxes(turned_step, 1, 2),
        step_mix,
    )


def solution(mesh):
    specs = (
        P(None, "fs", "tp"),
        P("fs", "tp"),
        P(None, "fs", "tp"),
        P("fs", "tp"),
        P(None, "fs", "tp"),
        P("fs", "tp"),
    )
    return jax.shard_map(local, mesh=mesh, in_specs=specs, out_specs=specs, check_vma=False)
```

```python
import functools
import math

import jax
import jax.numpy as jnp
from jax import lax
from jax.experimental import pallas as pl
from jax.experimental.pallas import tpu as pltpu
from jax.sharding import PartitionSpec as P

D = 2048
FF = 5632
ITERS = 3

A_COEF = 3.4445
B_COEF = -4.775
C_COEF = 2.0315
MOMENTUM_DECAY = 0.95
STEP_RATE = 0.02
MESH = pl.DeviceIdType.MESH

SIDE = 4
PLANE = SIDE * SIDE
LANE = 128
TURN = PLANE // 2 + 1
WIDE = 640
ODD = 64
MIX = 256
FFB = WIDE + ODD
PACKED = 2 * FFB + MIX
WAYS = (1, -1)
FAR = (-1, 1, 2)
SPANS = tuple((e, 0, PACKED) for e in FAR)
GROUPS = ((0, WIDE + LANE), (WIDE + LANE, WIDE), (2 * FFB, MIX))
LEFT = ((0, WIDE + LANE), (WIDE + LANE, WIDE + LANE), (2 * (WIDE + LANE), MIX))
RIGHT = (0, WIDE, 2 * FFB)
WIDTH_LEFT = 2 * (WIDE + LANE) + MIX
OWNER = (1, 0, 2)


def put(src, dst, send, recv, fs, tp):
    return pltpu.make_async_remote_copy(
        src_ref=src, dst_ref=dst, send_sem=send, recv_sem=recv, device_id=(fs, tp), device_id_type=MESH
    )


def greet(peers):
    barrier = pltpu.get_barrier_semaphore()
    for fs, tp in peers:
        pl.semaphore_signal(barrier, inc=1, device_id=(fs, tp), device_id_type=MESH)
    pl.semaphore_wait(barrier, len(peers))


def plane_gather(block, buf, high, low, crossed, send, recv, own_sem, pair_send, pair_recv):
    fs, tp, z, y, x, core = places()
    other = tp + 1 - 2 * core
    half = block.shape[0] // 2
    quarter = half // 2

    def near(h, first, second):
        return plane_at(z, y, second, first) if h == 0 else plane_at(z, y, first, second)

    started, moves, pairs = [], iter(range(40)), {}

    def move(origin, rows, target, src=None):
        lane = next(moves)
        dst = buf.at[origin, core, rows]
        copy = put(dst if src is None else src, dst, send.at[lane], recv.at[lane], target, tp)
        copy.start()
        started.append(copy)
        return copy

    def halves(h):
        return pl.ds(h * half, half)

    def quarters(h, i):
        return pl.ds(h * half + i * quarter, quarter)

    def to_pair(along_z, along_y, src=None):
        at = buf.at[plane_at(z, y, along_z, along_y), core]
        k = len(pairs)
        copy = put(at if src is None else src, at, pair_send.at[k], pair_recv.at[k], fs, other)
        copy.start()
        pairs[along_z, along_y] = copy
        started.append(copy)

    direct = {(h, i): move(fs, halves(h), near(h, w, 0), block.at[halves(h)]) for i, w in enumerate(WAYS) for h in (0, 1)}
    second = {(h, i, 0): move(fs, halves(h), near(h, 0, w), block.at[halves(h)]) for i, w in enumerate(WAYS) for h in (0, 1)}
    keep = pltpu.make_async_copy(block, buf.at[fs, core], own_sem)
    keep.start()
    to_pair(0, 0, block)
    relay = {}
    for i, w in enumerate(WAYS):
        for h in (0, 1):
            direct[h, i].wait_recv()
            origin = near(h, -w, 0)
            relay[h, i] = move(origin, quarters(h, i), near(h, w, 0))
            for j, w2 in enumerate(WAYS):
                second[h, j, -w] = move(origin, halves(h), near(h, 0, w2))
    for h in (0, 1):
        for i in (0, 1):
            relay[h, i].wait_recv()
        origin = near(h, 2, 0)
        for j, w2 in enumerate(WAYS):
            second[h, j, 2] = move(origin, halves(h), near(h, 0, w2))

    def rebuild(i):
        sent = buf.at[i]
        for b in range(TURN):
            j = lax.rem(i + b, PLANE)
            row, col = i, j
            if crossed:
                row = SIDE * (i // SIDE) + lax.rem(j, SIDE)
                col = SIDE * (j // SIDE) + lax.rem(i, SIDE)
            rows = pl.ds(pl.multiple_of(LANE * row, LANE), LANE)
            cols = pl.ds(pl.multiple_of(LANE * col, LANE), LANE)
            value = sent[:, :, pl.ds(LANE * b, LANE)].reshape(LANE, LANE)
            high[rows, cols], low[rows, cols] = split(value)
            if 0 < b < TURN - 1:
                high[cols, rows], low[cols, rows] = split(value.T)

    tail = {}
    for e in (0, -1, 1, 2):
        for j, w2 in enumerate(WAYS):
            for h in (0, 1):
                second[h, j, e].wait_recv()
                tail[h, j, e] = move(near(h, e, -w2), quarters(h, j), near(h, 0, w2))
        if e == 0:
            for w in WAYS:
                to_pair(0, w)
                to_pair(w, 0)
        if e == -1:
            keep.wait()
            for w in WAYS:
                pairs[0, w].wait_recv()
                pairs[w, 0].wait_recv()
            pairs[0, 0].wait_recv()

            @pl.loop(0, 3)
            def _(n):
                rebuild(plane_at(z, y, 0, n - 1))

            @pl.loop(0, 2)
            def _(n):
                rebuild(plane_at(z, y, 2 * n - 1, 0))

        if e == 1:
            for w in WAYS:
                for w2 in WAYS:
                    to_pair(w, w2)

    for w in WAYS:
        for w2 in WAYS:
            pairs[w, w2].wait_recv()

    @pl.loop(0, 4)
    def _(n):
        rebuild(plane_at(z, y, 2 * (n // 2) - 1, 2 * lax.rem(n, 2) - 1))

    def last_hop(e):
        for j in (0, 1):
            for h in (0, 1):
                tail[h, j, e].wait_recv()
        to_pair(2, e)
        if e != 2:
            to_pair(e, 2)

    for e in (0, -1, 1):
        last_hop(e)
    for e in (0, -1, 1):
        pairs[e, 2].wait_recv()
        pairs[2, e].wait_recv()

    @pl.loop(0, 3)
    def _(n):
        rebuild(plane_at(z, y, n - 1, 2))

    last_hop(2)

    @pl.loop(0, 3)
    def _(n):
        rebuild(plane_at(z, y, 2, n - 1))

    pairs[2, 2].wait_recv()
    rebuild(plane_at(z, y, 2, 2))
    for copy in started:
        copy.wait_send()


def places():
    fs, tp = lax.axis_index("fs"), lax.axis_index("tp")
    return fs, tp, fs // SIDE, lax.rem(fs, SIDE), tp // 2, lax.rem(tp, 2)


def plane_at(z, y, along_z, along_y):
    return SIDE * lax.rem(z + along_z + SIDE, SIDE) + lax.rem(y + along_y + SIDE, SIDE)


class Rest:
    def __init__(self, full, spans, send, recv):
        fs, tp, z, y, x, core = places()
        self.z, self.y, self.tp, self.full, self.spans, self.send, self.recv = z, y, tp, full, spans, send, recv
        self.half = full.shape[1] // 2

    def part(self, s, h, f, row, count):
        e, col, width = self.spans[s]
        origin = plane_at(self.z, self.y, f, e) if h == 0 else plane_at(self.z, self.y, e, f)
        return self.full.at[origin, pl.ds(h * self.half + row, count), pl.ds(col, width)]

    def copy(self, s, i, h, again):
        w, quarter = WAYS[i], self.half // 2
        part = self.part(s, h, -w, quarter * i, quarter) if again else self.part(s, h, 0, 0, self.half)
        target = plane_at(self.z, self.y, w, 0) if h == 0 else plane_at(self.z, self.y, 0, w)
        lane = 8 * s + 4 * again + 2 * i + h
        return put(part, part, self.send.at[lane], self.recv.at[lane], target, self.tp)

    def start(self, s):
        for i in (0, 1):
            for h in (0, 1):
                self.copy(s, i, h, 0).start()

    def relay(self, s):
        for i in (0, 1):
            for h in (0, 1):
                self.copy(s, i, h, 0).wait_recv()
                self.copy(s, i, h, 1).start()

    def finish(self):
        for s in range(len(self.spans)):
            for i in (0, 1):
                for h in (0, 1):
                    self.copy(s, i, h, 1).wait_recv()
                    for again in (0, 1):
                        self.copy(s, i, h, again).wait_send()


def opening(full, rest, out, lh, ll, rh, rl, whole_gram, part, pair, total, far, near, hold, send, recv, pair_send, pair_recv, sum_send, sum_recv):
    fs, tp, z, y, x, core = places()
    right = 2 * lax.rem(x + 1, SIDE) + core
    left = 2 * lax.rem(x + SIDE - 1, SIDE) + core
    other = tp + 1 - 2 * core
    near_by = [[plane_at(z, y, 0, w) for w in WAYS], [plane_at(z, y, w, 0) for w in WAYS]]
    rows = full.shape[1] // 2
    parts = [pl.ds(0, rows), pl.ds(rows, rows)]
    lane = iter(range(12 * len(GROUPS)))
    direct, relays, started = {}, {}, []

    def move(src, dst, target):
        i = next(lane)
        copy = put(src, dst, send.at[i], recv.at[i], target, tp)
        copy.start()
        started.append(copy)
        return copy

    def set_off(g):
        cols = pl.ds(*GROUPS[g])
        for k in (0, 1):
            for i in (0, 1):
                for d in (0, 1):
                    half = parts[(i + k) % 2]
                    mine = full.at[fs, half, cols]
                    direct[g, i, d, k] = move(mine, mine, near_by[d][i])

    def relay(g):
        cols = pl.ds(*GROUPS[g])
        for i, w in enumerate(WAYS):
            for d in (0, 1):
                direct[g, i, d, 0].wait_recv()
                half = full.at[near_by[d][1 - i], parts[i], cols]
                relays[g, i, d] = move(half, half, near_by[d][i])

    def arrived(g):
        for i in (0, 1):
            for d in (0, 1):
                direct[g, i, d, 1].wait_recv()
                relays[g, i, d].wait_recv()

    def prepare(g):
        first, width = GROUPS[g]
        last = first + width

        @pl.loop(0, 2 * SIDE)
        def _(n):
            at = pl.ds(pl.multiple_of(64 * n, 64), 64)
            src = pl.ds(pl.multiple_of(64 * lax.rem(n, 2), 64), 64)
            cols = pl.ds(first, width)
            rh[at, cols], rl[at, cols] = split(full[SIDE * (n // 2) + y, src, cols])
            if g == 0:
                plain, shared = pl.ds(0, WIDE), pl.ds(WIDE, LANE)
                lh[at, plain], ll[at, plain] = split(full[SIDE * z + n // 2, src, plain])
                value = full[SIDE * z + n // 2, src, shared]
                low_lane = lax.broadcasted_iota(jnp.int32, value.shape, 1) < ODD
                lh[at, shared], ll[at, shared] = split(jnp.where(low_lane, value, 0.0))
                next_to = pl.ds(WIDE + LANE, LANE)
                lh[at, next_to], ll[at, next_to] = split(jnp.where(low_lane, 0.0, value))
            else:
                to = pl.ds(first + LANE, width)
                lh[at, to], ll[at, to] = split(full[SIDE * z + n // 2, src, cols])

    def gram(m):
        lc = pl.ds(*LEFT[m])
        rc = pl.ds(RIGHT[m], LEFT[m][1])
        dot = functools.partial(
            lax.dot_general, dimension_numbers=(((1,), (1,)), ((), ())), preferred_element_type=jnp.float32
        )
        for r in (0, 1):
            at = pl.ds(256 * r, 256)
            value = dot(lh[at, lc], rh[:, rc]) + (dot(lh[at, lc], rl[:, rc]) + dot(ll[at, lc], rh[:, rc]))
            whole_gram[at, :] = value
        for d in range(TURN):
            chip = lax.rem(fs + d, PLANE)
            cols = pl.ds(pl.multiple_of(LANE * (chip // SIDE), LANE), LANE)
            for c in (0, 1):
                at = pl.ds(pl.multiple_of(LANE * lax.rem(chip, SIDE) + 64 * c, 64), 64)
                part[m, c, :, :, pl.ds(LANE * d, LANE)] = whole_gram[at, cols].reshape(part.shape[2:4] + (LANE,))

    def to_pair(m):
        return put(part.at[m, 1 - core], pair.at[m], pair_send.at[m], pair_recv.at[m], fs, other)

    up, down = pl.ds(0, 2), pl.ds(2, 2)

    def far_copy(m, side, c):
        src = total.at[m, c] if side == 0 else total.at[m, 2 + c]
        i = 2 * side + c
        return put(src, far.at[m, side, c], sum_send.at[m, i], sum_recv.at[m, i], fs, (right, left)[side])

    def near_copy(m, side):
        src = total.at[m, down] if side == 0 else total.at[m, up]
        return put(src, near.at[side], sum_send.at[m, 4 + side], sum_recv.at[m, 4 + side], fs, (right, left)[side])

    def hold_copy(m, side, c):
        i = 6 + 2 * side + c
        return put(hold.at[m, side, c], near.at[2 + side, c], sum_send.at[m, i], sum_recv.at[m, i], fs, (right, left)[side])

    def before(m):
        return x == (OWNER[m] + SIDE - 1) % SIDE

    def after(m):
        return x == (OWNER[m] + 1) % SIDE

    def beyond(m):
        return x == (OWNER[m] + 2) % SIDE

    def sums(m):
        to_pair(m).wait()
        total[m] = part[m, core] + pair[m]

        @pl.when(beyond(m))
        def _():
            for c in (0, 1):
                for side in (0, 1):
                    far_copy(m, side, c).start()

        for side, role in ((0, before), (1, after)):

            @pl.when(role(m))
            def _():
                near_copy(m, side).start()

    def pass_on(m):
        for side, role in ((0, before), (1, after)):

            @pl.when(role(m))
            def _():
                for c in (0, 1):
                    far_copy(m, side, c).wait_recv()
                    hold[m, side, c] = far[m, side, c] + total[m, c if side == 0 else 2 + c]
                    hold_copy(m, side, c).start()

    def keep_sum(m):
        @pl.when(x == OWNER[m])
        def _():
            near_copy(m, 0).wait_recv()
            near_copy(m, 1).wait_recv()
            for c in (0, 1):
                for side in (0, 1):
                    hold_copy(m, side, c).wait_recv()
            rows_up, rows_down = pl.ds(0, 32), pl.ds(32, 32)
            out[rows_up, :] = (total[m, up] + near[2] + near[1]).reshape(32, TURN * LANE)
            out[rows_down, :] = (total[m, down] + near[3] + near[0]).reshape(32, TURN * LANE)

    def sent(m):
        @pl.when(beyond(m))
        def _():
            for c in (0, 1):
                for side in (0, 1):
                    far_copy(m, side, c).wait_send()

        for side, role in ((0, before), (1, after)):

            @pl.when(role(m))
            def _():
                near_copy(m, side).wait_send()
                for c in (0, 1):
                    hold_copy(m, side, c).wait_send()

    set_off(0)
    relay(0)
    set_off(1)
    arrived(0)
    prepare(0)
    gram(0)
    to_pair(0).start()
    relay(1)
    set_off(2)
    sums(0)
    pass_on(0)
    arrived(1)
    prepare(1)
    relay(2)
    gram(1)
    to_pair(1).start()
    arrived(2)
    rest.start(0)
    prepare(2)
    gram(2)
    to_pair(2).start()
    sums(1)
    sums(2)
    pass_on(1)
    pass_on(2)

    @pl.when(x == SIDE - 1)
    def _():
        out[...] = jnp.zeros_like(out)

    for m in range(3):
        keep_sum(m)
    for m in range(3):
        sent(m)
    for copy in started:
        copy.wait_send()


def turned(rows, dst):
    fs = lax.axis_index("fs")
    for b in range(TURN):
        col = pl.multiple_of(LANE * lax.rem(fs + b, PLANE), LANE)
        dst[:, pl.ds(LANE * b, LANE)] = rows[:, pl.ds(col, LANE)]


def split(value):
    top = value.astype(jnp.bfloat16)
    return top, (value - top.astype(jnp.float32)).astype(jnp.bfloat16)


def times(src, dst, pair, high, low, scale=None):
    rows = src.shape[0]
    pair[:rows, :], pair[rows:, :] = split(src[...])
    main = jnp.dot(pair[...], high[...], preferred_element_type=jnp.float32)
    rest = jnp.dot(pair[...], low[...], preferred_element_type=jnp.float32)
    value = main[:rows] + (main[rows:] + (rest[:rows] + rest[rows:]))
    dst[...] = value if scale is None else scale * value


def plane_peers():
    fs, tp, z, y, x, core = places()
    return [(plane_at(z, y, 0, w), tp) for w in WAYS] + [(plane_at(z, y, w, 0), tp) for w in WAYS] + [(fs, tp + 1 - 2 * core)]


def first_chain(buf, high, low, pair, v, p, q, sent, coef, release):
    def diag(i, total):
        block = buf[i, :, :, pl.ds(0, LANE)].reshape(LANE, LANE)
        eye = lax.broadcasted_iota(jnp.int32, block.shape, 0) == lax.broadcasted_iota(jnp.int32, block.shape, 1)
        return total + jnp.where(eye, block, 0.0)

    acc = lax.fori_loop(0, PLANE, diag, jnp.zeros((LANE, LANE), jnp.float32))
    ssq = jnp.sum(jnp.sum(acc, axis=0, keepdims=True), axis=1, keepdims=True)
    s = 0.5 * lax.rsqrt(jnp.maximum(ssq / D, 1.0))
    s2 = s * s
    release()
    fs, tp = lax.axis_index("fs"), lax.axis_index("tp")
    shape = v.shape
    start = pl.multiple_of(128 * fs + 64 * lax.rem(tp, 2), 64)
    on_diag = lax.broadcasted_iota(jnp.int32, shape, 1) == start + lax.broadcasted_iota(jnp.int32, shape, 0)
    mine = pl.ds(start, shape[0])
    v[...] = s2 * (high[mine, :].astype(jnp.float32) + low[mine, :].astype(jnp.float32))

    @pl.loop(0, 2)
    def _(n):
        times(v, p, pair, high, low, s2)

        @pl.when(n == 0)
        def _():
            coef[...] = s * (jnp.where(on_diag, A_COEF, 0.0) + B_COEF * v[...] + C_COEF * p[...])

        times(p, q, pair, high, low, s2)
        v[...] = A_COEF * v[...] + B_COEF * p[...] + C_COEF * q[...]

    turned(v, sent)


def closing(
    poly, turned_out, mix_out, high, low, pair, v, p, q, full, rest, rows, left_side, go_send, go_recv, poly_own, poly_send, poly_recv
):
    fs, tp, z, y, x, core = places()
    right = 2 * lax.rem(x + 1, SIDE) + core
    left = 2 * lax.rem(x + SIDE - 1, SIDE) + core
    other = tp + 1 - 2 * core
    ahead, back, across = lax.rem(x + 1, SIDE), lax.rem(x + SIDE - 1, SIDE), lax.rem(x + 2, SIDE)

    rest.start(1)
    rest.start(2)
    v[...] = poly[...]

    @pl.loop(0, 5)
    def _(n):
        @pl.when(lax.rem(n, 2) == 1)
        def _():
            times(v, q, pair, high, low)
            v[...] = q[...]

        times(v, p, pair, high, low)
        times(p, q, pair, high, low)
        v[...] = A_COEF * v[...] + B_COEF * p[...] + C_COEF * q[...]

        @pl.when(n == 0)
        def _():
            poly[...] = A_COEF * v[...]

        @pl.when(n == 2)
        def _():
            poly[...] += B_COEF * v[...]
            rest.relay(1)

        @pl.when(n == 3)
        def _():
            rest.relay(2)

        @pl.when(n == 4)
        def _():
            poly[...] += C_COEF * v[...]

    half = poly.shape[0] // 2
    parts = [pl.ds(0, half), pl.ds(half, half)]

    def go(i, src, slot_x, part, target):
        return put(src, rows.at[slot_x, core, part], go_send.at[i], go_recv.at[i], fs, target)

    go_right = [go(h, poly.at[parts[h]], x, parts[h], right) for h in (0, 1)]
    go_left = [go(2 + h, poly.at[parts[1 - h]], x, parts[1 - h], left) for h in (0, 1)]
    for h in (0, 1):
        go_right[h].start()
        go_left[h].start()
    mine = pltpu.make_async_copy(poly, rows.at[x, core], poly_own)
    mine.start()

    def to_pair(i, slot_x, src=None):
        at = rows.at[slot_x, core]
        copy = put(at if src is None else src, at, poly_send.at[i], poly_recv.at[i], fs, other)
        copy.start()
        return copy

    pairs = [to_pair(0, x, poly)]
    rest.finish()

    @pl.loop(0, 2 * PLANE)
    def _(n):
        at = pl.ds(pl.multiple_of(64 * n, 64), 64)
        src = pl.ds(pl.multiple_of(64 * lax.rem(n, 2), 64), 64)
        high[at, pl.ds(0, PACKED)], low[at, pl.ds(0, PACKED)] = split(full[n // 2, src, :])

    go_right[0].wait_recv()
    relay_right = go(4, rows.at[back, core, parts[0]], back, parts[0], right)
    relay_right.start()
    go_left[0].wait_recv()
    relay_left = go(5, rows.at[ahead, core, parts[1]], ahead, parts[1], left)
    relay_left.start()
    go_right[1].wait_recv()
    pairs.append(to_pair(1, back))
    go_left[1].wait_recv()
    pairs.append(to_pair(2, ahead))

    def product(m):
        for c in (0, 1):
            left_side[pl.ds(64 * c, 64), :], left_side[pl.ds(LANE + 64 * c, 64), :] = split(rows[OWNER[m], c])
        first, tiles = ((0, 3), (WIDE, 3), (2 * FFB, 1))[m]
        for t in range(tiles):
            start = first + 256 * t
            cols = pl.ds(start, 256)
            main = jnp.dot(left_side[...], high[:, cols], preferred_element_type=jnp.float32)
            side = jnp.dot(left_side[:LANE, :], low[:, cols], preferred_element_type=jnp.float32)
            value = main[:LANE] + (main[LANE:] + side)
            if m == 2:
                mix_out[...] = value
                continue
            value = value.T
            low_cut, high_cut = max(start, FFB * m), min(start + 256, FFB * (m + 1))
            turned_out[pl.ds(low_cut, high_cut - low_cut), :] = value[low_cut - start : high_cut - start]

    mine.wait()
    for copy in pairs:
        copy.wait_recv()
    for m in range(3):

        @pl.when(across != OWNER[m])
        def _():
            product(m)

    relay_right.wait_recv()
    relay_left.wait_recv()
    pairs.append(to_pair(3, across))
    pairs[3].wait_recv()
    for m in range(3):

        @pl.when(across == OWNER[m])
        def _():
            product(m)

    for copy in go_right + go_left + [relay_right, relay_left] + pairs:
        copy.wait_send()


def whole_kernel(
    turned_in, mix, turned_out, mix_out, full, whole_gram, part, twin, total, far, near, hold, buf, high, low, left_side, v, p, q, coef, sent, rows,
    free, cross_send, cross_recv, twin_send, twin_recv, sum_send, sum_recv, first_send, first_recv, first_own, first_pair_send,
    first_pair_recv, next_send, next_recv, next_own, next_pair_send, next_pair_recv, rest_send, rest_recv, go_send, go_recv,
    poly_own, poly_send, poly_recv,
):
    fs, tp, z, y, x, core = places()
    for i in range(2 * FFB // LANE):
        full[fs, :, pl.ds(LANE * i, LANE)] = turned_in[pl.ds(LANE * i, LANE), :].T
    full[fs, :, pl.ds(2 * FFB, MIX)] = mix[...]
    peers = plane_peers()
    greet(peers + [(fs, 2 * lax.rem(x + w + SIDE, SIDE) + core) for w in WAYS])
    size = SIDE * LANE
    top, under = pl.ds(0, size), pl.ds(size, size)
    lh, ll = (ref.at[top, pl.ds(0, WIDTH_LEFT)] for ref in (high, low))
    rh, rl = (ref.at[under, pl.ds(0, PACKED)] for ref in (high, low))
    rest = Rest(full, SPANS, rest_send, rest_recv)
    opening(full, rest, sent, lh, ll, rh, rl, whole_gram, part, twin, total, far, near, hold, cross_send, cross_recv, twin_send, twin_recv, sum_send, sum_recv)
    plane_gather(sent, buf, high, low, True, first_send, first_recv, first_own, first_pair_send, first_pair_recv)
    rest.relay(0)
    pair = left_side.at[pl.ds(0, LANE)]

    def release():
        for to_fs, to_tp in peers:
            pl.semaphore_signal(free, inc=1, device_id=(to_fs, to_tp), device_id_type=MESH)

    first_chain(buf, high, low, pair, v, p, q, sent, coef, release)
    pl.semaphore_wait(free, len(peers))
    plane_gather(sent, buf, high, low, False, next_send, next_recv, next_own, next_pair_send, next_pair_recv)
    closing(
        coef, turned_out, mix_out, high, low, pair, v, p, q, full, rest, rows, left_side, go_send, go_recv, poly_own, poly_send, poly_recv
    )


def whole(turned_in, mix):
    f32, bf16, dma = jnp.float32, jnp.bfloat16, pltpu.SemaphoreType.DMA
    vmem = pl.BlockSpec(memory_space=pltpu.VMEM)
    half = 64
    size = SIDE * LANE
    quad = (4, half // 4, TURN * LANE)
    duo = (2,) + quad[1:]
    gather = [dma((40,)), dma((40,)), dma, dma((PLANE,)), dma((PLANE,))]
    moves = 12 * len(GROUPS)
    return pl.pallas_call(
        whole_kernel,
        out_shape=[jax.ShapeDtypeStruct((2 * FFB, LANE), f32), jax.ShapeDtypeStruct((LANE, MIX), f32)],
        in_specs=[vmem] * 2,
        out_specs=[vmem] * 2,
        scratch_shapes=[
            pltpu.VMEM((PLANE, LANE, PACKED), f32),
            pltpu.VMEM((size, size), f32),
            pltpu.VMEM((3, 2) + quad, f32),
            pltpu.VMEM((3,) + quad, f32),
            pltpu.VMEM((3,) + quad, f32),
            pltpu.VMEM((3, 2) + duo, f32),
            pltpu.VMEM((4,) + duo, f32),
            pltpu.VMEM((3, 2) + duo, f32),
            pltpu.VMEM((PLANE, 2, half, TURN * LANE), f32),
            pltpu.VMEM((D, D), bf16),
            pltpu.VMEM((D, D), bf16),
            pltpu.VMEM((2 * LANE, D), bf16),
        ]
        + [pltpu.VMEM((half, D), f32)] * 4
        + [
            pltpu.VMEM((half, TURN * LANE), f32),
            pltpu.VMEM((SIDE, 2, half, D), f32),
            pltpu.SemaphoreType.REGULAR,
            dma((moves,)),
            dma((moves,)),
            dma((3,)),
            dma((3,)),
            dma((3, 10)),
            dma((3, 10)),
        ]
        + gather
        + gather
        + [dma((8 * len(SPANS),))] * 2
        + [dma((6,)), dma((6,)), dma, dma((4,)), dma((4,))],
        compiler_params=pltpu.CompilerParams(collective_id=0, has_side_effects=True, vmem_limit_bytes=64000000),
        name="whole",
    )(turned_in, mix)


def local(weights_in, weights_mix, momentum_in, momentum_mix, grads_in, grads_mix):
    turned_in = MOMENTUM_DECAY * jnp.swapaxes(momentum_in, 1, 2) + jnp.swapaxes(grads_in, 1, 2)
    moment_mix = MOMENTUM_DECAY * momentum_mix + grads_mix
    turned_step, step_mix = whole(turned_in.reshape(2 * FFB, LANE), moment_mix)
    turned_step = math.sqrt(max(D, FF)) * turned_step
    step_mix = math.sqrt(D) * step_mix
    turned_weights = jnp.swapaxes(weights_in, 1, 2).reshape(2 * FFB, LANE) - STEP_RATE * turned_step
    turned_step, turned_weights = (t.reshape(2, FFB, LANE) for t in (turned_step, turned_weights))
    return (
        jnp.swapaxes(turned_in, 1, 2),
        moment_mix,
        jnp.swapaxes(turned_weights, 1, 2),
        weights_mix - STEP_RATE * step_mix,
        jnp.swapaxes(turned_step, 1, 2),
        step_mix,
    )


def solution(mesh):
    specs = (
        P(None, "fs", "tp"),
        P("fs", "tp"),
        P(None, "fs", "tp"),
        P("fs", "tp"),
        P(None, "fs", "tp"),
        P("fs", "tp"),
    )
    return jax.shard_map(local, mesh=mesh, in_specs=specs, out_specs=specs, check_vma=False)
```

```python
import functools
import math

import jax
import jax.numpy as jnp
from jax import lax
from jax.experimental import pallas as pl
from jax.experimental.pallas import tpu as pltpu
from jax.sharding import PartitionSpec as P

D = 2048
FF = 5632
ITERS = 3

A_COEF = 3.4445
B_COEF = -4.775
C_COEF = 2.0315
MOMENTUM_DECAY = 0.95
STEP_RATE = 0.02
MESH = pl.DeviceIdType.MESH

SIDE = 4
PLANE = SIDE * SIDE
LANE = 128
TURN = PLANE // 2 + 1
WIDE = 640
ODD = 64
MIX = 256
FFB = WIDE + ODD
PACKED = 2 * FFB + MIX
WAYS = (1, -1)
FAR = (-1, 1, 2)
SPANS = tuple((e, 0, PACKED) for e in FAR)
GROUPS = ((0, WIDE + LANE), (WIDE + LANE, WIDE), (2 * FFB, MIX))
LEFT = ((0, WIDE + LANE), (WIDE + LANE, WIDE + LANE), (2 * (WIDE + LANE), MIX))
RIGHT = (0, WIDE, 2 * FFB)
WIDTH_LEFT = 2 * (WIDE + LANE) + MIX
OWNER = (1, 0, 2)


def put(src, dst, send, recv, fs, tp):
    return pltpu.make_async_remote_copy(
        src_ref=src, dst_ref=dst, send_sem=send, recv_sem=recv, device_id=(fs, tp), device_id_type=MESH
    )


def greet(peers):
    barrier = pltpu.get_barrier_semaphore()
    for fs, tp in peers:
        pl.semaphore_signal(barrier, inc=1, device_id=(fs, tp), device_id_type=MESH)
    pl.semaphore_wait(barrier, len(peers))


def plane_gather(block, buf, high, low, crossed, send, recv, own_sem, pair_send, pair_recv):
    fs, tp, z, y, x, core = places()
    other = tp + 1 - 2 * core
    half = block.shape[0] // 2
    quarter = half // 2

    def near(h, first, second):
        return plane_at(z, y, second, first) if h == 0 else plane_at(z, y, first, second)

    started, moves, pairs = [], iter(range(40)), {}

    def move(origin, rows, target, src=None):
        lane = next(moves)
        dst = buf.at[origin, core, rows]
        copy = put(dst if src is None else src, dst, send.at[lane], recv.at[lane], target, tp)
        copy.start()
        started.append(copy)
        return copy

    def halves(h):
        return pl.ds(h * half, half)

    def quarters(h, i):
        return pl.ds(h * half + i * quarter, quarter)

    def to_pair(along_z, along_y, src=None):
        at = buf.at[plane_at(z, y, along_z, along_y), core]
        k = len(pairs)
        copy = put(at if src is None else src, at, pair_send.at[k], pair_recv.at[k], fs, other)
        copy.start()
        pairs[along_z, along_y] = copy
        started.append(copy)

    direct = {(h, i): move(fs, halves(h), near(h, w, 0), block.at[halves(h)]) for i, w in enumerate(WAYS) for h in (0, 1)}
    second = {(h, i, 0): move(fs, halves(h), near(h, 0, w), block.at[halves(h)]) for i, w in enumerate(WAYS) for h in (0, 1)}
    keep = pltpu.make_async_copy(block, buf.at[fs, core], own_sem)
    keep.start()
    to_pair(0, 0, block)
    relay = {}
    for i, w in enumerate(WAYS):
        for h in (0, 1):
            direct[h, i].wait_recv()
            origin = near(h, -w, 0)
            relay[h, i] = move(origin, quarters(h, i), near(h, w, 0))
            for j, w2 in enumerate(WAYS):
                second[h, j, -w] = move(origin, halves(h), near(h, 0, w2))
    for h in (0, 1):
        for i in (0, 1):
            relay[h, i].wait_recv()
        origin = near(h, 2, 0)
        for j, w2 in enumerate(WAYS):
            second[h, j, 2] = move(origin, halves(h), near(h, 0, w2))

    def rebuild(i):
        sent = buf.at[i]
        for b in range(TURN):
            j = lax.rem(i + b, PLANE)
            row, col = i, j
            if crossed:
                row = SIDE * (i // SIDE) + lax.rem(j, SIDE)
                col = SIDE * (j // SIDE) + lax.rem(i, SIDE)
            rows = pl.ds(pl.multiple_of(LANE * row, LANE), LANE)
            cols = pl.ds(pl.multiple_of(LANE * col, LANE), LANE)
            value = sent[:, :, pl.ds(LANE * b, LANE)].reshape(LANE, LANE)
            high[rows, cols], low[rows, cols] = split(value)
            if 0 < b < TURN - 1:
                high[cols, rows], low[cols, rows] = split(value.T)

    tail = {}
    for e in (0, -1, 1, 2):
        for j, w2 in enumerate(WAYS):
            for h in (0, 1):
                second[h, j, e].wait_recv()
                tail[h, j, e] = move(near(h, e, -w2), quarters(h, j), near(h, 0, w2))
        if e == 0:
            for w in WAYS:
                to_pair(0, w)
                to_pair(w, 0)
        if e == -1:
            keep.wait()
            for w in WAYS:
                pairs[0, w].wait_recv()
                pairs[w, 0].wait_recv()
            pairs[0, 0].wait_recv()

            @pl.loop(0, 3)
            def _(n):
                rebuild(plane_at(z, y, 0, n - 1))

            @pl.loop(0, 2)
            def _(n):
                rebuild(plane_at(z, y, 2 * n - 1, 0))

        if e == 1:
            for w in WAYS:
                for w2 in WAYS:
                    to_pair(w, w2)
            for w in WAYS:
                for w2 in WAYS:
                    pairs[w, w2].wait_recv()

            @pl.loop(0, 4)
            def _(n):
                rebuild(plane_at(z, y, 2 * (n // 2) - 1, 2 * lax.rem(n, 2) - 1))

    def last_hop(e):
        for j in (0, 1):
            for h in (0, 1):
                tail[h, j, e].wait_recv()
        to_pair(2, e)
        if e != 2:
            to_pair(e, 2)

    def across(e):
        pairs[2, e].wait_recv()
        pairs[e, 2].wait_recv()

        @pl.loop(0, 2)
        def _(n):
            rebuild(plane_at(z, y, 2 + (e - 2) * n, e + (2 - e) * n))

    last_hop(0)
    last_hop(-1)
    across(0)
    last_hop(1)
    across(-1)
    last_hop(2)
    across(1)
    pairs[2, 2].wait_recv()
    rebuild(plane_at(z, y, 2, 2))
    for copy in started:
        copy.wait_send()


def places():
    fs, tp = lax.axis_index("fs"), lax.axis_index("tp")
    return fs, tp, fs // SIDE, lax.rem(fs, SIDE), tp // 2, lax.rem(tp, 2)


def plane_at(z, y, along_z, along_y):
    return SIDE * lax.rem(z + along_z + SIDE, SIDE) + lax.rem(y + along_y + SIDE, SIDE)


class Rest:
    def __init__(self, full, spans, send, recv):
        fs, tp, z, y, x, core = places()
        self.z, self.y, self.tp, self.full, self.spans, self.send, self.recv = z, y, tp, full, spans, send, recv
        self.half = full.shape[1] // 2

    def part(self, s, h, f, row, count):
        e, col, width = self.spans[s]
        origin = plane_at(self.z, self.y, f, e) if h == 0 else plane_at(self.z, self.y, e, f)
        return self.full.at[origin, pl.ds(h * self.half + row, count), pl.ds(col, width)]

    def copy(self, s, i, h, again):
        w, quarter = WAYS[i], self.half // 2
        part = self.part(s, h, -w, quarter * i, quarter) if again else self.part(s, h, 0, 0, self.half)
        target = plane_at(self.z, self.y, w, 0) if h == 0 else plane_at(self.z, self.y, 0, w)
        lane = 8 * s + 4 * again + 2 * i + h
        return put(part, part, self.send.at[lane], self.recv.at[lane], target, self.tp)

    def start(self, s):
        for i in (0, 1):
            for h in (0, 1):
                self.copy(s, i, h, 0).start()

    def relay(self, s):
        for i in (0, 1):
            for h in (0, 1):
                self.copy(s, i, h, 0).wait_recv()
                self.copy(s, i, h, 1).start()

    def finish(self):
        for s in range(len(self.spans)):
            for i in (0, 1):
                for h in (0, 1):
                    self.copy(s, i, h, 1).wait_recv()
                    for again in (0, 1):
                        self.copy(s, i, h, again).wait_send()


def opening(full, rest, out, lh, ll, rh, rl, whole_gram, part, pair, total, far, near, hold, send, recv, pair_send, pair_recv, sum_send, sum_recv):
    fs, tp, z, y, x, core = places()
    right = 2 * lax.rem(x + 1, SIDE) + core
    left = 2 * lax.rem(x + SIDE - 1, SIDE) + core
    other = tp + 1 - 2 * core
    near_by = [[plane_at(z, y, 0, w) for w in WAYS], [plane_at(z, y, w, 0) for w in WAYS]]
    rows = full.shape[1] // 2
    parts = [pl.ds(0, rows), pl.ds(rows, rows)]
    lane = iter(range(12 * len(GROUPS)))
    direct, relays, started = {}, {}, []

    def move(src, dst, target):
        i = next(lane)
        copy = put(src, dst, send.at[i], recv.at[i], target, tp)
        copy.start()
        started.append(copy)
        return copy

    def set_off(g):
        cols = pl.ds(*GROUPS[g])
        for k in (0, 1):
            for i in (0, 1):
                for d in (0, 1):
                    half = parts[(i + k) % 2]
                    mine = full.at[fs, half, cols]
                    direct[g, i, d, k] = move(mine, mine, near_by[d][i])

    def relay(g):
        cols = pl.ds(*GROUPS[g])
        for i, w in enumerate(WAYS):
            for d in (0, 1):
                direct[g, i, d, 0].wait_recv()
                half = full.at[near_by[d][1 - i], parts[i], cols]
                relays[g, i, d] = move(half, half, near_by[d][i])

    def arrived(g):
        for i in (0, 1):
            for d in (0, 1):
                direct[g, i, d, 1].wait_recv()
                relays[g, i, d].wait_recv()

    def prepare(g):
        first, width = GROUPS[g]
        last = first + width

        @pl.loop(0, 2 * SIDE)
        def _(n):
            at = pl.ds(pl.multiple_of(64 * n, 64), 64)
            src = pl.ds(pl.multiple_of(64 * lax.rem(n, 2), 64), 64)
            cols = pl.ds(first, width)
            rh[at, cols], rl[at, cols] = split(full[SIDE * (n // 2) + y, src, cols])
            if g == 0:
                plain, shared = pl.ds(0, WIDE), pl.ds(WIDE, LANE)
                lh[at, plain], ll[at, plain] = split(full[SIDE * z + n // 2, src, plain])
                value = full[SIDE * z + n // 2, src, shared]
                low_lane = lax.broadcasted_iota(jnp.int32, value.shape, 1) < ODD
                lh[at, shared], ll[at, shared] = split(jnp.where(low_lane, value, 0.0))
                next_to = pl.ds(WIDE + LANE, LANE)
                lh[at, next_to], ll[at, next_to] = split(jnp.where(low_lane, 0.0, value))
            else:
                to = pl.ds(first + LANE, width)
                lh[at, to], ll[at, to] = split(full[SIDE * z + n // 2, src, cols])

    def gram(m):
        lc = pl.ds(*LEFT[m])
        rc = pl.ds(RIGHT[m], LEFT[m][1])
        dot = functools.partial(
            lax.dot_general, dimension_numbers=(((1,), (1,)), ((), ())), preferred_element_type=jnp.float32
        )
        for r in (0, 1):
            at = pl.ds(256 * r, 256)
            value = dot(lh[at, lc], rh[:, rc]) + (dot(lh[at, lc], rl[:, rc]) + dot(ll[at, lc], rh[:, rc]))
            whole_gram[at, :] = value
        for d in range(TURN):
            chip = lax.rem(fs + d, PLANE)
            cols = pl.ds(pl.multiple_of(LANE * (chip // SIDE), LANE), LANE)
            for c in (0, 1):
                at = pl.ds(pl.multiple_of(LANE * lax.rem(chip, SIDE) + 64 * c, 64), 64)
                part[m, c, :, :, pl.ds(LANE * d, LANE)] = whole_gram[at, cols].reshape(part.shape[2:4] + (LANE,))

    def to_pair(m):
        return put(part.at[m, 1 - core], pair.at[m], pair_send.at[m], pair_recv.at[m], fs, other)

    up, down = pl.ds(0, 2), pl.ds(2, 2)

    def far_copy(m, side, c):
        src = total.at[m, c] if side == 0 else total.at[m, 2 + c]
        i = 2 * side + c
        return put(src, far.at[m, side, c], sum_send.at[m, i], sum_recv.at[m, i], fs, (right, left)[side])

    def near_copy(m, side):
        src = total.at[m, down] if side == 0 else total.at[m, up]
        return put(src, near.at[side], sum_send.at[m, 4 + side], sum_recv.at[m, 4 + side], fs, (right, left)[side])

    def hold_copy(m, side, c):
        i = 6 + 2 * side + c
        return put(hold.at[m, side, c], near.at[2 + side, c], sum_send.at[m, i], sum_recv.at[m, i], fs, (right, left)[side])

    def before(m):
        return x == (OWNER[m] + SIDE - 1) % SIDE

    def after(m):
        return x == (OWNER[m] + 1) % SIDE

    def beyond(m):
        return x == (OWNER[m] + 2) % SIDE

    def sums(m):
        to_pair(m).wait()
        total[m] = part[m, core] + pair[m]

        @pl.when(beyond(m))
        def _():
            for c in (0, 1):
                for side in (0, 1):
                    far_copy(m, side, c).start()

        for side, role in ((0, before), (1, after)):

            @pl.when(role(m))
            def _():
                near_copy(m, side).start()

    def pass_on(m):
        for side, role in ((0, before), (1, after)):

            @pl.when(role(m))
            def _():
                for c in (0, 1):
                    far_copy(m, side, c).wait_recv()
                    hold[m, side, c] = far[m, side, c] + total[m, c if side == 0 else 2 + c]
                    hold_copy(m, side, c).start()

    def keep_sum(m):
        @pl.when(x == OWNER[m])
        def _():
            near_copy(m, 0).wait_recv()
            near_copy(m, 1).wait_recv()
            for c in (0, 1):
                for side in (0, 1):
                    hold_copy(m, side, c).wait_recv()
            rows_up, rows_down = pl.ds(0, 32), pl.ds(32, 32)
            out[rows_up, :] = (total[m, up] + near[2] + near[1]).reshape(32, TURN * LANE)
            out[rows_down, :] = (total[m, down] + near[3] + near[0]).reshape(32, TURN * LANE)

    def sent(m):
        @pl.when(beyond(m))
        def _():
            for c in (0, 1):
                for side in (0, 1):
                    far_copy(m, side, c).wait_send()

        for side, role in ((0, before), (1, after)):

            @pl.when(role(m))
            def _():
                near_copy(m, side).wait_send()
                for c in (0, 1):
                    hold_copy(m, side, c).wait_send()

    set_off(0)
    relay(0)
    set_off(1)
    arrived(0)
    prepare(0)
    gram(0)
    to_pair(0).start()
    relay(1)
    set_off(2)
    sums(0)
    pass_on(0)
    arrived(1)
    prepare(1)
    relay(2)
    gram(1)
    to_pair(1).start()
    arrived(2)
    rest.start(0)
    prepare(2)
    gram(2)
    to_pair(2).start()
    sums(1)
    sums(2)
    pass_on(1)
    pass_on(2)

    @pl.when(x == SIDE - 1)
    def _():
        out[...] = jnp.zeros_like(out)

    for m in range(3):
        keep_sum(m)
    for m in range(3):
        sent(m)
    for copy in started:
        copy.wait_send()


def turned(rows, dst):
    fs = lax.axis_index("fs")
    for b in range(TURN):
        col = pl.multiple_of(LANE * lax.rem(fs + b, PLANE), LANE)
        dst[:, pl.ds(LANE * b, LANE)] = rows[:, pl.ds(col, LANE)]


def split(value):
    top = value.astype(jnp.bfloat16)
    return top, (value - top.astype(jnp.float32)).astype(jnp.bfloat16)


def times(src, dst, pair, high, low, scale=None):
    rows = src.shape[0]
    pair[:rows, :], pair[rows:, :] = split(src[...])
    main = jnp.dot(pair[...], high[...], preferred_element_type=jnp.float32)
    rest = jnp.dot(pair[...], low[...], preferred_element_type=jnp.float32)
    value = main[:rows] + (main[rows:] + (rest[:rows] + rest[rows:]))
    dst[...] = value if scale is None else scale * value


def plane_peers():
    fs, tp, z, y, x, core = places()
    return [(plane_at(z, y, 0, w), tp) for w in WAYS] + [(plane_at(z, y, w, 0), tp) for w in WAYS] + [(fs, tp + 1 - 2 * core)]


def first_chain(buf, high, low, pair, v, p, q, sent, coef, release):
    def diag(i, total):
        block = buf[i, :, :, pl.ds(0, LANE)].reshape(LANE, LANE)
        eye = lax.broadcasted_iota(jnp.int32, block.shape, 0) == lax.broadcasted_iota(jnp.int32, block.shape, 1)
        return total + jnp.where(eye, block, 0.0)

    acc = lax.fori_loop(0, PLANE, diag, jnp.zeros((LANE, LANE), jnp.float32))
    ssq = jnp.sum(jnp.sum(acc, axis=0, keepdims=True), axis=1, keepdims=True)
    s = 0.5 * lax.rsqrt(jnp.maximum(ssq / D, 1.0))
    s2 = s * s
    release()
    fs, tp = lax.axis_index("fs"), lax.axis_index("tp")
    shape = v.shape
    start = pl.multiple_of(128 * fs + 64 * lax.rem(tp, 2), 64)
    on_diag = lax.broadcasted_iota(jnp.int32, shape, 1) == start + lax.broadcasted_iota(jnp.int32, shape, 0)
    mine = pl.ds(start, shape[0])
    v[...] = s2 * (high[mine, :].astype(jnp.float32) + low[mine, :].astype(jnp.float32))

    @pl.loop(0, 2)
    def _(n):
        times(v, p, pair, high, low, s2)

        @pl.when(n == 0)
        def _():
            coef[...] = s * (jnp.where(on_diag, A_COEF, 0.0) + B_COEF * v[...] + C_COEF * p[...])

        times(p, q, pair, high, low, s2)
        v[...] = A_COEF * v[...] + B_COEF * p[...] + C_COEF * q[...]

    turned(v, sent)


def closing(
    poly, turned_out, mix_out, high, low, pair, v, p, q, full, rest, rows, left_side, go_send, go_recv, poly_own, poly_send, poly_recv
):
    fs, tp, z, y, x, core = places()
    right = 2 * lax.rem(x + 1, SIDE) + core
    left = 2 * lax.rem(x + SIDE - 1, SIDE) + core
    other = tp + 1 - 2 * core
    ahead, back, across = lax.rem(x + 1, SIDE), lax.rem(x + SIDE - 1, SIDE), lax.rem(x + 2, SIDE)

    rest.start(1)
    rest.start(2)
    v[...] = poly[...]

    @pl.loop(0, 5)
    def _(n):
        @pl.when(lax.rem(n, 2) == 1)
        def _():
            times(v, q, pair, high, low)
            v[...] = q[...]

        times(v, p, pair, high, low)
        times(p, q, pair, high, low)
        v[...] = A_COEF * v[...] + B_COEF * p[...] + C_COEF * q[...]

        @pl.when(n == 0)
        def _():
            poly[...] = A_COEF * v[...]

        @pl.when(n == 2)
        def _():
            poly[...] += B_COEF * v[...]
            rest.relay(1)

        @pl.when(n == 3)
        def _():
            rest.relay(2)

        @pl.when(n == 4)
        def _():
            poly[...] += C_COEF * v[...]

    half = poly.shape[0] // 2
    parts = [pl.ds(0, half), pl.ds(half, half)]

    def go(i, src, slot_x, part, target):
        return put(src, rows.at[slot_x, core, part], go_send.at[i], go_recv.at[i], fs, target)

    go_right = [go(h, poly.at[parts[h]], x, parts[h], right) for h in (0, 1)]
    go_left = [go(2 + h, poly.at[parts[1 - h]], x, parts[1 - h], left) for h in (0, 1)]
    for h in (0, 1):
        go_right[h].start()
        go_left[h].start()
    mine = pltpu.make_async_copy(poly, rows.at[x, core], poly_own)
    mine.start()

    def to_pair(i, slot_x, src=None, part=slice(None)):
        at = rows.at[slot_x, core, part]
        copy = put(at if src is None else src, at, poly_send.at[i], poly_recv.at[i], fs, other)
        copy.start()
        return copy

    pairs = [to_pair(0, x, poly)]
    rest.finish()

    @pl.loop(0, 2 * PLANE)
    def _(n):
        at = pl.ds(pl.multiple_of(64 * n, 64), 64)
        src = pl.ds(pl.multiple_of(64 * lax.rem(n, 2), 64), 64)
        high[at, pl.ds(0, PACKED)], low[at, pl.ds(0, PACKED)] = split(full[n // 2, src, :])

    go_right[0].wait_recv()
    relay_right = go(4, rows.at[back, core, parts[0]], back, parts[0], right)
    relay_right.start()
    go_left[0].wait_recv()
    relay_left = go(5, rows.at[ahead, core, parts[1]], ahead, parts[1], left)
    relay_left.start()
    go_right[1].wait_recv()
    pairs.append(to_pair(1, back))
    go_left[1].wait_recv()
    pairs.append(to_pair(2, ahead))

    def product(m):
        for c in (0, 1):
            left_side[pl.ds(64 * c, 64), :], left_side[pl.ds(LANE + 64 * c, 64), :] = split(rows[OWNER[m], c])
        first, tiles = ((0, 3), (WIDE, 3), (2 * FFB, 1))[m]
        for t in range(tiles):
            start = first + 256 * t
            cols = pl.ds(start, 256)
            main = jnp.dot(left_side[...], high[:, cols], preferred_element_type=jnp.float32)
            side = jnp.dot(left_side[:LANE, :], low[:, cols], preferred_element_type=jnp.float32)
            value = main[:LANE] + (main[LANE:] + side)
            if m == 2:
                mix_out[...] = value
                continue
            value = value.T
            low_cut, high_cut = max(start, FFB * m), min(start + 256, FFB * (m + 1))
            turned_out[pl.ds(low_cut, high_cut - low_cut), :] = value[low_cut - start : high_cut - start]

    mine.wait()
    for copy in pairs:
        copy.wait_recv()
    for m in range(3):

        @pl.when(across != OWNER[m])
        def _():
            product(m)

    relay_right.wait_recv()
    pairs.append(to_pair(3, across, part=parts[0]))
    relay_left.wait_recv()
    pairs.append(to_pair(4, across, part=parts[1]))
    pairs[3].wait_recv()
    pairs[4].wait_recv()
    for m in range(3):

        @pl.when(across == OWNER[m])
        def _():
            product(m)

    for copy in go_right + go_left + [relay_right, relay_left] + pairs:
        copy.wait_send()


def whole_kernel(
    turned_in, mix, turned_out, mix_out, full, whole_gram, part, twin, total, far, near, hold, buf, high, low, left_side, v, p, q, coef, sent, rows,
    free, cross_send, cross_recv, twin_send, twin_recv, sum_send, sum_recv, first_send, first_recv, first_own, first_pair_send,
    first_pair_recv, next_send, next_recv, next_own, next_pair_send, next_pair_recv, rest_send, rest_recv, go_send, go_recv,
    poly_own, poly_send, poly_recv,
):
    fs, tp, z, y, x, core = places()
    for i in range(2 * FFB // LANE):
        full[fs, :, pl.ds(LANE * i, LANE)] = turned_in[pl.ds(LANE * i, LANE), :].T
    full[fs, :, pl.ds(2 * FFB, MIX)] = mix[...]
    peers = plane_peers()
    greet(peers + [(fs, 2 * lax.rem(x + w + SIDE, SIDE) + core) for w in WAYS])
    size = SIDE * LANE
    top, under = pl.ds(0, size), pl.ds(size, size)
    lh, ll = (ref.at[top, pl.ds(0, WIDTH_LEFT)] for ref in (high, low))
    rh, rl = (ref.at[under, pl.ds(0, PACKED)] for ref in (high, low))
    rest = Rest(full, SPANS, rest_send, rest_recv)
    opening(full, rest, sent, lh, ll, rh, rl, whole_gram, part, twin, total, far, near, hold, cross_send, cross_recv, twin_send, twin_recv, sum_send, sum_recv)
    plane_gather(sent, buf, high, low, True, first_send, first_recv, first_own, first_pair_send, first_pair_recv)
    rest.relay(0)
    pair = left_side.at[pl.ds(0, LANE)]

    def release():
        for to_fs, to_tp in peers:
            pl.semaphore_signal(free, inc=1, device_id=(to_fs, to_tp), device_id_type=MESH)

    first_chain(buf, high, low, pair, v, p, q, sent, coef, release)
    pl.semaphore_wait(free, len(peers))
    plane_gather(sent, buf, high, low, False, next_send, next_recv, next_own, next_pair_send, next_pair_recv)
    closing(
        coef, turned_out, mix_out, high, low, pair, v, p, q, full, rest, rows, left_side, go_send, go_recv, poly_own, poly_send, poly_recv
    )


def whole(turned_in, mix):
    f32, bf16, dma = jnp.float32, jnp.bfloat16, pltpu.SemaphoreType.DMA
    vmem = pl.BlockSpec(memory_space=pltpu.VMEM)
    half = 64
    size = SIDE * LANE
    quad = (4, half // 4, TURN * LANE)
    duo = (2,) + quad[1:]
    gather = [dma((40,)), dma((40,)), dma, dma((PLANE,)), dma((PLANE,))]
    moves = 12 * len(GROUPS)
    return pl.pallas_call(
        whole_kernel,
        out_shape=[jax.ShapeDtypeStruct((2 * FFB, LANE), f32), jax.ShapeDtypeStruct((LANE, MIX), f32)],
        in_specs=[vmem] * 2,
        out_specs=[vmem] * 2,
        scratch_shapes=[
            pltpu.VMEM((PLANE, LANE, PACKED), f32),
            pltpu.VMEM((size, size), f32),
            pltpu.VMEM((3, 2) + quad, f32),
            pltpu.VMEM((3,) + quad, f32),
            pltpu.VMEM((3,) + quad, f32),
            pltpu.VMEM((3, 2) + duo, f32),
            pltpu.VMEM((4,) + duo, f32),
            pltpu.VMEM((3, 2) + duo, f32),
            pltpu.VMEM((PLANE, 2, half, TURN * LANE), f32),
            pltpu.VMEM((D, D), bf16),
            pltpu.VMEM((D, D), bf16),
            pltpu.VMEM((2 * LANE, D), bf16),
        ]
        + [pltpu.VMEM((half, D), f32)] * 4
        + [
            pltpu.VMEM((half, TURN * LANE), f32),
            pltpu.VMEM((SIDE, 2, half, D), f32),
            pltpu.SemaphoreType.REGULAR,
            dma((moves,)),
            dma((moves,)),
            dma((3,)),
            dma((3,)),
            dma((3, 10)),
            dma((3, 10)),
        ]
        + gather
        + gather
        + [dma((8 * len(SPANS),))] * 2
        + [dma((6,)), dma((6,)), dma, dma((5,)), dma((5,))],
        compiler_params=pltpu.CompilerParams(collective_id=0, has_side_effects=True, vmem_limit_bytes=58000000),
        name="whole",
    )(turned_in, mix)


def local(weights_in, weights_mix, momentum_in, momentum_mix, grads_in, grads_mix):
    turned_in = MOMENTUM_DECAY * jnp.swapaxes(momentum_in, 1, 2) + jnp.swapaxes(grads_in, 1, 2)
    moment_mix = MOMENTUM_DECAY * momentum_mix + grads_mix
    turned_step, step_mix = whole(turned_in.reshape(2 * FFB, LANE), moment_mix)
    turned_step = math.sqrt(max(D, FF)) * turned_step
    step_mix = math.sqrt(D) * step_mix
    turned_weights = jnp.swapaxes(weights_in, 1, 2).reshape(2 * FFB, LANE) - STEP_RATE * turned_step
    turned_step, turned_weights = (t.reshape(2, FFB, LANE) for t in (turned_step, turned_weights))
    return (
        jnp.swapaxes(turned_in, 1, 2),
        moment_mix,
        jnp.swapaxes(turned_weights, 1, 2),
        weights_mix - STEP_RATE * step_mix,
        jnp.swapaxes(turned_step, 1, 2),
        step_mix,
    )


def solution(mesh):
    specs = (
        P(None, "fs", "tp"),
        P("fs", "tp"),
        P(None, "fs", "tp"),
        P("fs", "tp"),
        P(None, "fs", "tp"),
        P("fs", "tp"),
    )
    return jax.shard_map(local, mesh=mesh, in_specs=specs, out_specs=specs, check_vma=False)
```

```python
import functools
import math

import jax
import jax.numpy as jnp
from jax import lax
from jax.experimental import pallas as pl
from jax.experimental.pallas import tpu as pltpu
from jax.sharding import PartitionSpec as P

D = 2048
FF = 5632
ITERS = 3

A_COEF = 3.4445
B_COEF = -4.775
C_COEF = 2.0315
MOMENTUM_DECAY = 0.95
STEP_RATE = 0.02
MESH = pl.DeviceIdType.MESH

SIDE = 4
PLANE = SIDE * SIDE
LANE = 128
TURN = PLANE // 2 + 1
WIDE = 640
ODD = 64
MIX = 256
FFB = WIDE + ODD
PACKED = 2 * FFB + MIX
WAYS = (1, -1)
FAR = (-1, 1, 2)
SPANS = tuple((e, 0, PACKED) for e in FAR)
GROUPS = ((0, WIDE + LANE), (WIDE + LANE, WIDE), (2 * FFB, MIX))
LEFT = ((0, WIDE + LANE), (WIDE + LANE, WIDE + LANE), (2 * (WIDE + LANE), MIX))
RIGHT = (0, WIDE, 2 * FFB)
WIDTH_LEFT = 2 * (WIDE + LANE) + MIX
OWNER = (1, 0, 2)


def put(src, dst, send, recv, fs, tp):
    return pltpu.make_async_remote_copy(
        src_ref=src, dst_ref=dst, send_sem=send, recv_sem=recv, device_id=(fs, tp), device_id_type=MESH
    )


def greet(peers):
    barrier = pltpu.get_barrier_semaphore()
    for fs, tp in peers:
        pl.semaphore_signal(barrier, inc=1, device_id=(fs, tp), device_id_type=MESH)
    pl.semaphore_wait(barrier, len(peers))


def plane_gather(block, buf, high, low, crossed, send, recv, own_sem, pair_send, pair_recv):
    fs, tp, z, y, x, core = places()
    other = tp + 1 - 2 * core
    half = block.shape[0] // 2
    quarter = half // 2

    def near(h, first, second):
        return plane_at(z, y, second, first) if h == 0 else plane_at(z, y, first, second)

    started, moves, pairs = [], iter(range(40)), {}

    def move(origin, rows, target, src=None):
        lane = next(moves)
        dst = buf.at[origin, core, rows]
        copy = put(dst if src is None else src, dst, send.at[lane], recv.at[lane], target, tp)
        copy.start()
        started.append(copy)
        return copy

    def halves(h):
        return pl.ds(h * half, half)

    def quarters(h, i):
        return pl.ds(h * half + i * quarter, quarter)

    def to_pair(along_z, along_y, src=None):
        at = buf.at[plane_at(z, y, along_z, along_y), core]
        k = len(pairs)
        copy = put(at if src is None else src, at, pair_send.at[k], pair_recv.at[k], fs, other)
        copy.start()
        pairs[along_z, along_y] = copy
        started.append(copy)

    direct = {(h, i): move(fs, halves(h), near(h, w, 0), block.at[halves(h)]) for i, w in enumerate(WAYS) for h in (0, 1)}
    second = {(h, i, 0): move(fs, halves(h), near(h, 0, w), block.at[halves(h)]) for i, w in enumerate(WAYS) for h in (0, 1)}
    keep = pltpu.make_async_copy(block, buf.at[fs, core], own_sem)
    keep.start()
    to_pair(0, 0, block)
    relay = {}
    for i, w in enumerate(WAYS):
        for h in (0, 1):
            direct[h, i].wait_recv()
            origin = near(h, -w, 0)
            relay[h, i] = move(origin, quarters(h, i), near(h, w, 0))
            for j, w2 in enumerate(WAYS):
                second[h, j, -w] = move(origin, halves(h), near(h, 0, w2))
    for h in (0, 1):
        for i in (0, 1):
            relay[h, i].wait_recv()
        origin = near(h, 2, 0)
        for j, w2 in enumerate(WAYS):
            second[h, j, 2] = move(origin, halves(h), near(h, 0, w2))

    def rebuild(i):
        sent = buf.at[i]
        for b in range(TURN):
            j = lax.rem(i + b, PLANE)
            row, col = i, j
            if crossed:
                row = SIDE * (i // SIDE) + lax.rem(j, SIDE)
                col = SIDE * (j // SIDE) + lax.rem(i, SIDE)
            rows = pl.ds(pl.multiple_of(LANE * row, LANE), LANE)
            cols = pl.ds(pl.multiple_of(LANE * col, LANE), LANE)
            value = sent[:, :, pl.ds(LANE * b, LANE)].reshape(LANE, LANE)
            high[rows, cols], low[rows, cols] = split(value)
            if 0 < b < TURN - 1:
                high[cols, rows], low[cols, rows] = split(value.T)

    tail = {}
    for e in (0, -1, 1, 2):
        for j, w2 in enumerate(WAYS):
            for h in (0, 1):
                second[h, j, e].wait_recv()
                tail[h, j, e] = move(near(h, e, -w2), quarters(h, j), near(h, 0, w2))
        if e == 0:
            for w in WAYS:
                to_pair(0, w)
                to_pair(w, 0)
        if e == 1:
            for w in WAYS:
                for w2 in WAYS:
                    to_pair(w, w2)

    keep.wait()
    for copy in pairs.values():
        copy.wait_recv()

    @pl.loop(0, 9)
    def _(n):
        rebuild(plane_at(z, y, n // 3 - 1, lax.rem(n, 3) - 1))

    def last_hop(e):
        for j in (0, 1):
            for h in (0, 1):
                tail[h, j, e].wait_recv()
        to_pair(2, e)
        if e != 2:
            to_pair(e, 2)

    for e in (0, -1, 1):
        last_hop(e)
    for e in (0, -1, 1):
        pairs[e, 2].wait_recv()
        pairs[2, e].wait_recv()

    @pl.loop(0, 3)
    def _(n):
        rebuild(plane_at(z, y, n - 1, 2))

    last_hop(2)

    @pl.loop(0, 3)
    def _(n):
        rebuild(plane_at(z, y, 2, n - 1))

    pairs[2, 2].wait_recv()
    rebuild(plane_at(z, y, 2, 2))
    for copy in started:
        copy.wait_send()


def places():
    fs, tp = lax.axis_index("fs"), lax.axis_index("tp")
    return fs, tp, fs // SIDE, lax.rem(fs, SIDE), tp // 2, lax.rem(tp, 2)


def plane_at(z, y, along_z, along_y):
    return SIDE * lax.rem(z + along_z + SIDE, SIDE) + lax.rem(y + along_y + SIDE, SIDE)


class Rest:
    def __init__(self, full, spans, send, recv):
        fs, tp, z, y, x, core = places()
        self.z, self.y, self.tp, self.full, self.spans, self.send, self.recv = z, y, tp, full, spans, send, recv
        self.half = full.shape[1] // 2

    def part(self, s, h, f, row, count):
        e, col, width = self.spans[s]
        origin = plane_at(self.z, self.y, f, e) if h == 0 else plane_at(self.z, self.y, e, f)
        return self.full.at[origin, pl.ds(h * self.half + row, count), pl.ds(col, width)]

    def copy(self, s, i, h, again):
        w, quarter = WAYS[i], self.half // 2
        part = self.part(s, h, -w, quarter * i, quarter) if again else self.part(s, h, 0, 0, self.half)
        target = plane_at(self.z, self.y, w, 0) if h == 0 else plane_at(self.z, self.y, 0, w)
        lane = 8 * s + 4 * again + 2 * i + h
        return put(part, part, self.send.at[lane], self.recv.at[lane], target, self.tp)

    def start(self, s):
        for i in (0, 1):
            for h in (0, 1):
                self.copy(s, i, h, 0).start()

    def relay(self, s):
        for i in (0, 1):
            for h in (0, 1):
                self.copy(s, i, h, 0).wait_recv()
                self.copy(s, i, h, 1).start()

    def finish(self):
        for s in range(len(self.spans)):
            for i in (0, 1):
                for h in (0, 1):
                    self.copy(s, i, h, 1).wait_recv()
                    for again in (0, 1):
                        self.copy(s, i, h, again).wait_send()


def opening(full, rest, out, lh, ll, rh, rl, whole_gram, part, pair, total, far, near, hold, send, recv, pair_send, pair_recv, sum_send, sum_recv):
    fs, tp, z, y, x, core = places()
    right = 2 * lax.rem(x + 1, SIDE) + core
    left = 2 * lax.rem(x + SIDE - 1, SIDE) + core
    other = tp + 1 - 2 * core
    near_by = [[plane_at(z, y, 0, w) for w in WAYS], [plane_at(z, y, w, 0) for w in WAYS]]
    rows = full.shape[1] // 2
    parts = [pl.ds(0, rows), pl.ds(rows, rows)]
    lane = iter(range(12 * len(GROUPS)))
    direct, relays, started = {}, {}, []

    def move(src, dst, target):
        i = next(lane)
        copy = put(src, dst, send.at[i], recv.at[i], target, tp)
        copy.start()
        started.append(copy)
        return copy

    def set_off(g):
        cols = pl.ds(*GROUPS[g])
        for k in (0, 1):
            for i in (0, 1):
                for d in (0, 1):
                    half = parts[(i + k) % 2]
                    mine = full.at[fs, half, cols]
                    direct[g, i, d, k] = move(mine, mine, near_by[d][i])

    def relay(g):
        cols = pl.ds(*GROUPS[g])
        for i, w in enumerate(WAYS):
            for d in (0, 1):
                direct[g, i, d, 0].wait_recv()
                half = full.at[near_by[d][1 - i], parts[i], cols]
                relays[g, i, d] = move(half, half, near_by[d][i])

    def arrived(g):
        for i in (0, 1):
            for d in (0, 1):
                direct[g, i, d, 1].wait_recv()
                relays[g, i, d].wait_recv()

    def prepare(g):
        first, width = GROUPS[g]
        last = first + width

        @pl.loop(0, 2 * SIDE)
        def _(n):
            at = pl.ds(pl.multiple_of(64 * n, 64), 64)
            src = pl.ds(pl.multiple_of(64 * lax.rem(n, 2), 64), 64)
            cols = pl.ds(first, width)
            rh[at, cols], rl[at, cols] = split(full[SIDE * (n // 2) + y, src, cols])
            if g == 0:
                plain, shared = pl.ds(0, WIDE), pl.ds(WIDE, LANE)
                lh[at, plain], ll[at, plain] = split(full[SIDE * z + n // 2, src, plain])
                value = full[SIDE * z + n // 2, src, shared]
                low_lane = lax.broadcasted_iota(jnp.int32, value.shape, 1) < ODD
                lh[at, shared], ll[at, shared] = split(jnp.where(low_lane, value, 0.0))
                next_to = pl.ds(WIDE + LANE, LANE)
                lh[at, next_to], ll[at, next_to] = split(jnp.where(low_lane, 0.0, value))
            else:
                to = pl.ds(first + LANE, width)
                lh[at, to], ll[at, to] = split(full[SIDE * z + n // 2, src, cols])

    def gram(m):
        lc = pl.ds(*LEFT[m])
        rc = pl.ds(RIGHT[m], LEFT[m][1])
        dot = functools.partial(
            lax.dot_general, dimension_numbers=(((1,), (1,)), ((), ())), preferred_element_type=jnp.float32
        )
        for r in (0, 1):
            at = pl.ds(256 * r, 256)
            value = dot(lh[at, lc], rh[:, rc]) + (dot(lh[at, lc], rl[:, rc]) + dot(ll[at, lc], rh[:, rc]))
            whole_gram[at, :] = value
        for d in range(TURN):
            chip = lax.rem(fs + d, PLANE)
            cols = pl.ds(pl.multiple_of(LANE * (chip // SIDE), LANE), LANE)
            for c in (0, 1):
                at = pl.ds(pl.multiple_of(LANE * lax.rem(chip, SIDE) + 64 * c, 64), 64)
                part[m, c, :, :, pl.ds(LANE * d, LANE)] = whole_gram[at, cols].reshape(part.shape[2:4] + (LANE,))

    def to_pair(m):
        return put(part.at[m, 1 - core], pair.at[m], pair_send.at[m], pair_recv.at[m], fs, other)

    up, down = pl.ds(0, 2), pl.ds(2, 2)

    def far_copy(m, side, c):
        src = total.at[m, c] if side == 0 else total.at[m, 2 + c]
        i = 2 * side + c
        return put(src, far.at[m, side, c], sum_send.at[m, i], sum_recv.at[m, i], fs, (right, left)[side])

    def near_copy(m, side):
        src = total.at[m, down] if side == 0 else total.at[m, up]
        return put(src, near.at[side], sum_send.at[m, 4 + side], sum_recv.at[m, 4 + side], fs, (right, left)[side])

    def hold_copy(m, side, c):
        i = 6 + 2 * side + c
        return put(hold.at[m, side, c], near.at[2 + side, c], sum_send.at[m, i], sum_recv.at[m, i], fs, (right, left)[side])

    def before(m):
        return x == (OWNER[m] + SIDE - 1) % SIDE

    def after(m):
        return x == (OWNER[m] + 1) % SIDE

    def beyond(m):
        return x == (OWNER[m] + 2) % SIDE

    def sums(m):
        to_pair(m).wait()
        total[m] = part[m, core] + pair[m]

        @pl.when(beyond(m))
        def _():
            for c in (0, 1):
                for side in (0, 1):
                    far_copy(m, side, c).start()

        for side, role in ((0, before), (1, after)):

            @pl.when(role(m))
            def _():
                near_copy(m, side).start()

    def pass_on(m):
        for side, role in ((0, before), (1, after)):

            @pl.when(role(m))
            def _():
                for c in (0, 1):
                    far_copy(m, side, c).wait_recv()
                    hold[m, side, c] = far[m, side, c] + total[m, c if side == 0 else 2 + c]
                    hold_copy(m, side, c).start()

    def keep_sum(m):
        @pl.when(x == OWNER[m])
        def _():
            near_copy(m, 0).wait_recv()
            near_copy(m, 1).wait_recv()
            for c in (0, 1):
                for side in (0, 1):
                    hold_copy(m, side, c).wait_recv()
            rows_up, rows_down = pl.ds(0, 32), pl.ds(32, 32)
            out[rows_up, :] = (total[m, up] + near[2] + near[1]).reshape(32, TURN * LANE)
            out[rows_down, :] = (total[m, down] + near[3] + near[0]).reshape(32, TURN * LANE)

    def sent(m):
        @pl.when(beyond(m))
        def _():
            for c in (0, 1):
                for side in (0, 1):
                    far_copy(m, side, c).wait_send()

        for side, role in ((0, before), (1, after)):

            @pl.when(role(m))
            def _():
                near_copy(m, side).wait_send()
                for c in (0, 1):
                    hold_copy(m, side, c).wait_send()

    set_off(0)
    relay(0)
    set_off(1)
    arrived(0)
    prepare(0)
    gram(0)
    to_pair(0).start()
    relay(1)
    set_off(2)
    sums(0)
    pass_on(0)
    arrived(1)
    prepare(1)
    relay(2)
    gram(1)
    to_pair(1).start()
    arrived(2)
    rest.start(0)
    prepare(2)
    gram(2)
    to_pair(2).start()
    sums(1)
    sums(2)
    pass_on(1)
    pass_on(2)

    @pl.when(x == SIDE - 1)
    def _():
        out[...] = jnp.zeros_like(out)

    for m in range(3):
        keep_sum(m)
    for m in range(3):
        sent(m)
    for copy in started:
        copy.wait_send()


def turned(rows, dst):
    fs = lax.axis_index("fs")
    for b in range(TURN):
        col = pl.multiple_of(LANE * lax.rem(fs + b, PLANE), LANE)
        dst[:, pl.ds(LANE * b, LANE)] = rows[:, pl.ds(col, LANE)]


def split(value):
    top = value.astype(jnp.bfloat16)
    return top, (value - top.astype(jnp.float32)).astype(jnp.bfloat16)


def times(src, dst, pair, high, low, scale=None):
    rows = src.shape[0]
    pair[:rows, :], pair[rows:, :] = split(src[...])
    main = jnp.dot(pair[...], high[...], preferred_element_type=jnp.float32)
    rest = jnp.dot(pair[...], low[...], preferred_element_type=jnp.float32)
    value = main[:rows] + (main[rows:] + (rest[:rows] + rest[rows:]))
    dst[...] = value if scale is None else scale * value


def plane_peers():
    fs, tp, z, y, x, core = places()
    return [(plane_at(z, y, 0, w), tp) for w in WAYS] + [(plane_at(z, y, w, 0), tp) for w in WAYS] + [(fs, tp + 1 - 2 * core)]


def first_chain(buf, high, low, pair, v, p, q, sent, coef, release):
    def diag(i, total):
        block = buf[i, :, :, pl.ds(0, LANE)].reshape(LANE, LANE)
        eye = lax.broadcasted_iota(jnp.int32, block.shape, 0) == lax.broadcasted_iota(jnp.int32, block.shape, 1)
        return total + jnp.where(eye, block, 0.0)

    acc = lax.fori_loop(0, PLANE, diag, jnp.zeros((LANE, LANE), jnp.float32))
    ssq = jnp.sum(jnp.sum(acc, axis=0, keepdims=True), axis=1, keepdims=True)
    s = 0.5 * lax.rsqrt(jnp.maximum(ssq / D, 1.0))
    s2 = s * s
    release()
    fs, tp = lax.axis_index("fs"), lax.axis_index("tp")
    shape = v.shape
    start = pl.multiple_of(128 * fs + 64 * lax.rem(tp, 2), 64)
    on_diag = lax.broadcasted_iota(jnp.int32, shape, 1) == start + lax.broadcasted_iota(jnp.int32, shape, 0)
    mine = pl.ds(start, shape[0])
    v[...] = s2 * (high[mine, :].astype(jnp.float32) + low[mine, :].astype(jnp.float32))

    @pl.loop(0, 2)
    def _(n):
        times(v, p, pair, high, low, s2)

        @pl.when(n == 0)
        def _():
            coef[...] = s * (jnp.where(on_diag, A_COEF, 0.0) + B_COEF * v[...] + C_COEF * p[...])

        times(p, q, pair, high, low, s2)
        v[...] = A_COEF * v[...] + B_COEF * p[...] + C_COEF * q[...]

    turned(v, sent)


def closing(
    poly, turned_out, mix_out, high, low, pair, v, p, q, full, rest, rows, left_side, go_send, go_recv, poly_own, poly_send, poly_recv
):
    fs, tp, z, y, x, core = places()
    right = 2 * lax.rem(x + 1, SIDE) + core
    left = 2 * lax.rem(x + SIDE - 1, SIDE) + core
    other = tp + 1 - 2 * core
    ahead, back, across = lax.rem(x + 1, SIDE), lax.rem(x + SIDE - 1, SIDE), lax.rem(x + 2, SIDE)

    rest.start(1)
    rest.start(2)
    v[...] = poly[...]

    @pl.loop(0, 5)
    def _(n):
        @pl.when(lax.rem(n, 2) == 1)
        def _():
            times(v, q, pair, high, low)
            v[...] = q[...]

        times(v, p, pair, high, low)
        times(p, q, pair, high, low)
        v[...] = A_COEF * v[...] + B_COEF * p[...] + C_COEF * q[...]

        @pl.when(n == 0)
        def _():
            poly[...] = A_COEF * v[...]

        @pl.when(n == 2)
        def _():
            poly[...] += B_COEF * v[...]
            rest.relay(1)

        @pl.when(n == 3)
        def _():
            rest.relay(2)

        @pl.when(n == 4)
        def _():
            poly[...] += C_COEF * v[...]

    half = poly.shape[0] // 2
    parts = [pl.ds(0, half), pl.ds(half, half)]

    def go(i, src, slot_x, part, target):
        return put(src, rows.at[slot_x, core, part], go_send.at[i], go_recv.at[i], fs, target)

    go_right = [go(h, poly.at[parts[h]], x, parts[h], right) for h in (0, 1)]
    go_left = [go(2 + h, poly.at[parts[1 - h]], x, parts[1 - h], left) for h in (0, 1)]
    for h in (0, 1):
        go_right[h].start()
        go_left[h].start()
    mine = pltpu.make_async_copy(poly, rows.at[x, core], poly_own)
    mine.start()

    def to_pair(i, slot_x, src=None):
        at = rows.at[slot_x, core]
        copy = put(at if src is None else src, at, poly_send.at[i], poly_recv.at[i], fs, other)
        copy.start()
        return copy

    pairs = [to_pair(0, x, poly)]
    rest.finish()

    @pl.loop(0, 2 * PLANE)
    def _(n):
        at = pl.ds(pl.multiple_of(64 * n, 64), 64)
        src = pl.ds(pl.multiple_of(64 * lax.rem(n, 2), 64), 64)
        high[at, pl.ds(0, PACKED)], low[at, pl.ds(0, PACKED)] = split(full[n // 2, src, :])

    go_right[0].wait_recv()
    relay_right = go(4, rows.at[back, core, parts[0]], back, parts[0], right)
    relay_right.start()
    go_left[0].wait_recv()
    relay_left = go(5, rows.at[ahead, core, parts[1]], ahead, parts[1], left)
    relay_left.start()
    go_right[1].wait_recv()
    pairs.append(to_pair(1, back))
    go_left[1].wait_recv()
    pairs.append(to_pair(2, ahead))

    def product(m):
        for c in (0, 1):
            left_side[pl.ds(64 * c, 64), :], left_side[pl.ds(LANE + 64 * c, 64), :] = split(rows[OWNER[m], c])
        first, tiles = ((0, 3), (WIDE, 3), (2 * FFB, 1))[m]
        for t in range(tiles):
            start = first + 256 * t
            cols = pl.ds(start, 256)
            main = jnp.dot(left_side[...], high[:, cols], preferred_element_type=jnp.float32)
            side = jnp.dot(left_side[:LANE, :], low[:, cols], preferred_element_type=jnp.float32)
            value = main[:LANE] + (main[LANE:] + side)
            if m == 2:
                mix_out[...] = value
                continue
            value = value.T
            low_cut, high_cut = max(start, FFB * m), min(start + 256, FFB * (m + 1))
            turned_out[pl.ds(low_cut, high_cut - low_cut), :] = value[low_cut - start : high_cut - start]

    mine.wait()
    for copy in pairs:
        copy.wait_recv()
    for m in range(3):

        @pl.when(across != OWNER[m])
        def _():
            product(m)

    relay_right.wait_recv()
    relay_left.wait_recv()
    pairs.append(to_pair(3, across))
    pairs[3].wait_recv()
    for m in range(3):

        @pl.when(across == OWNER[m])
        def _():
            product(m)

    for copy in go_right + go_left + [relay_right, relay_left] + pairs:
        copy.wait_send()


def whole_kernel(
    turned_in, mix, turned_out, mix_out, full, whole_gram, part, twin, total, far, near, hold, buf, high, low, left_side, v, p, q, coef, sent, rows,
    free, cross_send, cross_recv, twin_send, twin_recv, sum_send, sum_recv, first_send, first_recv, first_own, first_pair_send,
    first_pair_recv, next_send, next_recv, next_own, next_pair_send, next_pair_recv, rest_send, rest_recv, go_send, go_recv,
    poly_own, poly_send, poly_recv,
):
    fs, tp, z, y, x, core = places()
    for i in range(2 * FFB // LANE):
        full[fs, :, pl.ds(LANE * i, LANE)] = turned_in[pl.ds(LANE * i, LANE), :].T
    full[fs, :, pl.ds(2 * FFB, MIX)] = mix[...]
    peers = plane_peers()
    greet(peers + [(fs, 2 * lax.rem(x + w + SIDE, SIDE) + core) for w in WAYS])
    size = SIDE * LANE
    top, under = pl.ds(0, size), pl.ds(size, size)
    lh, ll = (ref.at[top, pl.ds(0, WIDTH_LEFT)] for ref in (high, low))
    rh, rl = (ref.at[under, pl.ds(0, PACKED)] for ref in (high, low))
    rest = Rest(full, SPANS, rest_send, rest_recv)
    opening(full, rest, sent, lh, ll, rh, rl, whole_gram, part, twin, total, far, near, hold, cross_send, cross_recv, twin_send, twin_recv, sum_send, sum_recv)
    plane_gather(sent, buf, high, low, True, first_send, first_recv, first_own, first_pair_send, first_pair_recv)
    rest.relay(0)
    pair = left_side.at[pl.ds(0, LANE)]

    def release():
        for to_fs, to_tp in peers:
            pl.semaphore_signal(free, inc=1, device_id=(to_fs, to_tp), device_id_type=MESH)

    first_chain(buf, high, low, pair, v, p, q, sent, coef, release)
    pl.semaphore_wait(free, len(peers))
    plane_gather(sent, buf, high, low, False, next_send, next_recv, next_own, next_pair_send, next_pair_recv)
    closing(
        coef, turned_out, mix_out, high, low, pair, v, p, q, full, rest, rows, left_side, go_send, go_recv, poly_own, poly_send, poly_recv
    )


def whole(turned_in, mix):
    f32, bf16, dma = jnp.float32, jnp.bfloat16, pltpu.SemaphoreType.DMA
    vmem = pl.BlockSpec(memory_space=pltpu.VMEM)
    half = 64
    size = SIDE * LANE
    quad = (4, half // 4, TURN * LANE)
    duo = (2,) + quad[1:]
    gather = [dma((40,)), dma((40,)), dma, dma((PLANE,)), dma((PLANE,))]
    moves = 12 * len(GROUPS)
    return pl.pallas_call(
        whole_kernel,
        out_shape=[jax.ShapeDtypeStruct((2 * FFB, LANE), f32), jax.ShapeDtypeStruct((LANE, MIX), f32)],
        in_specs=[vmem] * 2,
        out_specs=[vmem] * 2,
        scratch_shapes=[
            pltpu.VMEM((PLANE, LANE, PACKED), f32),
            pltpu.VMEM((size, size), f32),
            pltpu.VMEM((3, 2) + quad, f32),
            pltpu.VMEM((3,) + quad, f32),
            pltpu.VMEM((3,) + quad, f32),
            pltpu.VMEM((3, 2) + duo, f32),
            pltpu.VMEM((4,) + duo, f32),
            pltpu.VMEM((3, 2) + duo, f32),
            pltpu.VMEM((PLANE, 2, half, TURN * LANE), f32),
            pltpu.VMEM((D, D), bf16),
            pltpu.VMEM((D, D), bf16),
            pltpu.VMEM((2 * LANE, D), bf16),
        ]
        + [pltpu.VMEM((half, D), f32)] * 4
        + [
            pltpu.VMEM((half, TURN * LANE), f32),
            pltpu.VMEM((SIDE, 2, half, D), f32),
            pltpu.SemaphoreType.REGULAR,
            dma((moves,)),
            dma((moves,)),
            dma((3,)),
            dma((3,)),
            dma((3, 10)),
            dma((3, 10)),
        ]
        + gather
        + gather
        + [dma((8 * len(SPANS),))] * 2
        + [dma((6,)), dma((6,)), dma, dma((4,)), dma((4,))],
        compiler_params=pltpu.CompilerParams(collective_id=0, has_side_effects=True, vmem_limit_bytes=64000000),
        name="whole",
    )(turned_in, mix)


def local(weights_in, weights_mix, momentum_in, momentum_mix, grads_in, grads_mix):
    turned_in = MOMENTUM_DECAY * jnp.swapaxes(momentum_in, 1, 2) + jnp.swapaxes(grads_in, 1, 2)
    moment_mix = MOMENTUM_DECAY * momentum_mix + grads_mix
    turned_step, step_mix = whole(turned_in.reshape(2 * FFB, LANE), moment_mix)
    turned_step = math.sqrt(max(D, FF)) * turned_step
    step_mix = math.sqrt(D) * step_mix
    turned_weights = jnp.swapaxes(weights_in, 1, 2).reshape(2 * FFB, LANE) - STEP_RATE * turned_step
    turned_step, turned_weights = (t.reshape(2, FFB, LANE) for t in (turned_step, turned_weights))
    return (
        jnp.swapaxes(turned_in, 1, 2),
        moment_mix,
        jnp.swapaxes(turned_weights, 1, 2),
        weights_mix - STEP_RATE * step_mix,
        jnp.swapaxes(turned_step, 1, 2),
        step_mix,
    )


def solution(mesh):
    specs = (
        P(None, "fs", "tp"),
        P("fs", "tp"),
        P(None, "fs", "tp"),
        P("fs", "tp"),
        P(None, "fs", "tp"),
        P("fs", "tp"),
    )
    return jax.shard_map(local, mesh=mesh, in_specs=specs, out_specs=specs, check_vma=False)
```
